32 devices in a mesh: ep: 32 (over z, y, x, core).
Axes of the slice: x: 2, y: 2, z: 4, core: 2. Of those that a mesh axis runs over, the one named last changes fastest.
Arguments:
- tokens: bfloat16 [512, 2048], P('ep'), may hold values from -6 to 6
- cache_keys: bfloat16 [512, 1024, 128], P('ep'), may hold values from -6 to 6
- cache_values: bfloat16 [512, 1024, 128], P('ep'), may hold values from -6 to 6
- cache_len: int32 [512], P('ep'), may hold values from 1 to 1024
- norm_gain_first: float32 [2048], replicated, may hold values from 0.1 to 1.9
- w_query: bfloat16 [2048, 2048], P(None, 'ep'), may hold values from -0.125 to 0.125
- w_key: bfloat16 [2048, 128], replicated, may hold values from -0.125 to 0.125
- w_value: bfloat16 [2048, 128], replicated, may hold values from -0.125 to 0.125
- head_bias: float32 [32], replicated, may hold values from -8.5 to -3
- w_output: bfloat16 [2048, 2048], P(None, 'ep'), may hold values from -0.125 to 0.125
- norm_gain_second: float32 [2048], replicated, may hold values from 0.1 to 1.9
- group_id: int32 [512], P('ep'), may hold values from 0 to 1, as said below
- member: int32 [512, 6], P('ep'), may hold values from 0 to 15, as said below
- group_gate: float32 [512], P('ep'), may hold values from 0.3 to 1
- member_weight: float32 [512, 6], P('ep'), may hold values from 0.05 to 0.5
- expert_gate_w: bfloat16 [32, 2048, 512], P('ep'), may hold values from -0.125 to 0.125
- expert_up_w: bfloat16 [32, 2048, 512], P('ep'), may hold values from -0.125 to 0.125
- expert_down_w: bfloat16 [32, 512, 2048], P('ep'), may hold values from -0.25 to 0.25
- dense_gate_w: bfloat16 [2048, 2048], P(None, 'ep'), may hold values from -0.125 to 0.125
- dense_up_w: bfloat16 [2048, 2048], P(None, 'ep'), may hold values from -1 to 1
- hidden_gain: float32 [2048], replicated, may hold values from 0.1 to 1.9
- dense_down_w: bfloat16 [2048, 2048], P(None, 'ep'), may hold values from -0.125 to 0.125
- branch_logit: float32 [2048], replicated, may hold values from -8 to 8
Outputs:
- mixed_out: bfloat16 [512, 2048], P('ep')
- new_keys: bfloat16 [512, 128], P('ep')
- new_values: bfloat16 [512, 128], P('ep')
The draws below stay inside these ranges and needn't reach their ends.
Inputs may be any that keep to these rules, and one draw needn't show every extreme that they name: `group_id`: each group number is named by exactly 8 of the tokens of one device. `member`: each row names 6 different members; with group_id, no expert is named by more than 8 tokens of one device, and some expert is named by 8 tokens of every device.
All inputs are finite; a program needn't handle non-finite values.
Results may differ from the reference program's by a relative error of at most 0.0085.
Values may be sent and summed in bfloat16 or wider, within the bound.
A program may use at most 128 MiB of HBM per device.

```python
import math
import jax
import jax.numpy as jnp
from jax import lax

D = 2048
HEADS = 32
HEAD_DIM = 64
KV_HEADS = 2
FD = 2048
FE = 512
PER_GROUP = 16
TOP_K = 6
SEQ_DEV = 16
CACHE = 1024
TOKENS = 512
EXPERTS = 32
GROUPS = 2
N_EP = 32


def group_table(key):
    block_count = TOKENS // SEQ_DEV
    block_keys = jax.random.split(jax.random.fold_in(key, 11), block_count)

    def shuffle_block(block_key):
        return jax.random.permutation(block_key, SEQ_DEV)
    shuffled = jax.vmap(shuffle_block)(block_keys)
    return (shuffled % GROUPS).reshape(TOKENS).astype(jnp.int32)


def draw_group_id(key, part):
    return group_table(key)


def draw_member(key, part):
    groups_of = group_table(key)
    common = jax.random.randint(jax.random.fold_in(key, 12), (GROUPS,), 0, PER_GROUP)
    common_token = jnp.take(common, groups_of)
    columns = jnp.arange(PER_GROUP, dtype=jnp.int32)[None, :]
    scores = jax.random.randint(jax.random.fold_in(key, 13), (TOKENS, PER_GROUP), 0, 1 << 20) * PER_GROUP + columns
    scores = jnp.where(columns == common_token[:, None], 1 << 26, scores)
    unused, chosen = lax.top_k(scores, TOP_K)
    order_scores = jax.random.randint(jax.random.fold_in(key, 14), (TOKENS, TOP_K), 0, 1 << 20) * TOP_K
    order_scores = order_scores + jnp.arange(TOP_K, dtype=jnp.int32)[None, :]
    reorder = jnp.argsort(order_scores, axis=1)
    return jnp.take_along_axis(chosen, reorder, axis=1).astype(jnp.int32)


def draw_head_bias(key, part):
    return jax.random.uniform(key, (HEADS,), jnp.float32, -7.5, -3.0)


def draw_dense_up_w(key, part):
    base = jax.random.normal(jax.random.fold_in(key, 21), (D, FD), jnp.float32) * D ** (-0.5)
    ramp = jnp.arange(FD, dtype=jnp.float32) / FD
    rising = jnp.exp(ramp * math.log(4.0))
    rough = jnp.exp(jax.random.uniform(jax.random.fold_in(key, 22), (FD,), jnp.float32, -0.7, 0.7))
    scaled = jnp.clip(base * (rising * rough)[None, :], -1.0, 1.0)
    return scaled.astype(jnp.bfloat16)


def place_ends(array, rng, low, top_value):
    place = [jax.random.randint(jax.random.fold_in(rng, axis), (), 0, length) for axis, length in enumerate(array.shape)]
    main_axis = array.shape.index(max(array.shape))
    neighbour = place[:main_axis] + [(place[main_axis] + 1) % array.shape[main_axis]] + place[main_axis + 1:]
    return array.at[tuple(place)].set(low).at[tuple(neighbour)].set(top_value)


def block_levels(own_key, extent, shards, least, high):
    gain = 1.0
    for axis_at, parts in shards:
        steps = jax.random.uniform(jax.random.fold_in(jax.random.fold_in(own_key, 6), axis_at), (parts,), jnp.float32, least / len(shards), high / len(shards))
        gain = gain * jnp.repeat(jnp.exp(steps), extent[axis_at] // parts).reshape((-1,) + (1,) * (len(extent) - 1 - axis_at))
    return gain


def bell_draw(key, dims, scale, most, pieces=(), kind=jnp.bfloat16):
    loudness = block_levels(key, dims, pieces, -0.22, 0.18) if pieces else 1.0
    values = jax.random.normal(key, dims, jnp.float32) * scale * loudness
    return jnp.minimum(jnp.maximum(values, -most), most).astype(kind)


def setup_inputs(seed: int = 0) -> dict:
    seeds = jax.random.split(jax.random.key(seed), 24)
    tokens = bell_draw(seeds[0], (TOKENS, D), 1.0, 6.0, ((0, 32),))
    cache_keys = bell_draw(seeds[1], (TOKENS, CACHE, KV_HEADS * HEAD_DIM), 1.0, 6.0, ((0, 32),))
    cache_values = bell_draw(seeds[2], (TOKENS, CACHE, KV_HEADS * HEAD_DIM), 1.0, 6.0, ((0, 32),))
    cache_len = place_ends(jax.random.randint(seeds[3], (TOKENS,), 1, CACHE + 1), jax.random.fold_in(seeds[3], 1), 1, CACHE).astype(jnp.int32)
    norm_gain_first = jnp.clip(1.0 + 0.18 * jax.random.normal(seeds[4], (D,), jnp.float32), 0.1, 1.9)
    w_query = bell_draw(seeds[5], (D, HEADS * HEAD_DIM), D ** -0.5, 0.125, ((1, 32),))
    w_key = bell_draw(seeds[6], (D, KV_HEADS * HEAD_DIM), D ** -0.5, 0.125)
    w_value = bell_draw(seeds[7], (D, KV_HEADS * HEAD_DIM), D ** -0.5, 0.125)
    head_bias = draw_head_bias(jax.random.fold_in(seeds[23], 71), 0)
    w_output = bell_draw(seeds[9], (HEADS * HEAD_DIM, D), (HEADS * HEAD_DIM) ** -0.5, 0.125, ((1, 32),))
    norm_gain_second = jnp.clip(1.0 + 0.18 * jax.random.normal(seeds[10], (D,), jnp.float32), 0.1, 1.9)
    group_id = draw_group_id(jax.random.fold_in(seeds[23], 71), 0)
    member = draw_member(jax.random.fold_in(seeds[23], 71), 0)
    group_gate = jnp.clip(jnp.exp(math.log(1.0) - 1.2039728 * jax.random.uniform(seeds[13], (TOKENS,), jnp.float32) ** block_levels(seeds[13], (TOKENS,), ((0, 32),), -0.2, 0.2)), 0.3, 1.0)
    member_weight = jnp.clip(jnp.exp(math.log(0.5) - 2.3025851 * jax.random.uniform(seeds[14], (TOKENS, TOP_K), jnp.float32) ** block_levels(seeds[14], (TOKENS, TOP_K), ((0, 32),), -0.2, 0.2)), 0.05, 0.5)
    expert_gate_w = bell_draw(seeds[15], (EXPERTS, D, FE), D ** -0.5, 0.125, ((0, 32),))
    expert_up_w = bell_draw(seeds[16], (EXPERTS, D, FE), D ** -0.5, 0.125, ((0, 32),))
    expert_down_w = bell_draw(seeds[17], (EXPERTS, FE, D), FE ** -0.5, 0.25, ((0, 32),))
    dense_gate_w = bell_draw(seeds[18], (D, FD), D ** -0.5, 0.125, ((1, 32),))
    dense_up_w = draw_dense_up_w(jax.random.fold_in(seeds[23], 71), 0)
    hidden_gain = jnp.clip(1.0 + 0.18 * jax.random.normal(seeds[20], (FD,), jnp.float32), 0.1, 1.9)
    dense_down_w = bell_draw(seeds[21], (FD, D), FD ** -0.5, 0.125, ((1, 32),))
    branch_logit = bell_draw(seeds[22], (D,), 1.5, 8.0, (), jnp.float32)
    return {"tokens": tokens, "cache_keys": cache_keys, "cache_values": cache_values, "cache_len": cache_len, "norm_gain_first": norm_gain_first, "w_query": w_query, "w_key": w_key, "w_value": w_value, "head_bias": head_bias, "w_output": w_output, "norm_gain_second": norm_gain_second, "group_id": group_id, "member": member, "group_gate": group_gate, "member_weight": member_weight, "expert_gate_w": expert_gate_w, "expert_up_w": expert_up_w, "expert_down_w": expert_down_w, "dense_gate_w": dense_gate_w, "dense_up_w": dense_up_w, "hidden_gain": hidden_gain, "dense_down_w": dense_down_w, "branch_logit": branch_logit}


epsilon = 1e-06
pair_block = 32

def rms_scale(values):
    return lax.rsqrt(lax.optimization_barrier(jnp.mean(values * values, axis=-1, keepdims=True)) + epsilon)

def stick_read(queries, key_cache, value_cache, lengths, head_bias):
    batch_size = queries.shape[0]
    span_len = key_cache.shape[1]
    group_size = HEADS // KV_HEADS
    query_heads = queries.reshape(batch_size, KV_HEADS, group_size, HEAD_DIM).astype(jnp.float32)
    key_heads = key_cache.reshape(batch_size, span_len, KV_HEADS, HEAD_DIM).astype(jnp.float32)
    value_heads = value_cache.reshape(batch_size, span_len, KV_HEADS, HEAD_DIM).astype(jnp.float32)
    scores = jnp.einsum('bkgd,bskd->bkgs', query_heads, key_heads) * HEAD_DIM ** (-0.5)
    scores = scores + head_bias.reshape(KV_HEADS, group_size)[None, :, :, None]
    live_mask = (jnp.arange(span_len, dtype=jnp.int32)[None, :] < lengths[:, None])[:, None, None, :]
    log_remain = jnp.where(live_mask, jax.nn.log_sigmoid(-scores), 0.0)
    remain_after = lax.cumsum(log_remain, axis=3, reverse=True) - log_remain
    weights = jnp.where(live_mask, jnp.exp(jax.nn.log_sigmoid(scores) + remain_after), 0.0).astype(jnp.bfloat16)
    mixed_heads = jnp.einsum('bkgs,bskd->bkgd', weights.astype(jnp.float32), value_heads)
    return mixed_heads.reshape(batch_size, HEADS * HEAD_DIM).astype(jnp.bfloat16)

def expert_apply(expert, pair_rows, expert_gate_w, expert_up_w, expert_down_w):
    gate_w = lax.dynamic_index_in_dim(expert_gate_w, expert, 0, keepdims=False)
    up_w = lax.dynamic_index_in_dim(expert_up_w, expert, 0, keepdims=False)
    down_w = lax.dynamic_index_in_dim(expert_down_w, expert, 0, keepdims=False)
    gate_pre = jnp.dot(pair_rows, gate_w, preferred_element_type=jnp.float32)
    upper_pre = jnp.dot(pair_rows, up_w, preferred_element_type=jnp.float32)
    hidden = (jax.nn.silu(gate_pre) * upper_pre).astype(jnp.bfloat16)
    return jnp.dot(hidden, down_w, preferred_element_type=jnp.float32).astype(jnp.bfloat16)

def reference(tokens, cache_keys, cache_values, cache_len, norm_gain_first, w_query, w_key, w_value, head_bias, w_output, norm_gain_second, group_id, member, group_gate, member_weight, expert_gate_w, expert_up_w, expert_down_w, dense_gate_w, dense_up_w, hidden_gain, dense_down_w, branch_logit):
    stream = tokens.astype(jnp.float32)
    normed_first = (stream * rms_scale(stream) * norm_gain_first).astype(jnp.bfloat16)
    queries = jnp.dot(normed_first, w_query, preferred_element_type=jnp.float32).astype(jnp.bfloat16)
    new_keys = jnp.dot(normed_first, w_key, preferred_element_type=jnp.float32).astype(jnp.bfloat16)
    new_values = jnp.dot(normed_first, w_value, preferred_element_type=jnp.float32).astype(jnp.bfloat16)

    def attend_block(block_args):
        block_queries, block_keys, block_values, block_lens = block_args
        return stick_read(block_queries, block_keys, block_values, block_lens, head_bias)
    attended = lax.map(attend_block, (queries.reshape(N_EP, SEQ_DEV, HEADS * HEAD_DIM), cache_keys.reshape(N_EP, SEQ_DEV, CACHE, KV_HEADS * HEAD_DIM), cache_values.reshape(N_EP, SEQ_DEV, CACHE, KV_HEADS * HEAD_DIM), cache_len.reshape(N_EP, SEQ_DEV))).reshape(TOKENS, HEADS * HEAD_DIM)
    projected = jnp.dot(attended, w_output, preferred_element_type=jnp.float32).astype(jnp.bfloat16)
    second_stream = stream + projected.astype(jnp.float32)
    normed_second = (second_stream * rms_scale(second_stream) * norm_gain_second).astype(jnp.bfloat16)
    pair_expert = (group_id[:, None] * PER_GROUP + member).reshape(-1).astype(jnp.int32)
    pair_total = pair_expert.shape[0]
    sort_order = jnp.argsort(pair_expert, stable=True).astype(jnp.int32)
    sorted_expert = pair_expert[sort_order]
    pair_rows = normed_second[sort_order // TOP_K]

    def run_block(block_index):
        block_rows = lax.dynamic_slice_in_dim(pair_rows, block_index * pair_block, pair_block, 0)
        block_expert = lax.dynamic_slice_in_dim(sorted_expert, block_index * pair_block, pair_block, 0)

        def visit(expert, accum):
            result_rows = expert_apply(expert, block_rows, expert_gate_w, expert_up_w, expert_down_w)
            return jnp.where((block_expert == expert)[:, None], result_rows.astype(jnp.float32), accum)
        return lax.fori_loop(block_expert[0], block_expert[pair_block - 1] + 1, visit, jnp.zeros((pair_block, D), jnp.float32))
    sorted_out = lax.map(run_block, jnp.arange(pair_total // pair_block, dtype=jnp.int32)).reshape(pair_total, D)
    expert_out = jnp.zeros((pair_total, D), jnp.float32).at[sort_order].set(sorted_out)
    combine = group_gate[:, None] * member_weight
    routed = lax.optimization_barrier(jnp.sum(expert_out.reshape(TOKENS, TOP_K, D) * combine[:, :, None], axis=1))
    dense_gate = jnp.dot(normed_second, dense_gate_w, preferred_element_type=jnp.float32)
    dense_upper = jnp.dot(normed_second, dense_up_w, preferred_element_type=jnp.float32)
    dense_hidden = jax.nn.silu(dense_gate) * dense_upper
    dense_normed = (dense_hidden * rms_scale(dense_hidden) * hidden_gain).astype(jnp.bfloat16)
    dense_out = jnp.dot(dense_normed, dense_down_w, preferred_element_type=jnp.float32).astype(jnp.bfloat16)
    mixed_out = second_stream + routed + jax.nn.sigmoid(branch_logit) * dense_out.astype(jnp.float32)
    return (mixed_out.astype(jnp.bfloat16), new_keys, new_values)
```

```python
import functools
import types

import jax
import jax.numpy as jnp
from jax import lax
from jax.experimental import pallas as pl
from jax.experimental.pallas import tpu as pltpu
from jax.sharding import PartitionSpec as P

HEADS = 32
HEAD_DIM = 64
KV_HEADS = 2
PER_GROUP = 16
TOP_K = 6
LANES = 128
MESH = pl.DeviceIdType.MESH

epsilon = 1e-06


def torus_of(chips):
    best = (chips, 1, 1)
    for x in range(1, chips + 1):
        for y in range(x, chips + 1):
            if chips % (x * y) == 0 and chips // (x * y) >= y:
                z = chips // (x * y)
                if z + y + x < sum(best):
                    best = (z, y, x)
    return best


def rms_scale(values):
    return lax.rsqrt(jnp.mean(values * values, axis=-1, keepdims=True) + epsilon)


class Place:
    def __init__(self, chips):
        self.chips = chips
        self.dims = torus_of(chips)
        me = lax.axis_index("ep")
        self.core = lax.rem(me, 2)
        self.chip = me // 2
        depth, height, width = self.dims
        self.x = lax.rem(self.chip, width)
        self.y = lax.rem(self.chip // width, height)
        self.z = self.chip // (width * height)

    def at(self, dz, dy, dx):
        depth, height, width = self.dims
        z = lax.rem(self.z + dz + depth, depth)
        y = lax.rem(self.y + dy + height, height)
        x = lax.rem(self.x + dx + width, width)
        return (z * height + y) * width + x

    def device(self, chip):
        return (chip * 2 + self.core,)

    def greet(self):
        barrier = pltpu.get_barrier_semaphore()
        for step in range(1, self.chips):
            other = lax.rem(self.chip + step, self.chips)
            pl.semaphore_signal(barrier, inc=1, device_id=self.device(other), device_id_type=MESH)
        pl.semaphore_wait(barrier, self.chips - 1)


def spread(place, halves):
    depth, height, width = place.dims
    sent = []
    counts = [0, 0]

    def push(half, source, origin, target):
        own, slots, send, recv = halves[half]
        copy = pltpu.make_async_remote_copy(
            src_ref=own if source is None else slots.at[source],
            dst_ref=slots.at[origin],
            send_sem=send.at[counts[half]],
            recv_sem=recv.at[origin],
            device_id=place.device(target),
            device_id_type=MESH,
        )
        counts[half] += 1
        copy.start()
        sent.append(copy)

    def arrive(half, origin):
        own, slots, send, recv = halves[half]
        pltpu.make_async_remote_copy(
            src_ref=slots.at[origin],
            dst_ref=slots.at[origin],
            send_sem=send.at[0],
            recv_sem=recv.at[origin],
            device_id=place.device(place.chip),
            device_id_type=MESH,
        ).wait_recv()

    def along(half, source, origin, axis):
        if axis == "x":
            for step in range(1, width):
                push(half, source, origin, place.at(0, 0, step))
        else:
            for step in range(1, height):
                push(half, source, origin, place.at(0, step, 0))

    orders = (("x", "y"), ("y", "x"))
    for step in range(1, depth):
        for half in range(2):
            push(half, None, place.chip, place.at(step, 0, 0))
    for half in range(2):
        for axis in orders[half]:
            along(half, None, place.chip, axis)
    for step in range(1, depth):
        for half in range(2):
            origin = place.at(-step, 0, 0)
            arrive(half, origin)
            for axis in orders[half]:
                along(half, origin, origin, axis)
    for up in range(depth):
        for half in range(2):
            reach = width if half == 0 else height
            for step in range(1, reach):
                origin = place.at(-up, 0, -step) if half == 0 else place.at(-up, -step, 0)
                arrive(half, origin)
                along(half, origin, origin, orders[half][1])
    for up in range(depth):
        for half in range(2):
            for dy in range(height):
                for dx in range(width):
                    if (dy if half == 0 else dx) != 0:
                        arrive(half, place.at(-up, -dy, -dx))
    for half in range(2):
        own, slots, _, _ = halves[half]
        slots[place.chip] = own[...]
    return sent


def deliver(place, tiles, landed, send, recv, out_ref):
    copies = []
    for step in range(1, place.chips):
        other = lax.rem(place.chip + step, place.chips)
        copy = pltpu.make_async_remote_copy(
            src_ref=tiles.at[other],
            dst_ref=landed.at[place.chip],
            send_sem=send.at[step],
            recv_sem=recv.at[place.chip],
            device_id=place.device(other),
            device_id_type=MESH,
        )
        copy.start()
        copies.append(copy)
    landed[place.chip] = tiles[place.chip]
    for step in range(1, place.chips):
        origin = lax.rem(place.chip - step + place.chips, place.chips)
        pltpu.make_async_remote_copy(
            src_ref=landed.at[origin],
            dst_ref=landed.at[origin],
            send_sem=send.at[0],
            recv_sem=recv.at[origin],
            device_id=place.device(place.chip),
            device_id_type=MESH,
        ).wait_recv()
    lanes = landed.shape[2]
    for block in range(place.chips):
        out_ref[:, block * lanes : (block + 1) * lanes] = landed[block]
    for copy in copies:
        copy.wait_send()


def flat(slots):
    count, rows, columns = slots.shape
    return slots[...].reshape(count * rows, columns)


def project_kernel(chips, a_ref, b_ref, w_ref, out_ref, slots_a, slots_b, tiles, landed,
                   send_a, recv_a, send_b, recv_b, send_t, recv_t):
    place = Place(chips)
    place.greet()
    sent = spread(place, ((a_ref, slots_a, send_a, recv_a), (b_ref, slots_b, send_b, recv_b)))
    cut = a_ref.shape[1]
    product = jnp.dot(flat(slots_a), w_ref[:cut], preferred_element_type=jnp.float32)
    product = product + jnp.dot(flat(slots_b), w_ref[cut:], preferred_element_type=jnp.float32)
    tiles[...] = product.astype(jnp.bfloat16).reshape(tiles.shape)
    deliver(place, tiles, landed, send_t, recv_t, out_ref)
    for copy in sent:
        copy.wait_send()


def gather_kernel(chips, a_ref, b_ref, gate_ref, up_ref, rows_ref, notes_ref, hidden_ref, slots_a, slots_b,
                  send_a, recv_a, send_b, recv_b):
    place = Place(chips)
    place.greet()
    sent = spread(place, ((a_ref, slots_a, send_a, recv_a), (b_ref, slots_b, send_b, recv_b)))
    cut = b_ref.shape[1]
    rows_a = slots_a[:, :, :cut].reshape(chips * a_ref.shape[0], cut)
    rows_b = flat(slots_b)
    rows_ref[:, :cut] = rows_a
    rows_ref[:, cut:] = rows_b
    notes_ref[...] = slots_a[:, :, cut:].reshape(notes_ref.shape)
    gate = jnp.dot(rows_a, gate_ref[:cut], preferred_element_type=jnp.float32)
    gate = gate + jnp.dot(rows_b, gate_ref[cut:], preferred_element_type=jnp.float32)
    upper = jnp.dot(rows_a, up_ref[:cut], preferred_element_type=jnp.float32)
    upper = upper + jnp.dot(rows_b, up_ref[cut:], preferred_element_type=jnp.float32)
    hidden_ref[...] = (jax.nn.silu(gate) * upper).astype(jnp.bfloat16)
    for copy in sent:
        copy.wait_send()


def down_kernel(chips, a_ref, b_ref, gain_ref, w_ref, out_ref, slots_a, slots_b, tiles, landed,
                send_a, recv_a, send_b, recv_b, send_t, recv_t):
    place = Place(chips)
    place.greet()
    sent = spread(place, ((a_ref, slots_a, send_a, recv_a), (b_ref, slots_b, send_b, recv_b)))
    rows, lanes = a_ref.shape
    part = chips // 2
    for half, slots in enumerate((slots_a, slots_b)):
        square = jnp.zeros((rows, lanes), jnp.float32)
        for block in range(chips):
            value = slots[block].astype(jnp.float32)
            square = square + value * value
        mean = jnp.sum(square, axis=1, keepdims=True) / (chips * lanes)
        scale = lax.rsqrt(mean + epsilon)
        total = jnp.zeros((rows, lanes), jnp.float32)
        for block in range(chips):
            gain = gain_ref[:, block * lanes : (block + 1) * lanes]
            normed = (slots[block].astype(jnp.float32) * scale * gain).astype(jnp.bfloat16)
            total = total + jnp.dot(
                normed,
                w_ref[block * lanes : (block + 1) * lanes],
                preferred_element_type=jnp.float32,
            )
        tiles[half * part : (half + 1) * part] = total.astype(jnp.bfloat16).reshape(
            part, rows // part, lanes
        )
    deliver(place, tiles, landed, send_t, recv_t, out_ref)
    for copy in sent:
        copy.wait_send()


def whole():
    return pl.BlockSpec(memory_space=pltpu.VMEM)


def spread_scratch(chips, a, b):
    slots = [pltpu.VMEM((chips,) + a.shape, a.dtype), pltpu.VMEM((chips,) + b.shape, b.dtype)]
    return slots, [pltpu.SemaphoreType.DMA((chips,))] * 4


def remote_params(number):
    return pltpu.CompilerParams(collective_id=number, has_side_effects=True)


def project(chips, number, rows, weight):
    count, width = rows.shape
    lanes = weight.shape[1]
    a, b = rows[:, : width // 2], rows[:, width // 2 :]
    slots, sems = spread_scratch(chips, a, b)
    tile = pltpu.VMEM((chips, count, lanes), jnp.bfloat16)
    return pl.pallas_call(
        functools.partial(project_kernel, chips),
        out_shape=jax.ShapeDtypeStruct((count, chips * lanes), jnp.bfloat16),
        in_specs=[whole()] * 3,
        out_specs=whole(),
        scratch_shapes=slots + [tile, tile] + sems + [pltpu.SemaphoreType.DMA((chips,))] * 2,
        compiler_params=remote_params(number),
        name="project",
    )(a, b, weight)


def gather_rows(chips, number, rows, notes, gate_w, up_w):
    count, width = rows.shape
    a = jnp.concatenate([rows[:, : width // 2], notes], axis=1)
    b = rows[:, width // 2 :]
    slots, sems = spread_scratch(chips, a, b)
    return pl.pallas_call(
        functools.partial(gather_kernel, chips),
        out_shape=(
            jax.ShapeDtypeStruct((chips * count, width), jnp.bfloat16),
            jax.ShapeDtypeStruct((chips * count, LANES), jnp.bfloat16),
            jax.ShapeDtypeStruct((chips * count, gate_w.shape[1]), jnp.bfloat16),
        ),
        in_specs=[whole()] * 4,
        out_specs=(whole(),) * 3,
        scratch_shapes=slots + sems,
        compiler_params=remote_params(number),
        name="gather_rows",
    )(a, b, gate_w, up_w)


def down_project(chips, number, hidden, gain, weight):
    count, lanes = hidden.shape
    a, b = hidden[: count // 2], hidden[count // 2 :]
    slots, sems = spread_scratch(chips, a, b)
    tile = pltpu.VMEM((chips, count // chips, lanes), jnp.bfloat16)
    return pl.pallas_call(
        functools.partial(down_kernel, chips),
        out_shape=jax.ShapeDtypeStruct((count // chips, chips * lanes), jnp.bfloat16),
        in_specs=[whole()] * 4,
        out_specs=whole(),
        scratch_shapes=slots + [tile, tile] + sems + [pltpu.SemaphoreType.DMA((chips,))] * 2,
        compiler_params=remote_params(number),
        name="down_project",
    )(a, b, gain[None, :], weight)


def stick_kernel(lens_ref, q_ref, k_ref, v_ref, bias_ref, out_ref):
    step = pl.program_id(0)
    batch, span, _ = k_ref.shape
    blocks = span // LANES
    row = lax.broadcasted_iota(jnp.int32, (3 * LANES, LANES), 0)
    column = lax.broadcasted_iota(jnp.int32, (3 * LANES, LANES), 1)
    after = (lax.rem(row, LANES) > column).astype(jnp.bfloat16)
    place = lax.broadcasted_iota(jnp.int32, (HEADS, span), 1)
    bias = bias_ref[:, :1]
    group = HEADS // KV_HEADS
    head = lax.broadcasted_iota(jnp.int32, (HEADS, LANES), 0)
    lane = lax.broadcasted_iota(jnp.int32, (HEADS, LANES), 1)
    own_lanes = (head // group) == (lane // HEAD_DIM)
    late = lax.broadcasted_iota(jnp.int32, (HEADS, HEAD_DIM), 0) >= group
    for item in range(batch):
        heads = q_ref[item].astype(jnp.float32)
        heads = jnp.where(own_lanes, jnp.concatenate([heads] * KV_HEADS, axis=1), 0.0)
        scores = lax.dot_general(
            heads.astype(jnp.bfloat16), k_ref[item], (((1,), (1,)), ((), ())), preferred_element_type=jnp.float32
        )
        scores = scores * HEAD_DIM ** (-0.5) + bias
        live = place < lens_ref[step * batch + item]
        remain = -(jnp.maximum(scores, 0.0) + jnp.log1p(jnp.exp(-jnp.abs(scores))))
        log_remain = jnp.where(live, remain, 0.0)
        stacked = jnp.concatenate(
            [log_remain[:, n * LANES : (n + 1) * LANES] for n in range(blocks)], axis=0
        )
        high = stacked.astype(jnp.bfloat16)
        rest = stacked - high.astype(jnp.float32)
        middle = rest.astype(jnp.bfloat16)
        low = (rest - middle.astype(jnp.float32)).astype(jnp.bfloat16)
        within = jnp.dot(
            jnp.concatenate([high, middle, low], axis=1), after, preferred_element_type=jnp.float32
        )
        totals = jnp.sum(stacked, axis=1, keepdims=True)
        carried = jnp.zeros((HEADS, 1), jnp.float32)
        pieces = [None] * blocks
        for n in range(blocks - 1, -1, -1):
            pieces[n] = within[n * HEADS : (n + 1) * HEADS] + carried
            carried = carried + totals[n * HEADS : (n + 1) * HEADS]
        remain_after = jnp.concatenate(pieces, axis=1)
        weights = jnp.where(live, jnp.exp(scores + remain + remain_after), 0.0)
        mixed = jnp.dot(
            weights.astype(jnp.bfloat16), v_ref[item], preferred_element_type=jnp.float32
        )
        mixed = jnp.where(late, mixed[:, HEAD_DIM:], mixed[:, :HEAD_DIM])
        out_ref[item] = mixed.astype(jnp.bfloat16)


def stick_read(queries, key_cache, value_cache, lengths, head_bias):
    batch, span, lanes = key_cache.shape
    heads = queries.reshape(batch, HEADS, HEAD_DIM)
    each = min(4, batch)
    mixed = pl.pallas_call(
        stick_kernel,
        out_shape=jax.ShapeDtypeStruct((batch, HEADS, HEAD_DIM), jnp.bfloat16),
        grid=(batch // each,),
        in_specs=[
            pl.BlockSpec(memory_space=pltpu.SMEM),
            pl.BlockSpec((each, HEADS, HEAD_DIM), lambda i: (i, 0, 0)),
            pl.BlockSpec((each, span, lanes), lambda i: (i, 0, 0)),
            pl.BlockSpec((each, span, lanes), lambda i: (i, 0, 0)),
            pl.BlockSpec((HEADS, LANES), lambda i: (0, 0)),
        ],
        out_specs=pl.BlockSpec((each, HEADS, HEAD_DIM), lambda i: (i, 0, 0)),
        name="stick_read",
    )(lengths, heads, key_cache, value_cache, jnp.broadcast_to(head_bias[:, None], (HEADS, LANES)))
    return mixed.reshape(batch, HEADS * HEAD_DIM)


def shards(
    tokens,
    cache_keys,
    cache_values,
    cache_len,
    norm_gain_first,
    w_query,
    w_key,
    w_value,
    head_bias,
    w_output,
    norm_gain_second,
    group_id,
    member,
    group_gate,
    member_weight,
    expert_gate_w,
    expert_up_w,
    expert_down_w,
    dense_gate_w,
    dense_up_w,
    hidden_gain,
    dense_down_w,
    branch_logit,
):
    devices = lax.axis_size("ep")
    chips = devices // 2
    me = lax.axis_index("ep")
    first = lax.rem(me, 2) == 0
    partner = [(i, i + 1 - 2 * (i % 2)) for i in range(devices)]
    seq_dev, width = tokens.shape

    def both(own):
        other = lax.ppermute(own, "ep", partner)
        return jnp.where(
            first, jnp.concatenate([own, other], axis=-1), jnp.concatenate([other, own], axis=-1)
        )

    query_w = both(w_query)
    output_w = both(w_output)
    gate_w = both(dense_gate_w)
    up_w = both(dense_up_w)
    down_w = both(dense_down_w)

    stream = tokens.astype(jnp.float32)
    normed_first = (stream * rms_scale(stream) * norm_gain_first).astype(jnp.bfloat16)
    new_keys = jnp.dot(normed_first, w_key, preferred_element_type=jnp.float32).astype(jnp.bfloat16)
    new_values = jnp.dot(normed_first, w_value, preferred_element_type=jnp.float32).astype(
        jnp.bfloat16
    )
    queries = project(chips, 1, normed_first, query_w)
    attended = stick_read(queries, cache_keys, cache_values, cache_len, head_bias)
    projected = project(chips, 2, attended, output_w)
    second_stream = stream + projected.astype(jnp.float32)
    normed_second = (second_stream * rms_scale(second_stream) * norm_gain_second).astype(
        jnp.bfloat16
    )

    experts = devices * expert_gate_w.shape[0]
    capacity = seq_dev // (experts // PER_GROUP)
    notes = jnp.concatenate(
        [member, group_id[:, None], jnp.zeros((seq_dev, LANES - TOP_K - 1), jnp.int32)], axis=1
    ).astype(jnp.bfloat16)
    own_rows, own_notes, hidden = gather_rows(chips, 3, normed_second, notes, gate_w, up_w)
    other_rows = lax.ppermute(own_rows, "ep", partner)
    other_notes = lax.ppermute(own_notes, "ep", partner)
    dense_out = down_project(chips, 4, hidden, hidden_gain, down_w)

    def selection(rows_notes, parity):
        table = rows_notes[:, : TOP_K + 1].astype(jnp.int32)
        named = table[:, TOP_K :] * PER_GROUP + table[:, :TOP_K]
        hits = jnp.any(named == me, axis=1).reshape(chips, seq_dev)
        index = jnp.arange(seq_dev)
        earlier = (index[:, None] < index[None, :]).astype(jnp.float32)
        slot = jnp.dot(hits.astype(jnp.float32), earlier).astype(jnp.int32)
        spot = ((jnp.arange(chips)[:, None] * 2 + parity) * capacity + slot).reshape(-1)
        spot = jnp.where(hits.reshape(-1), spot, -1)
        return (jnp.arange(devices * capacity)[:, None] == spot[None, :]).astype(jnp.bfloat16)

    parity = lax.rem(me, 2)
    packed = jnp.dot(selection(own_notes, parity), own_rows, preferred_element_type=jnp.float32)
    packed = packed + jnp.dot(
        selection(other_notes, 1 - parity), other_rows, preferred_element_type=jnp.float32
    )
    packed = packed.astype(jnp.bfloat16)
    gate_pre = jnp.dot(packed, expert_gate_w[0], preferred_element_type=jnp.float32)
    upper_pre = jnp.dot(packed, expert_up_w[0], preferred_element_type=jnp.float32)
    expert_hidden = (jax.nn.silu(gate_pre) * upper_pre).astype(jnp.bfloat16)
    served = jnp.dot(expert_hidden, expert_down_w[0], preferred_element_type=jnp.float32).astype(
        jnp.bfloat16
    )
    returned = lax.all_to_all(
        served.reshape(devices, capacity, width), "ep", split_axis=0, concat_axis=0, tiled=True
    ).reshape(experts * capacity, width)

    pair_expert = (group_id[:, None] * PER_GROUP + member).reshape(-1)
    pair_count = pair_expert.shape[0]
    expert_hits = (pair_expert[:, None] == jnp.arange(experts, dtype=jnp.int32)[None, :]).astype(
        jnp.float32
    )
    earlier = (jnp.arange(pair_count)[:, None] > jnp.arange(pair_count)[None, :]).astype(
        jnp.float32
    )
    before = jnp.dot(earlier, expert_hits, preferred_element_type=jnp.float32)
    slot_index = jnp.sum(before * expert_hits, axis=1).astype(jnp.int32)
    target = pair_expert * capacity + slot_index
    select = (target[:, None] == jnp.arange(experts * capacity, dtype=jnp.int32)[None, :]).astype(
        jnp.bfloat16
    )
    pair_out = jnp.dot(select, returned, preferred_element_type=jnp.float32)
    combine = (group_gate[:, None] * member_weight).reshape(-1, 1)
    routed = jnp.sum((pair_out * combine).reshape(seq_dev, TOP_K, width), axis=1)
    mixed_out = (
        second_stream + routed + jax.nn.sigmoid(branch_logit) * dense_out.astype(jnp.float32)
    )
    return (mixed_out.astype(jnp.bfloat16), new_keys, new_values)


LOG2E = 1.4426950408889634
DEAD = -1e30
TRANSPOSED = (((1,), (1,)), ((), ()))


def dot_t(a, b):
    return lax.dot_general(a, b, TRANSPOSED, preferred_element_type=jnp.float32)


def dot(a, b):
    return jnp.dot(a, b, preferred_element_type=jnp.float32)


def remote(src, dst, send, recv, device):
    return pltpu.make_async_remote_copy(
        src_ref=src, dst_ref=dst, send_sem=send, recv_sem=recv, device_id=device, device_id_type=MESH
    )


class Grid(Place):
    def __init__(self, chips):
        super().__init__(chips)
        self.partner = (self.chip * 2 + 1 - self.core,)
        self.depth = self.dims[0]
        self.plane = chips // self.depth

    def on(self, z, dy=0, dx=0):
        depth, height, width = self.dims
        y = lax.rem(self.y + dy, height)
        x = lax.rem(self.x + dx, width)
        return (z * height + y) * width + x

    def turn(self, axis):
        return (1, 0) if axis == "y" else (0, 1)

    def sweep(self, step):
        toward = 1 - 2 * (self.z // (self.depth // 2))
        return lax.rem(self.z + step * toward + self.depth, self.depth)

    def enter(self):
        barrier = pltpu.get_barrier_semaphore()
        for step in range(1, self.chips):
            other = lax.rem(self.chip + step, self.chips)
            pl.semaphore_signal(barrier, inc=1, device_id=self.device(other), device_id_type=MESH)
        pl.semaphore_signal(barrier, inc=1, device_id=self.partner, device_id_type=MESH)
        pl.semaphore_wait(barrier, self.chips)


class Gather:
    def __init__(self, place, pieces):
        self.place = place
        self.pieces = pieces

    def copy(self, piece, kind, origin, target):
        view, send, recv, _ = self.pieces[piece]
        z = origin // self.place.plane
        return remote(view(origin), view(origin), send.at[kind * self.place.depth + z], recv.at[origin],
                      self.place.device(target))

    def arrive(self, piece, origin):
        self.copy(piece, 0, origin, self.place.chip).wait_recv()

    def turns(self, piece):
        first, second = self.pieces[piece][3]
        return self.place.turn(first), self.place.turn(second)

    def across(self, piece, z):
        place = self.place
        first, second = self.turns(piece)
        self.copy(piece, 2, place.on(z), place.on(place.z, *first)).start()
        self.copy(piece, 3, place.on(z), place.on(place.z, *second)).start()

    def corner(self, piece, z):
        place = self.place
        first, second = self.turns(piece)
        origin = place.on(z, *first)
        self.arrive(piece, origin)
        self.copy(piece, 4, origin, place.on(place.z, *second)).start()

    def start(self):
        place, z, depth = self.place, self.place.z, self.place.depth
        every = range(len(self.pieces))

        @pl.when(z < depth - 1)
        def _():
            for piece in every:
                self.copy(piece, 0, place.chip, place.on(z + 1)).start()

        @pl.when(z > 0)
        def _():
            for piece in every:
                self.copy(piece, 1, place.chip, place.on(z - 1)).start()

        for piece in every:
            self.across(piece, z)

    def relay(self):
        place, z, depth = self.place, self.place.z, self.place.depth
        every = range(len(self.pieces))
        for piece in every:
            self.corner(piece, z)
        for step in range(1, depth):

            @pl.when(z >= step)
            def _():
                for piece in every:
                    self.arrive(piece, place.on(z - step))

                    @pl.when(z < depth - 1)
                    def _():
                        self.copy(piece, 0, place.on(z - step), place.on(z + 1)).start()

                    self.across(piece, z - step)

            @pl.when(z + step < depth)
            def _():
                for piece in every:
                    self.arrive(piece, place.on(z + step))

                    @pl.when(z > 0)
                    def _():
                        self.copy(piece, 1, place.on(z + step), place.on(z - 1)).start()

                    self.across(piece, z + step)

            @pl.when(z >= step)
            def _():
                for piece in every:
                    self.corner(piece, z - step)

            @pl.when(z + step < depth)
            def _():
                for piece in every:
                    self.corner(piece, z + step)

    def rest(self, piece, z):
        first, second = self.turns(piece)
        self.arrive(piece, self.place.on(z, *second))
        self.arrive(piece, self.place.on(z, 1, 1))

    def finish(self):
        place, depth = self.place, self.place.depth
        for piece in range(len(self.pieces)):
            for z in range(depth):
                for kind in (2, 3, 4):
                    self.copy(piece, kind, place.on(z), place.chip).wait_send()

                @pl.when((place.z >= z) & (place.z < depth - 1))
                def _():
                    self.copy(piece, 0, place.on(z), place.chip).wait_send()

                @pl.when((place.z <= z) & (place.z > 0))
                def _():
                    self.copy(piece, 1, place.on(z), place.chip).wait_send()


def norm_rows(values, gain):
    square = jnp.mean(values * values, axis=-1, keepdims=True)
    return (values * lax.rsqrt(square + epsilon) * gain).astype(jnp.bfloat16)


ORDERS = (("x", "y"), ("y", "x"))


def layer_kernel(
    chips, names,
    lens_ref, bias_ref, tokens_ref, gain1_ref, gain2_ref, hgain_ref, logit_ref,
    member_ref, mweight_ref, group_ref, ggate_ref,
    keys_hbm, values_hbm, wq_hbm, wo_hbm, wg_hbm, wu_hbm, wd_hbm, wk_hbm, wv_hbm, eg_hbm, eu_hbm, ed_hbm,
    out_ref, newk_ref, newv_ref,
    *scratch,
):
    s = types.SimpleNamespace(**dict(zip(names, scratch)))
    place = Grid(chips)
    me = place.chip * 2 + place.core
    chip, z, depth, plane = place.chip, place.z, place.depth, place.plane
    seq, width = tokens_ref.shape
    half = width // 2
    rows = chips * seq
    lanes = LANES
    experts = chips * 2
    part = plane * seq
    bf16 = jnp.bfloat16

    own_rows = pl.ds(pl.multiple_of(place.core * 64, 64), 64)
    weights = ((s.wq, wq_hbm), (s.wo, wo_hbm), (s.wg, wg_hbm), (s.wu, wu_hbm))
    local = types.SimpleNamespace()

    def fetch(src, dst, index):
        copy = pltpu.make_async_copy(src, dst, s.local_sem.at[index])
        copy.start()
        return copy

    local.wq, local.wo, local.wg, local.wu = (
        fetch(src, dst.at[own_rows], i) for i, (dst, src) in enumerate(weights)
    )
    local.wk = fetch(wk_hbm, s.wk, 4)
    local.wv = fetch(wv_hbm, s.wv, 5)
    local.keys = fetch(keys_hbm, s.keys, 6)
    local.values = fetch(values_hbm, s.values, 7)
    local.eg = fetch(eg_hbm.at[0], s.eg, 8)
    local.eu = fetch(eu_hbm.at[0], s.eu, 9)
    local.ed = fetch(ed_hbm.at[0], s.ed, 10)

    place_of = lax.broadcasted_iota(jnp.int32, (lanes, seq), 0)
    expert = lax.rem(place_of, experts)
    combine = jnp.zeros((lanes, seq), jnp.float32)
    for k in range(TOP_K):
        named = group_ref[...] * PER_GROUP + member_ref[k : k + 1, :]
        weight = ggate_ref[...] * mweight_ref[k : k + 1, :]
        combine = jnp.where(expert == named, weight, combine)
    high = combine.astype(bf16).astype(jnp.float32)
    notes = jnp.where(place_of < experts, high, jnp.where(place_of < 2 * experts, combine - high, 0.0))
    diagonal = lax.broadcasted_iota(jnp.int32, (seq, seq), 0) == lax.broadcasted_iota(jnp.int32, (seq, seq), 1)
    notes = dot_t(jnp.where(diagonal, 1.0, 0.0).astype(bf16), notes.astype(bf16))
    slots1, slots2, slots3 = s.slots1, s.slots2, s.slots3
    slots1[chip, :, :lanes] = notes.astype(bf16)
    slots1[chip, :, lanes:] = tokens_ref[...]

    place.enter()

    cut = lanes + half
    gather1 = Gather(place, (
        (lambda o: slots1.at[o, :, pl.ds(0, cut)], s.send1a, s.recv1a, ORDERS[0]),
        (lambda o: slots1.at[o, :, pl.ds(cut, half)], s.send1b, s.recv1b, ORDERS[1]),
    ))
    gather1.start()
    swaps = [
        remote(src, dst.at[own_rows], s.swap_send.at[i], s.swap_recv.at[i], place.partner)
        for i, (dst, src) in enumerate(weights)
    ]
    for swap in swaps:
        swap.start()
    gather1.relay()
    local.wq.wait()
    swaps[0].wait_recv()

    tiles, landed = s.tiles, s.landed

    def tile_copy(index, target):
        return remote(tiles.at[target], landed.at[chip], s.tile_send.at[index], s.tile_recv.at[chip],
                      place.device(target))

    for step in range(depth):
        zo = place.sweep(step)
        for piece in range(2):
            gather1.rest(piece, zo)
        at = pl.ds(zo * plane, plane)
        rows_f = slots1[at, :, lanes:].reshape(part, width).astype(jnp.float32)
        product = dot_t(norm_rows(rows_f, gain1_ref[...]), s.wq[...])
        tiles[at] = product.astype(bf16).reshape(plane, seq, lanes)
        for dy in (1, 0):
            for dx in (1, 0):
                target = place.on(zo, dy, dx)
                if (step, dy, dx) == (0, 0, 0):
                    landed[chip] = tiles[chip]
                else:
                    tile_copy(step * plane + dy * 2 + dx, target).start()

    own_normed = norm_rows(tokens_ref[...].astype(jnp.float32), gain1_ref[...])
    local.wk.wait()
    local.wv.wait()
    newk_ref[...] = dot(own_normed, s.wk[...]).astype(bf16)
    newv_ref[...] = dot(own_normed, s.wv[...]).astype(bf16)

    for step in range(1, chips):
        origin = lax.rem(chip + step, chips)
        remote(tiles.at[origin], landed.at[origin], s.tile_send.at[0], s.tile_recv.at[origin],
               place.device(chip)).wait_recv()

    def down_copy(target):
        columns = pl.ds(pl.multiple_of(target * lanes, lanes), lanes)
        return remote(wd_hbm.at[:, columns], s.wd.at[chip, place.core], s.down_send.at[target],
                      s.down_recv.at[chip], place.device(target))

    for step in range(1, chips):
        down_copy(lax.rem(chip + step, chips)).start()
    local.wd = fetch(wd_hbm.at[:, pl.ds(pl.multiple_of(chip * lanes, lanes), lanes)], s.wd.at[chip, place.core], 11)

    heads, mixed = s.heads, s.mixed
    for j in range(chips):
        heads[:, j, :] = landed[j].astype(jnp.float32)
    local.keys.wait()
    local.values.wait()
    span = s.keys.shape[1]
    blocks = span // LANES
    row = lax.broadcasted_iota(jnp.int32, (2 * LANES, 2 * LANES), 0)
    column = lax.broadcasted_iota(jnp.int32, (2 * LANES, 2 * LANES), 1)
    after = ((lax.rem(row, LANES) > column) | (column >= LANES)).astype(bf16)
    position = lax.broadcasted_iota(jnp.int32, (HEADS, span), 1)
    jrow = lax.broadcasted_iota(jnp.int32, (chips, LANES), 0)
    jlane = lax.broadcasted_iota(jnp.int32, (chips, LANES), 1)
    early = jrow < chips // KV_HEADS
    own = (jlane // HEAD_DIM) == (jrow // (chips // KV_HEADS))
    head_row = lax.broadcasted_iota(jnp.int32, (HEADS, LANES), 0)
    bias = jnp.zeros((HEADS, LANES), jnp.float32)
    for head in range(HEADS):
        bias = jnp.where(head_row == (head % 2) * chips + head // 2, bias_ref[head] * LOG2E, bias)
    bias = jnp.concatenate([bias] * blocks, axis=1)

    def attend(item):
        even = heads[item]
        turned = pltpu.roll(even, HEAD_DIM, axis=1)
        query = jnp.concatenate([
            jnp.where(own, jnp.where(early, even, turned), 0.0),
            jnp.where(own, jnp.where(early, turned, even), 0.0),
        ], axis=0).astype(bf16)
        scores = dot_t(query, s.keys[item]) * (HEAD_DIM ** (-0.5) * LOG2E) + bias
        scores = jnp.where(position < lens_ref[item], scores, DEAD)
        soft = jnp.maximum(scores, 0.0) + jnp.log(1.0 + jnp.exp2(-jnp.abs(scores))) * LOG2E
        stacked = jnp.concatenate([soft[:, n * LANES : (n + 1) * LANES] for n in range(blocks)], axis=0)
        top = stacked.astype(bf16)
        low = (stacked - top.astype(jnp.float32)).astype(bf16)
        sums = dot(jnp.concatenate([top, low], axis=1), after)
        sums = sums
        carried = jnp.zeros((HEADS, LANES), jnp.float32)
        pieces = [None] * blocks
        for n in range(blocks - 1, -1, -1):
            band = sums[n * HEADS : (n + 1) * HEADS]
            spent = stacked[n * HEADS : (n + 1) * HEADS] + band[:, :LANES] + carried
            pieces[n] = jnp.exp2(scores[:, n * LANES : (n + 1) * LANES] - spent).astype(bf16)
            carried = carried + band[:, LANES:]
        found = dot(jnp.concatenate(pieces, axis=1), s.values[item])
        first, second = found[:chips], found[chips:]
        mixed[item] = jnp.where(
            jlane < HEAD_DIM,
            jnp.where(early, first, pltpu.roll(first, HEAD_DIM, axis=1)),
            jnp.where(early, pltpu.roll(second, HEAD_DIM, axis=1), second),
        )

    together = 4 if seq % 4 == 0 else 1

    @pl.loop(0, seq // together)
    def _(index):
        for t in range(together):
            attend(index * together + t)

    for j in range(chips):
        slots2[chip, :, j * LANES : (j + 1) * LANES] = mixed[:, j, :].astype(bf16)

    gather2 = Gather(place, (
        (lambda o: slots2.at[o, :, pl.ds(0, half)], s.send2a, s.recv2a, ORDERS[0]),
        (lambda o: slots2.at[o, :, pl.ds(half, half)], s.send2b, s.recv2b, ORDERS[1]),
    ))
    gather2.start()
    gather2.relay()
    local.wo.wait()
    swaps[1].wait_recv()
    for step in range(depth):
        zo = place.sweep(step)
        for piece in range(2):
            gather2.rest(piece, zo)
        product = dot_t(slots2[pl.ds(zo * plane, plane)].reshape(part, width), s.wo[...])
        slots3[chip, pl.ds(pl.multiple_of(zo * part, part), part), :] = product.astype(bf16)

    gather3 = Gather(place, (
        (lambda o: slots3.at[o, pl.ds(0, rows // 2), :], s.send3a, s.recv3a, ORDERS[0]),
        (lambda o: slots3.at[o, pl.ds(rows // 2, rows // 2), :], s.send3b, s.recv3b, ORDERS[1]),
    ))
    gather3.start()
    gather3.relay()
    local.wd.wait()
    for step in range(1, chips):
        origin = lax.rem(chip + step, chips)
        remote(s.wd.at[origin, place.core], s.wd.at[origin, place.core], s.down_send.at[0],
               s.down_recv.at[origin], place.device(chip)).wait_recv()
    down_swap = remote(s.wd.at[:, place.core], s.wd.at[:, place.core], s.swap_send.at[4],
                       s.swap_recv.at[4], place.partner)
    down_swap.start()
    for step in range(depth):
        for piece in range(2):
            gather3.rest(piece, place.sweep(step))

    rows_own, rows_other = s.rows_own, s.rows_other
    row_copies = []
    for block in range(depth):
        at = slice(block * part, (block + 1) * part)
        token = slots1[block * plane : (block + 1) * plane, :, lanes:].reshape(part, width).astype(jnp.float32)
        projected = jnp.concatenate([slots3[c, at, :] for c in range(chips)], axis=1).astype(jnp.float32)
        rows_own[at, :width] = norm_rows(token + projected, gain2_ref[...])
        rows_own[at, width:] = slots1[block * plane : (block + 1) * plane, :, :lanes].reshape(part, lanes)
        row_copies.append(remote(rows_own.at[at], rows_other.at[at], s.row_send.at[block],
                                 s.row_recv.at[block], place.partner))
        row_copies[-1].start()

    local.wg.wait()
    local.wu.wait()
    swaps[2].wait_recv()
    swaps[3].wait_recv()
    normed = rows_own[:, :width]
    gate = dot_t(normed, s.wg[...])
    hidden = jax.nn.silu(gate) * dot_t(normed, s.wu[...])
    s.hidden[...] = hidden
    squares = jnp.broadcast_to(jnp.sum(hidden * hidden, axis=1, keepdims=True), (rows, LANES))
    s.squares[chip] = jnp.transpose(squares)[:1]

    def square_copy(target):
        return remote(s.squares.at[chip], s.squares.at[chip], s.square_send.at[target],
                      s.square_recv.at[chip], place.device(target))

    for step in range(1, chips):
        square_copy(lax.rem(chip + step, chips)).start()

    local.eg.wait()
    local.eu.wait()

    def expert_hidden(ref):
        gate_pre = dot(ref[:, :width], s.eg[...])
        return (jax.nn.silu(gate_pre) * dot(ref[:, :width], s.eu[...])).astype(bf16)

    note_lane = lax.broadcasted_iota(jnp.int32, (rows, LANES), 1)
    mine = (note_lane == me) | (note_lane == me + experts)

    def weight_of(ref):
        return jnp.sum(jnp.where(mine, ref[:, width:].astype(jnp.float32), 0.0), axis=1, keepdims=True)

    s.hid_own[...] = expert_hidden(rows_own)
    for copy in row_copies:
        copy.wait_recv()
    s.hid_other[...] = expert_hidden(rows_other)
    local.ed.wait()
    chunk = width // 4
    weight_other = weight_of(rows_other)
    gift_copies = []
    for c in range(4):
        at = slice(c * chunk, (c + 1) * chunk)
        served = dot(s.hid_other[...], s.ed[:, at])
        s.gift[c] = jnp.where(weight_other != 0.0, served * weight_other, 0.0).astype(bf16)
        gift_copies.append(remote(s.gift.at[c], s.given.at[c], s.gift_send.at[c],
                                  s.gift_recv.at[c], place.partner))
        gift_copies[-1].start()

    for step in range(1, chips):
        origin = lax.rem(chip + step, chips)
        remote(s.squares.at[origin], s.squares.at[origin], s.square_send.at[0],
               s.square_recv.at[origin], place.device(chip)).wait_recv()
    total = s.squares[0]
    for c in range(1, chips):
        total = total + s.squares[c]
    scale = lax.rsqrt(total / width + epsilon)
    scale = jnp.transpose(jnp.broadcast_to(scale, (LANES, rows)))
    gain = hgain_ref[:, pl.ds(pl.multiple_of(chip * lanes, lanes), lanes)]
    dense = (s.hidden[...] * scale * gain).astype(bf16)
    down_swap.wait_recv()
    weight_own = weight_of(rows_own)
    acc = s.acc

    def first_index(zo, beside):
        return zo * 2 + beside

    def columns_of(piece):
        return slice(piece * half, (piece + 1) * half)

    def staged(piece, value, slot, dst, index, recv, target):
        stage = s.stage
        stage[piece, slot] = value.astype(bf16)
        remote(stage.at[piece, slot], dst, s.sum_send.at[piece, index], recv, place.device(target)).start()

    def first_dst(piece, zo, beside):
        return s.sum1.at[piece, first_index(zo, beside)], s.sum1_recv.at[piece, first_index(zo, beside)]

    def send_first(piece, step, beside):
        first, second = (place.turn(a) for a in ORDERS[piece])
        zo = place.sweep(step)
        turn = (1, 1) if beside else first
        dst, recv = first_dst(piece, zo, beside)
        slot = step * 2 + beside
        staged(piece, acc[place.on(zo, *turn), :, columns_of(piece)], slot, dst, slot, recv, place.on(z, *first))

    def wait_into(ref, recv):
        remote(ref, ref, s.sum_send.at[0, 0], recv, place.device(chip)).wait_recv()
        return ref[...].astype(jnp.float32)

    for piece in range(2):
        for c in (2 * piece, 2 * piece + 1):
            at = slice(c * chunk, (c + 1) * chunk)
            served = dot(s.hid_own[...], s.ed[:, at])
            value = jnp.where(weight_own != 0.0, served * weight_own, 0.0)
            down = s.wd[c * (chips // 4) : (c + 1) * (chips // 4)].reshape(chunk, LANES)
            value = value + jax.nn.sigmoid(logit_ref[:, at]) * dot_t(dense, down)
            gift_copies[c].wait_recv()
            value = value + s.given[c].astype(jnp.float32)
            acc[:, :, at] = value.reshape(chips, seq, chunk)
        for beside in (1, 0):
            for step in range(depth - 1, -1, -1):
                send_first(piece, step, beside)

    base = 2 * depth
    for step in range(depth - 1, -1, -1):
        for piece in range(2):
            first, second = (place.turn(a) for a in ORDERS[piece])
            zo = place.sweep(step)
            value = acc[place.on(zo, *second), :, columns_of(piece)] + wait_into(*first_dst(piece, zo, 1))
            staged(piece, value, base + step, s.sum2.at[piece, zo], base + step,
                   s.sum2_recv.at[piece, zo], place.on(z, *second))

    def folded(piece, zo):
        value = acc[place.on(zo), :, columns_of(piece)] + wait_into(*first_dst(piece, zo, 0))
        return value + wait_into(s.sum2.at[piece, zo], s.sum2_recv.at[piece, zo])

    base = 3 * depth

    def along(piece, step, up):
        zo = z + step if up else z - step
        line, recv = (s.sum_up, s.sum_up_recv) if up else (s.sum_down, s.sum_down_recv)
        acc[place.on(zo), :, columns_of(piece)] = folded(piece, zo)

        @pl.when((z > 0) if up else (z < depth - 1))
        def _():
            acc[place.on(zo), :, columns_of(piece)] += wait_into(line.at[piece, zo], recv.at[piece, zo])

        slot = base + zo
        staged(piece, acc[place.on(zo), :, columns_of(piece)], slot, line.at[piece, zo], slot,
               recv.at[piece, zo], place.on(z + 1 if up else z - 1))

    for step in range(depth - 1, 0, -1):

        @pl.when(z + step < depth)
        def _():
            for piece in range(2):
                along(piece, step, True)

        @pl.when(z >= step)
        def _():
            for piece in range(2):
                along(piece, step, False)

    own_at = pl.ds(pl.multiple_of(chip * seq, seq), seq)
    for piece in range(2):
        at = columns_of(piece)
        value = tokens_ref[:, at].astype(jnp.float32)
        value = value + jnp.concatenate(
            [slots3[c, own_at, :] for c in range(piece * chips // 2, (piece + 1) * chips // 2)], axis=1
        ).astype(jnp.float32)
        acc[chip, :, at] = value + folded(piece, z)
    for piece in range(2):

        @pl.when(z > 0)
        def _():
            acc[chip, :, columns_of(piece)] += wait_into(s.sum_up.at[piece, z], s.sum_up_recv.at[piece, z])

        @pl.when(z < depth - 1)
        def _():
            acc[chip, :, columns_of(piece)] += wait_into(s.sum_down.at[piece, z], s.sum_down_recv.at[piece, z])

        out_ref[:, columns_of(piece)] = acc[chip, :, columns_of(piece)].astype(bf16)

    for gather in (gather1, gather2, gather3):
        gather.finish()
    for step in range(1, chips):
        tile_copy(step, lax.rem(chip + 1, chips)).wait_send()
        target = lax.rem(chip + step, chips)
        down_copy(target).wait_send()
        square_copy(target).wait_send()
    for copy in swaps + [down_swap] + row_copies + gift_copies:
        copy.wait_send()

    def sum_sent(piece, slot):
        remote(s.stage.at[piece, slot], s.stage.at[piece, slot], s.sum_send.at[piece, slot],
               s.sum1_recv.at[0, 0], place.device(chip)).wait_send()

    for piece in range(2):
        for slot in range(3 * depth):
            sum_sent(piece, slot)
        for zo in range(depth):

            @pl.when(z != zo)
            def _():
                sum_sent(piece, 3 * depth + zo)


def copy_kernel(a_ref, b_ref, c_ref, a_out, b_out, c_out):
    a_out[...] = a_ref[...]
    b_out[...] = b_ref[...]
    c_out[...] = c_ref[...]


def layer_scratch(chips, depth, seq, width, span, fe):
    rows = chips * seq
    bf16, f32, DMA = jnp.bfloat16, jnp.float32, pltpu.SemaphoreType.DMA
    half = width // 2
    return dict(
        slots1=pltpu.VMEM((chips, seq, LANES + width), bf16),
        slots2=pltpu.VMEM((chips, seq, width), bf16),
        slots3=pltpu.VMEM((chips, rows, LANES), bf16),
        keys=pltpu.VMEM((seq, span, LANES), bf16),
        values=pltpu.VMEM((seq, span, LANES), bf16),
        wk=pltpu.VMEM((width, LANES), bf16),
        wv=pltpu.VMEM((width, LANES), bf16),
        eg=pltpu.VMEM((width, fe), bf16),
        eu=pltpu.VMEM((width, fe), bf16),
        ed=pltpu.VMEM((fe, width), bf16),
        wd=pltpu.VMEM((chips, 2, LANES // 2, LANES), bf16),
        tiles=pltpu.VMEM((chips, seq, LANES), bf16),
        landed=pltpu.VMEM((chips, seq, LANES), bf16),
        heads=pltpu.VMEM((seq, chips, LANES), f32),
        mixed=pltpu.VMEM((seq, chips, LANES), f32),
        rows_own=pltpu.VMEM((rows, width + LANES), bf16),
        rows_other=pltpu.VMEM((rows, width + LANES), bf16),
        hidden=pltpu.VMEM((rows, LANES), f32),
        squares=pltpu.VMEM((chips, 1, rows), f32),
        hid_own=pltpu.VMEM((rows, fe), bf16),
        hid_other=pltpu.VMEM((rows, fe), bf16),
        gift=pltpu.VMEM((4, rows, width // 4), bf16),
        given=pltpu.VMEM((4, rows, width // 4), bf16),
        acc=pltpu.VMEM((chips, seq, width), f32),
        stage=pltpu.VMEM((2, 4 * depth, seq, half), bf16),
        sum1=pltpu.VMEM((2, 2 * depth, seq, half), bf16),
        sum2=pltpu.VMEM((2, depth, seq, half), bf16),
        sum_up=pltpu.VMEM((2, depth, seq, half), bf16),
        sum_down=pltpu.VMEM((2, depth, seq, half), bf16),
        local_sem=DMA((12,)),
        swap_send=DMA((5,)),
        swap_recv=DMA((5,)),
        tile_send=DMA((chips,)),
        tile_recv=DMA((chips,)),
        down_send=DMA((chips,)),
        down_recv=DMA((chips,)),
        square_send=DMA((chips,)),
        square_recv=DMA((chips,)),
        row_send=DMA((depth,)),
        row_recv=DMA((depth,)),
        gift_send=DMA((4,)),
        gift_recv=DMA((4,)),
        sum_send=DMA((2, 4 * depth)),
        sum1_recv=DMA((2, 2 * depth)),
        sum2_recv=DMA((2, depth)),
        sum_up_recv=DMA((2, depth)),
        sum_down_recv=DMA((2, depth)),
        wq=pltpu.VMEM((LANES, width), bf16),
        wo=pltpu.VMEM((LANES, width), bf16),
        wg=pltpu.VMEM((LANES, width), bf16),
        wu=pltpu.VMEM((LANES, width), bf16),
        send1a=DMA((5 * depth,)),
        recv1a=DMA((chips,)),
        send1b=DMA((5 * depth,)),
        recv1b=DMA((chips,)),
        send2a=DMA((5 * depth,)),
        recv2a=DMA((chips,)),
        send2b=DMA((5 * depth,)),
        recv2b=DMA((chips,)),
        send3a=DMA((5 * depth,)),
        recv3a=DMA((chips,)),
        send3b=DMA((5 * depth,)),
        recv3b=DMA((chips,)),
    )


def fused_shards(
    tokens, cache_keys, cache_values, cache_len, norm_gain_first, w_query, w_key, w_value, head_bias,
    w_output, norm_gain_second, group_id, member, group_gate, member_weight, expert_gate_w,
    expert_up_w, expert_down_w, dense_gate_w, dense_up_w, hidden_gain, dense_down_w, branch_logit,
):
    chips = lax.axis_size("ep") // 2
    seq, width = tokens.shape
    span = cache_keys.shape[1]
    bf16 = jnp.bfloat16
    scratch = layer_scratch(chips, torus_of(chips)[0], seq, width, span, expert_gate_w.shape[2])
    smem = pl.BlockSpec(memory_space=pltpu.SMEM)
    anywhere = pl.BlockSpec(memory_space=pl.ANY)
    out_shape = (
        jax.ShapeDtypeStruct((seq, width), bf16),
        jax.ShapeDtypeStruct((seq, LANES), bf16),
        jax.ShapeDtypeStruct((seq, LANES), bf16),
    )
    results = pl.pallas_call(
        functools.partial(layer_kernel, chips, tuple(scratch)),
        out_shape=out_shape,
        in_specs=[smem] * 2 + [whole()] * 9 + [anywhere] * 12,
        out_specs=(whole(),) * 3,
        scratch_shapes=list(scratch.values()),
        compiler_params=pltpu.CompilerParams(
            collective_id=1, has_side_effects=True, vmem_limit_bytes=60 * 1024 * 1024
        ),
        name="layer",
    )(
        cache_len, head_bias, tokens, norm_gain_first[None], norm_gain_second[None], hidden_gain[None],
        branch_logit[None], member.T, member_weight.T, group_id[None], group_gate[None],
        cache_keys, cache_values, w_query.T, w_output.T, dense_gate_w.T, dense_up_w.T, dense_down_w.T,
        w_key, w_value, expert_gate_w, expert_up_w, expert_down_w,
    )
    return pl.pallas_call(
        copy_kernel, out_shape=out_shape, in_specs=[whole()] * 3, out_specs=(whole(),) * 3, name="results"
    )(*results)


def one_kernel(mesh):
    chips = mesh.shape["ep"] // 2
    depth, height, width = torus_of(chips)
    return (height, width) == (2, 2) and chips * LANES == HEADS * HEAD_DIM and 4 * chips <= LANES


def solution(mesh):
    in_specs = (
        P("ep", None),
        P("ep", None, None),
        P("ep", None, None),
        P("ep"),
        P(),
        P(None, "ep"),
        P(),
        P(),
        P(),
        P(None, "ep"),
        P(),
        P("ep"),
        P("ep", None),
        P("ep"),
        P("ep", None),
        P("ep", None, None),
        P("ep", None, None),
        P("ep", None, None),
        P(None, "ep"),
        P(None, "ep"),
        P(),
        P(None, "ep"),
        P(),
    )
    out_specs = (P("ep", None), P("ep", None), P("ep", None))
    body = fused_shards if one_kernel(mesh) else shards
    return jax.shard_map(body, mesh=mesh, in_specs=in_specs, out_specs=out_specs, check_vma=False)
```

```python
import functools
import types

import jax
import jax.numpy as jnp
from jax import lax
from jax.experimental import pallas as pl
from jax.experimental.pallas import tpu as pltpu
from jax.sharding import PartitionSpec as P

HEADS = 32
HEAD_DIM = 64
KV_HEADS = 2
PER_GROUP = 16
TOP_K = 6
LANES = 128
MESH = pl.DeviceIdType.MESH

epsilon = 1e-06


def torus_of(chips):
    best = (chips, 1, 1)
    for x in range(1, chips + 1):
        for y in range(x, chips + 1):
            if chips % (x * y) == 0 and chips // (x * y) >= y:
                z = chips // (x * y)
                if z + y + x < sum(best):
                    best = (z, y, x)
    return best


def rms_scale(values):
    return lax.rsqrt(jnp.mean(values * values, axis=-1, keepdims=True) + epsilon)


class Place:
    def __init__(self, chips):
        self.chips = chips
        self.dims = torus_of(chips)
        me = lax.axis_index("ep")
        self.core = lax.rem(me, 2)
        self.chip = me // 2
        depth, height, width = self.dims
        self.x = lax.rem(self.chip, width)
        self.y = lax.rem(self.chip // width, height)
        self.z = self.chip // (width * height)

    def at(self, dz, dy, dx):
        depth, height, width = self.dims
        z = lax.rem(self.z + dz + depth, depth)
        y = lax.rem(self.y + dy + height, height)
        x = lax.rem(self.x + dx + width, width)
        return (z * height + y) * width + x

    def device(self, chip):
        return (chip * 2 + self.core,)

    def greet(self):
        barrier = pltpu.get_barrier_semaphore()
        for step in range(1, self.chips):
            other = lax.rem(self.chip + step, self.chips)
            pl.semaphore_signal(barrier, inc=1, device_id=self.device(other), device_id_type=MESH)
        pl.semaphore_wait(barrier, self.chips - 1)


def spread(place, halves):
    depth, height, width = place.dims
    sent = []
    counts = [0, 0]

    def push(half, source, origin, target):
        own, slots, send, recv = halves[half]
        copy = pltpu.make_async_remote_copy(
            src_ref=own if source is None else slots.at[source],
            dst_ref=slots.at[origin],
            send_sem=send.at[counts[half]],
            recv_sem=recv.at[origin],
            device_id=place.device(target),
            device_id_type=MESH,
        )
        counts[half] += 1
        copy.start()
        sent.append(copy)

    def arrive(half, origin):
        own, slots, send, recv = halves[half]
        pltpu.make_async_remote_copy(
            src_ref=slots.at[origin],
            dst_ref=slots.at[origin],
            send_sem=send.at[0],
            recv_sem=recv.at[origin],
            device_id=place.device(place.chip),
            device_id_type=MESH,
        ).wait_recv()

    def along(half, source, origin, axis):
        if axis == "x":
            for step in range(1, width):
                push(half, source, origin, place.at(0, 0, step))
        else:
            for step in range(1, height):
                push(half, source, origin, place.at(0, step, 0))

    orders = (("x", "y"), ("y", "x"))
    for step in range(1, depth):
        for half in range(2):
            push(half, None, place.chip, place.at(step, 0, 0))
    for half in range(2):
        for axis in orders[half]:
            along(half, None, place.chip, axis)
    for step in range(1, depth):
        for half in range(2):
            origin = place.at(-step, 0, 0)
            arrive(half, origin)
            for axis in orders[half]:
                along(half, origin, origin, axis)
    for up in range(depth):
        for half in range(2):
            reach = width if half == 0 else height
            for step in range(1, reach):
                origin = place.at(-up, 0, -step) if half == 0 else place.at(-up, -step, 0)
                arrive(half, origin)
                along(half, origin, origin, orders[half][1])
    for up in range(depth):
        for half in range(2):
            for dy in range(height):
                for dx in range(width):
                    if (dy if half == 0 else dx) != 0:
                        arrive(half, place.at(-up, -dy, -dx))
    for half in range(2):
        own, slots, _, _ = halves[half]
        slots[place.chip] = own[...]
    return sent


def deliver(place, tiles, landed, send, recv, out_ref):
    copies = []
    for step in range(1, place.chips):
        other = lax.rem(place.chip + step, place.chips)
        copy = pltpu.make_async_remote_copy(
            src_ref=tiles.at[other],
            dst_ref=landed.at[place.chip],
            send_sem=send.at[step],
            recv_sem=recv.at[place.chip],
            device_id=place.device(other),
            device_id_type=MESH,
        )
        copy.start()
        copies.append(copy)
    landed[place.chip] = tiles[place.chip]
    for step in range(1, place.chips):
        origin = lax.rem(place.chip - step + place.chips, place.chips)
        pltpu.make_async_remote_copy(
            src_ref=landed.at[origin],
            dst_ref=landed.at[origin],
            send_sem=send.at[0],
            recv_sem=recv.at[origin],
            device_id=place.device(place.chip),
            device_id_type=MESH,
        ).wait_recv()
    lanes = landed.shape[2]
    for block in range(place.chips):
        out_ref[:, block * lanes : (block + 1) * lanes] = landed[block]
    for copy in copies:
        copy.wait_send()


def flat(slots):
    count, rows, columns = slots.shape
    return slots[...].reshape(count * rows, columns)


def project_kernel(chips, a_ref, b_ref, w_ref, out_ref, slots_a, slots_b, tiles, landed,
                   send_a, recv_a, send_b, recv_b, send_t, recv_t):
    place = Place(chips)
    place.greet()
    sent = spread(place, ((a_ref, slots_a, send_a, recv_a), (b_ref, slots_b, send_b, recv_b)))
    cut = a_ref.shape[1]
    product = jnp.dot(flat(slots_a), w_ref[:cut], preferred_element_type=jnp.float32)
    product = product + jnp.dot(flat(slots_b), w_ref[cut:], preferred_element_type=jnp.float32)
    tiles[...] = product.astype(jnp.bfloat16).reshape(tiles.shape)
    deliver(place, tiles, landed, send_t, recv_t, out_ref)
    for copy in sent:
        copy.wait_send()


def gather_kernel(chips, a_ref, b_ref, gate_ref, up_ref, rows_ref, notes_ref, hidden_ref, slots_a, slots_b,
                  send_a, recv_a, send_b, recv_b):
    place = Place(chips)
    place.greet()
    sent = spread(place, ((a_ref, slots_a, send_a, recv_a), (b_ref, slots_b, send_b, recv_b)))
    cut = b_ref.shape[1]
    rows_a = slots_a[:, :, :cut].reshape(chips * a_ref.shape[0], cut)
    rows_b = flat(slots_b)
    rows_ref[:, :cut] = rows_a
    rows_ref[:, cut:] = rows_b
    notes_ref[...] = slots_a[:, :, cut:].reshape(notes_ref.shape)
    gate = jnp.dot(rows_a, gate_ref[:cut], preferred_element_type=jnp.float32)
    gate = gate + jnp.dot(rows_b, gate_ref[cut:], preferred_element_type=jnp.float32)
    upper = jnp.dot(rows_a, up_ref[:cut], preferred_element_type=jnp.float32)
    upper = upper + jnp.dot(rows_b, up_ref[cut:], preferred_element_type=jnp.float32)
    hidden_ref[...] = (jax.nn.silu(gate) * upper).astype(jnp.bfloat16)
    for copy in sent:
        copy.wait_send()


def down_kernel(chips, a_ref, b_ref, gain_ref, w_ref, out_ref, slots_a, slots_b, tiles, landed,
                send_a, recv_a, send_b, recv_b, send_t, recv_t):
    place = Place(chips)
    place.greet()
    sent = spread(place, ((a_ref, slots_a, send_a, recv_a), (b_ref, slots_b, send_b, recv_b)))
    rows, lanes = a_ref.shape
    part = chips // 2
    for half, slots in enumerate((slots_a, slots_b)):
        square = jnp.zeros((rows, lanes), jnp.float32)
        for block in range(chips):
            value = slots[block].astype(jnp.float32)
            square = square + value * value
        mean = jnp.sum(square, axis=1, keepdims=True) / (chips * lanes)
        scale = lax.rsqrt(mean + epsilon)
        total = jnp.zeros((rows, lanes), jnp.float32)
        for block in range(chips):
            gain = gain_ref[:, block * lanes : (block + 1) * lanes]
            normed = (slots[block].astype(jnp.float32) * scale * gain).astype(jnp.bfloat16)
            total = total + jnp.dot(
                normed,
                w_ref[block * lanes : (block + 1) * lanes],
                preferred_element_type=jnp.float32,
            )
        tiles[half * part : (half + 1) * part] = total.astype(jnp.bfloat16).reshape(
            part, rows // part, lanes
        )
    deliver(place, tiles, landed, send_t, recv_t, out_ref)
    for copy in sent:
        copy.wait_send()


def whole():
    return pl.BlockSpec(memory_space=pltpu.VMEM)


def spread_scratch(chips, a, b):
    slots = [pltpu.VMEM((chips,) + a.shape, a.dtype), pltpu.VMEM((chips,) + b.shape, b.dtype)]
    return slots, [pltpu.SemaphoreType.DMA((chips,))] * 4


def remote_params(number):
    return pltpu.CompilerParams(collective_id=number, has_side_effects=True)


def project(chips, number, rows, weight):
    count, width = rows.shape
    lanes = weight.shape[1]
    a, b = rows[:, : width // 2], rows[:, width // 2 :]
    slots, sems = spread_scratch(chips, a, b)
    tile = pltpu.VMEM((chips, count, lanes), jnp.bfloat16)
    return pl.pallas_call(
        functools.partial(project_kernel, chips),
        out_shape=jax.ShapeDtypeStruct((count, chips * lanes), jnp.bfloat16),
        in_specs=[whole()] * 3,
        out_specs=whole(),
        scratch_shapes=slots + [tile, tile] + sems + [pltpu.SemaphoreType.DMA((chips,))] * 2,
        compiler_params=remote_params(number),
        name="project",
    )(a, b, weight)


def gather_rows(chips, number, rows, notes, gate_w, up_w):
    count, width = rows.shape
    a = jnp.concatenate([rows[:, : width // 2], notes], axis=1)
    b = rows[:, width // 2 :]
    slots, sems = spread_scratch(chips, a, b)
    return pl.pallas_call(
        functools.partial(gather_kernel, chips),
        out_shape=(
            jax.ShapeDtypeStruct((chips * count, width), jnp.bfloat16),
            jax.ShapeDtypeStruct((chips * count, LANES), jnp.bfloat16),
            jax.ShapeDtypeStruct((chips * count, gate_w.shape[1]), jnp.bfloat16),
        ),
        in_specs=[whole()] * 4,
        out_specs=(whole(),) * 3,
        scratch_shapes=slots + sems,
        compiler_params=remote_params(number),
        name="gather_rows",
    )(a, b, gate_w, up_w)


def down_project(chips, number, hidden, gain, weight):
    count, lanes = hidden.shape
    a, b = hidden[: count // 2], hidden[count // 2 :]
    slots, sems = spread_scratch(chips, a, b)
    tile = pltpu.VMEM((chips, count // chips, lanes), jnp.bfloat16)
    return pl.pallas_call(
        functools.partial(down_kernel, chips),
        out_shape=jax.ShapeDtypeStruct((count // chips, chips * lanes), jnp.bfloat16),
        in_specs=[whole()] * 4,
        out_specs=whole(),
        scratch_shapes=slots + [tile, tile] + sems + [pltpu.SemaphoreType.DMA((chips,))] * 2,
        compiler_params=remote_params(number),
        name="down_project",
    )(a, b, gain[None, :], weight)


def stick_kernel(lens_ref, q_ref, k_ref, v_ref, bias_ref, out_ref):
    step = pl.program_id(0)
    batch, span, _ = k_ref.shape
    blocks = span // LANES
    row = lax.broadcasted_iota(jnp.int32, (3 * LANES, LANES), 0)
    column = lax.broadcasted_iota(jnp.int32, (3 * LANES, LANES), 1)
    after = (lax.rem(row, LANES) > column).astype(jnp.bfloat16)
    place = lax.broadcasted_iota(jnp.int32, (HEADS, span), 1)
    bias = bias_ref[:, :1]
    group = HEADS // KV_HEADS
    head = lax.broadcasted_iota(jnp.int32, (HEADS, LANES), 0)
    lane = lax.broadcasted_iota(jnp.int32, (HEADS, LANES), 1)
    own_lanes = (head // group) == (lane // HEAD_DIM)
    late = lax.broadcasted_iota(jnp.int32, (HEADS, HEAD_DIM), 0) >= group
    for item in range(batch):
        heads = q_ref[item].astype(jnp.float32)
        heads = jnp.where(own_lanes, jnp.concatenate([heads] * KV_HEADS, axis=1), 0.0)
        scores = lax.dot_general(
            heads.astype(jnp.bfloat16), k_ref[item], (((1,), (1,)), ((), ())), preferred_element_type=jnp.float32
        )
        scores = scores * HEAD_DIM ** (-0.5) + bias
        live = place < lens_ref[step * batch + item]
        remain = -(jnp.maximum(scores, 0.0) + jnp.log1p(jnp.exp(-jnp.abs(scores))))
        log_remain = jnp.where(live, remain, 0.0)
        stacked = jnp.concatenate(
            [log_remain[:, n * LANES : (n + 1) * LANES] for n in range(blocks)], axis=0
        )
        high = stacked.astype(jnp.bfloat16)
        rest = stacked - high.astype(jnp.float32)
        middle = rest.astype(jnp.bfloat16)
        low = (rest - middle.astype(jnp.float32)).astype(jnp.bfloat16)
        within = jnp.dot(
            jnp.concatenate([high, middle, low], axis=1), after, preferred_element_type=jnp.float32
        )
        totals = jnp.sum(stacked, axis=1, keepdims=True)
        carried = jnp.zeros((HEADS, 1), jnp.float32)
        pieces = [None] * blocks
        for n in range(blocks - 1, -1, -1):
            pieces[n] = within[n * HEADS : (n + 1) * HEADS] + carried
            carried = carried + totals[n * HEADS : (n + 1) * HEADS]
        remain_after = jnp.concatenate(pieces, axis=1)
        weights = jnp.where(live, jnp.exp(scores + remain + remain_after), 0.0)
        mixed = jnp.dot(
            weights.astype(jnp.bfloat16), v_ref[item], preferred_element_type=jnp.float32
        )
        mixed = jnp.where(late, mixed[:, HEAD_DIM:], mixed[:, :HEAD_DIM])
        out_ref[item] = mixed.astype(jnp.bfloat16)


def stick_read(queries, key_cache, value_cache, lengths, head_bias):
    batch, span, lanes = key_cache.shape
    heads = queries.reshape(batch, HEADS, HEAD_DIM)
    each = min(4, batch)
    mixed = pl.pallas_call(
        stick_kernel,
        out_shape=jax.ShapeDtypeStruct((batch, HEADS, HEAD_DIM), jnp.bfloat16),
        grid=(batch // each,),
        in_specs=[
            pl.BlockSpec(memory_space=pltpu.SMEM),
            pl.BlockSpec((each, HEADS, HEAD_DIM), lambda i: (i, 0, 0)),
            pl.BlockSpec((each, span, lanes), lambda i: (i, 0, 0)),
            pl.BlockSpec((each, span, lanes), lambda i: (i, 0, 0)),
            pl.BlockSpec((HEADS, LANES), lambda i: (0, 0)),
        ],
        out_specs=pl.BlockSpec((each, HEADS, HEAD_DIM), lambda i: (i, 0, 0)),
        name="stick_read",
    )(lengths, heads, key_cache, value_cache, jnp.broadcast_to(head_bias[:, None], (HEADS, LANES)))
    return mixed.reshape(batch, HEADS * HEAD_DIM)


def shards(
    tokens,
    cache_keys,
    cache_values,
    cache_len,
    norm_gain_first,
    w_query,
    w_key,
    w_value,
    head_bias,
    w_output,
    norm_gain_second,
    group_id,
    member,
    group_gate,
    member_weight,
    expert_gate_w,
    expert_up_w,
    expert_down_w,
    dense_gate_w,
    dense_up_w,
    hidden_gain,
    dense_down_w,
    branch_logit,
):
    devices = lax.axis_size("ep")
    chips = devices // 2
    me = lax.axis_index("ep")
    first = lax.rem(me, 2) == 0
    partner = [(i, i + 1 - 2 * (i % 2)) for i in range(devices)]
    seq_dev, width = tokens.shape

    def both(own):
        other = lax.ppermute(own, "ep", partner)
        return jnp.where(
            first, jnp.concatenate([own, other], axis=-1), jnp.concatenate([other, own], axis=-1)
        )

    query_w = both(w_query)
    output_w = both(w_output)
    gate_w = both(dense_gate_w)
    up_w = both(dense_up_w)
    down_w = both(dense_down_w)

    stream = tokens.astype(jnp.float32)
    normed_first = (stream * rms_scale(stream) * norm_gain_first).astype(jnp.bfloat16)
    new_keys = jnp.dot(normed_first, w_key, preferred_element_type=jnp.float32).astype(jnp.bfloat16)
    new_values = jnp.dot(normed_first, w_value, preferred_element_type=jnp.float32).astype(
        jnp.bfloat16
    )
    queries = project(chips, 1, normed_first, query_w)
    attended = stick_read(queries, cache_keys, cache_values, cache_len, head_bias)
    projected = project(chips, 2, attended, output_w)
    second_stream = stream + projected.astype(jnp.float32)
    normed_second = (second_stream * rms_scale(second_stream) * norm_gain_second).astype(
        jnp.bfloat16
    )

    experts = devices * expert_gate_w.shape[0]
    capacity = seq_dev // (experts // PER_GROUP)
    notes = jnp.concatenate(
        [member, group_id[:, None], jnp.zeros((seq_dev, LANES - TOP_K - 1), jnp.int32)], axis=1
    ).astype(jnp.bfloat16)
    own_rows, own_notes, hidden = gather_rows(chips, 3, normed_second, notes, gate_w, up_w)
    other_rows = lax.ppermute(own_rows, "ep", partner)
    other_notes = lax.ppermute(own_notes, "ep", partner)
    dense_out = down_project(chips, 4, hidden, hidden_gain, down_w)

    def selection(rows_notes, parity):
        table = rows_notes[:, : TOP_K + 1].astype(jnp.int32)
        named = table[:, TOP_K :] * PER_GROUP + table[:, :TOP_K]
        hits = jnp.any(named == me, axis=1).reshape(chips, seq_dev)
        index = jnp.arange(seq_dev)
        earlier = (index[:, None] < index[None, :]).astype(jnp.float32)
        slot = jnp.dot(hits.astype(jnp.float32), earlier).astype(jnp.int32)
        spot = ((jnp.arange(chips)[:, None] * 2 + parity) * capacity + slot).reshape(-1)
        spot = jnp.where(hits.reshape(-1), spot, -1)
        return (jnp.arange(devices * capacity)[:, None] == spot[None, :]).astype(jnp.bfloat16)

    parity = lax.rem(me, 2)
    packed = jnp.dot(selection(own_notes, parity), own_rows, preferred_element_type=jnp.float32)
    packed = packed + jnp.dot(
        selection(other_notes, 1 - parity), other_rows, preferred_element_type=jnp.float32
    )
    packed = packed.astype(jnp.bfloat16)
    gate_pre = jnp.dot(packed, expert_gate_w[0], preferred_element_type=jnp.float32)
    upper_pre = jnp.dot(packed, expert_up_w[0], preferred_element_type=jnp.float32)
    expert_hidden = (jax.nn.silu(gate_pre) * upper_pre).astype(jnp.bfloat16)
    served = jnp.dot(expert_hidden, expert_down_w[0], preferred_element_type=jnp.float32).astype(
        jnp.bfloat16
    )
    returned = lax.all_to_all(
        served.reshape(devices, capacity, width), "ep", split_axis=0, concat_axis=0, tiled=True
    ).reshape(experts * capacity, width)

    pair_expert = (group_id[:, None] * PER_GROUP + member).reshape(-1)
    pair_count = pair_expert.shape[0]
    expert_hits = (pair_expert[:, None] == jnp.arange(experts, dtype=jnp.int32)[None, :]).astype(
        jnp.float32
    )
    earlier = (jnp.arange(pair_count)[:, None] > jnp.arange(pair_count)[None, :]).astype(
        jnp.float32
    )
    before = jnp.dot(earlier, expert_hits, preferred_element_type=jnp.float32)
    slot_index = jnp.sum(before * expert_hits, axis=1).astype(jnp.int32)
    target = pair_expert * capacity + slot_index
    select = (target[:, None] == jnp.arange(experts * capacity, dtype=jnp.int32)[None, :]).astype(
        jnp.bfloat16
    )
    pair_out = jnp.dot(select, returned, preferred_element_type=jnp.float32)
    combine = (group_gate[:, None] * member_weight).reshape(-1, 1)
    routed = jnp.sum((pair_out * combine).reshape(seq_dev, TOP_K, width), axis=1)
    mixed_out = (
        second_stream + routed + jax.nn.sigmoid(branch_logit) * dense_out.astype(jnp.float32)
    )
    return (mixed_out.astype(jnp.bfloat16), new_keys, new_values)


LOG2E = 1.4426950408889634
DEAD = -1e30
BATCHES = 2
TRANSPOSED = (((1,), (1,)), ((), ()))
ORDERS = (("x", "y"), ("y", "x"))


def dot_t(a, b):
    return lax.dot_general(a, b, TRANSPOSED, preferred_element_type=jnp.float32)


def dot(a, b):
    return jnp.dot(a, b, preferred_element_type=jnp.float32)


def remote(src, dst, send, recv, device):
    return pltpu.make_async_remote_copy(
        src_ref=src, dst_ref=dst, send_sem=send, recv_sem=recv, device_id=device, device_id_type=MESH
    )


class Grid(Place):
    def __init__(self, chips):
        super().__init__(chips)
        self.partner = (self.chip * 2 + 1 - self.core,)
        self.depth = self.dims[0]
        self.plane = chips // self.depth

    def on(self, z, dy=0, dx=0):
        depth, height, width = self.dims
        y = lax.rem(self.y + dy, height)
        x = lax.rem(self.x + dx, width)
        return (z * height + y) * width + x

    def turn(self, axis):
        return (1, 0) if axis == "y" else (0, 1)

    def sweep(self, step):
        toward = 1 - 2 * (self.z // (self.depth // 2))
        return lax.rem(self.z + step * toward + self.depth, self.depth)

    def enter(self):
        barrier = pltpu.get_barrier_semaphore()
        for step in range(1, self.chips):
            other = lax.rem(self.chip + step, self.chips)
            pl.semaphore_signal(barrier, inc=1, device_id=self.device(other), device_id_type=MESH)
        pl.semaphore_signal(barrier, inc=1, device_id=self.partner, device_id_type=MESH)
        pl.semaphore_wait(barrier, self.chips)


class Clock:
    def __init__(self):
        self.now = 0.0

    def spend(self, time):
        self.now += time

    def run(self, batches):
        ready = {batch: 0.0 for batch in batches}
        while ready:
            batch = min(ready, key=lambda b: (max(ready[b], self.now), batches.index(b)))
            self.now = max(self.now, ready[batch])
            following = next(batch, None)
            if following is None:
                del ready[batch]
            else:
                ready[batch] = following


class Gather:
    def __init__(self, place, clock, send, recv, groups, pieces):
        self.place = place
        self.clock = clock
        self.send = send
        self.recv = recv
        self.groups = groups
        self.pieces = pieces

    def copy(self, piece, origin, index, target):
        view = self.pieces[piece](origin)
        return remote(view, view, self.send.at[piece], self.recv.at[piece, index], self.place.device(target))

    def several(self, piece, count, index):
        view = self.pieces[piece](pl.ds(0, count))
        return remote(view, view, self.send.at[piece], self.recv.at[piece, index],
                      self.place.device(self.place.chip))

    def turns(self, piece):
        first, second = ORDERS[piece]
        return self.place.turn(first), self.place.turn(second)

    def last(self, step):
        return 2 * self.place.depth + step * self.groups // self.place.depth

    def across(self, piece, step):
        place = self.place
        first, second = self.turns(piece)
        z = place.sweep(step)
        self.copy(piece, place.on(z), place.depth + z, place.on(place.z, *first)).start()
        self.copy(piece, place.on(z), self.last(step), place.on(place.z, *second)).start()

    def corner(self, piece, step):
        place = self.place
        first, second = self.turns(piece)
        z = place.sweep(step)
        origin = place.on(z, *first)
        self.copy(piece, origin, place.depth + z, place.chip).wait_recv()
        self.copy(piece, origin, self.last(step), place.on(place.z, *second)).start()

    def steps(self):
        place, depth = self.place, self.place.depth
        every = range(len(self.pieces))
        begin = self.begin = self.clock.now
        for step in range(1, depth):
            for piece in every:
                self.copy(piece, place.chip, place.z, place.on(place.sweep(step))).start()
        for piece in every:
            self.across(piece, 0)
        self.clock.spend(0.1)
        yield begin + 3.0
        for piece in every:
            self.corner(piece, 0)
        for step in range(1, depth):
            yield begin + 2.6 + 1.1 * step
            for piece in every:
                z = place.sweep(step)
                self.copy(piece, place.on(z), z, place.chip).wait_recv()
                self.across(piece, step)
        for step in range(1, depth):
            yield begin + 5.0 + 1.1 * step
            for piece in every:
                self.corner(piece, step)

    def rest(self, group):
        for piece in range(len(self.pieces)):
            self.several(piece, 2 * self.place.depth // self.groups, 2 * self.place.depth + group).wait_recv()

    def due(self, group):
        return self.begin + 7.5 + 1.1 * ((group + 1) * self.place.depth // self.groups - 1)

    def finish(self):
        for piece in range(len(self.pieces)):
            self.several(piece, self.place.chips - 1, 0).wait_send()


def norm_rows(values, gain):
    square = jnp.mean(values * values, axis=-1, keepdims=True)
    return (values * lax.rsqrt(square + epsilon) * gain).astype(jnp.bfloat16)


def layer_kernel(
    chips, names,
    lens_ref, ids_ref, bias_ref, tokens_ref, gain1_ref, gain2_ref, hgain_ref, logit_ref,
    member_ref, mweight_ref, group_ref, ggate_ref,
    keys_hbm, values_hbm, wq_hbm, wo_hbm, wg_hbm, wu_hbm, wd_hbm, wk_hbm, wv_hbm, eg_hbm, eu_hbm, ed_hbm,
    out_ref, newk_ref, newv_ref,
    *scratch,
):
    s = types.SimpleNamespace(**dict(zip(names, scratch)))
    place = Grid(chips)
    clock = Clock()
    me = place.chip * 2 + place.core
    chip, core, z, depth, plane = place.chip, place.core, place.z, place.depth, place.plane
    tokens, width = tokens_ref.shape
    seq = tokens // BATCHES
    half = width // 2
    rows = chips * seq
    lanes = LANES
    experts = chips * 2
    part = plane * seq
    bf16, f32 = jnp.bfloat16, jnp.float32
    cut = lanes + half
    chunk = width // 4
    group = me // PER_GROUP

    own_rows = pl.ds(pl.multiple_of(core * (lanes // 2), lanes // 2), lanes // 2)
    spot_me = lax.rem(chip, plane)
    weights = (
        (s.wq.at[own_rows], wq_hbm), (s.wo.at[spot_me, core], wo_hbm),
        (s.wg.at[own_rows], wg_hbm), (s.wu.at[own_rows], wu_hbm),
    )
    waiting = {}

    def fetch(key, src, dst):
        copy = pltpu.make_async_copy(src, dst, s.local_sem.at[len([k for k in waiting if k < 20])])
        copy.start()
        waiting[key] = copy.wait

    ended = set()

    def need(*keys):
        for key in keys:
            if key not in ended:
                ended.add(key)
                waiting[key]()

    for i, (dst, src) in enumerate(weights):
        fetch(i, src, dst)
    fetch(4, wk_hbm, s.wk)
    fetch(5, wv_hbm, s.wv)
    fetch(6, keys_hbm, s.keys)
    fetch(7, values_hbm, s.values)
    fetch(8, eg_hbm.at[0], s.eg)
    fetch(9, eu_hbm.at[0], s.eu)
    fetch(10, ed_hbm.at[0], s.ed)

    place_of = lax.broadcasted_iota(jnp.int32, (lanes, tokens), 0)
    expert = lax.rem(place_of, experts)
    combine = jnp.zeros((lanes, tokens), f32)
    for k in range(TOP_K):
        named = group_ref[...] * PER_GROUP + member_ref[k : k + 1, :]
        weight = ggate_ref[...] * mweight_ref[k : k + 1, :]
        combine = jnp.where(expert == named, weight, combine)
    high = combine.astype(bf16).astype(f32)
    notes = jnp.where(place_of < experts, high, jnp.where(place_of < 2 * experts, combine - high, 0.0))
    square = (tokens, tokens)
    row, column = (lax.broadcasted_iota(jnp.int32, square, axis) for axis in (0, 1))
    forward = backward = jnp.zeros(square, f32)
    order = [0] * tokens
    later = 0
    for token in range(tokens):
        named = ids_ref[token]
        slot = named * (seq + later) + (1 - named) * (token - later)
        later = later + named
        forward = jnp.where((row == slot) & (column == token), 1.0, forward)
        backward = jnp.where((row == token) & (column == slot), 1.0, backward)
        order = [jnp.where(slot == k, token, order[k]) for k in range(tokens)]
    forward, backward = forward.astype(bf16), backward.astype(bf16)
    notes = dot_t(forward, notes.astype(bf16)).astype(bf16)
    sorted_tokens = dot(forward, tokens_ref[...]).astype(bf16)
    for b in range(BATCHES):
        s.slots1[b, chip, :, :lanes] = notes[b * seq : (b + 1) * seq]
        s.slots1[b, chip, :, lanes:] = sorted_tokens[b * seq : (b + 1) * seq]

    span = s.keys.shape[1]
    blocks = span // lanes
    row = lax.broadcasted_iota(jnp.int32, (2 * lanes, 2 * lanes), 0)
    column = lax.broadcasted_iota(jnp.int32, (2 * lanes, 2 * lanes), 1)
    s.after[...] = jnp.where((lax.rem(row, lanes) > column) | (column >= lanes), 1.0, 0.0).astype(bf16)
    head_row = lax.broadcasted_iota(jnp.int32, (HEADS, lanes), 0)
    bias = jnp.zeros((HEADS, lanes), f32)
    for head in range(HEADS):
        bias = jnp.where(head_row == (head % 2) * chips + head // 2, bias_ref[head] * LOG2E, bias)
    s.bias[...] = bias

    place.enter()

    swaps = [
        remote(src, dst, s.swap_send.at[i], s.swap_recv.at[i], place.partner)
        for i, (dst, src) in enumerate(weights)
    ]
    for i, swap in enumerate(swaps):
        waiting[20 + i] = swap.wait_recv

    def down_copy(target):
        columns = pl.ds(pl.multiple_of(target * lanes, lanes), lanes)
        return remote(wd_hbm.at[:, columns], s.wd.at[chip, core], s.down_send.at[0],
                      s.down_recv.at[0], place.device(target))

    peers = ((0, 1), (1, 0), (1, 1))

    def wide_copy(index, target):
        return remote(wo_hbm, s.wo.at[spot_me, core], s.wide_send.at[0], s.wide_recv.at[index], place.device(target))

    def wide_pass(index):
        view = s.wo.at[lax.rem(place.on(z, *peers[index]), plane), core]
        arrived(view, s.wide_recv.at[index])
        remote(view, view, s.pass_send.at[0], s.pass_recv.at[0], place.partner).start()

    def spot(of):
        return lax.rem(of, plane) * depth + of // plane

    down_swap = remote(s.wd.at[:, core], s.wd.at[:, core], s.swap_send.at[4], s.swap_recv.at[4], place.partner)
    waiting[24] = down_swap.wait_recv

    def arrived(view, recv):
        remote(view, view, s.down_send.at[0], recv, place.device(chip)).wait_recv()

    def departed(view, send):
        return remote(view, view, send, s.down_recv.at[0], place.device(chip)).wait_send

    def others():
        return [lax.rem(chip + step, chips) for step in range(1, chips)]

    others_ds = pl.ds(0, chips - 1)

    def attend(b, item):
        jrow = lax.broadcasted_iota(jnp.int32, (chips, lanes), 0)
        jlane = lax.broadcasted_iota(jnp.int32, (chips, lanes), 1)
        early = jrow < chips // KV_HEADS
        own = (jlane // HEAD_DIM) == (jrow // (chips // KV_HEADS))
        even = s.heads[b, item]
        turned = pltpu.roll(even, HEAD_DIM, axis=1)
        query = jnp.concatenate([
            jnp.where(own, jnp.where(early, even, turned), 0.0),
            jnp.where(own, jnp.where(early, turned, even), 0.0),
        ], axis=0).astype(bf16)
        index = order[b * seq + item]
        scores = dot_t(query, s.keys[index]) * (HEAD_DIM ** (-0.5) * LOG2E)
        scores = scores + jnp.concatenate([s.bias[...]] * blocks, axis=1)
        position = lax.broadcasted_iota(jnp.int32, (HEADS, span), 1)
        scores = jnp.where(position < lens_ref[index], scores, DEAD)
        soft = jnp.maximum(scores, 0.0) + jnp.log(1.0 + jnp.exp2(-jnp.abs(scores))) * LOG2E
        stacked = jnp.concatenate([soft[:, n * lanes : (n + 1) * lanes] for n in range(blocks)], axis=0)
        top = stacked.astype(bf16)
        low = (stacked - top.astype(f32)).astype(bf16)
        sums = dot(jnp.concatenate([top, low], axis=1), s.after[...])
        carried = jnp.zeros((HEADS, lanes), f32)
        pieces = [None] * blocks
        for n in range(blocks - 1, -1, -1):
            band = sums[n * HEADS : (n + 1) * HEADS]
            spent = stacked[n * HEADS : (n + 1) * HEADS] + band[:, :lanes] + carried
            pieces[n] = jnp.exp2(scores[:, n * lanes : (n + 1) * lanes] - spent).astype(bf16)
            carried = carried + band[:, lanes:]
        found = dot(jnp.concatenate(pieces, axis=1), s.values[index])
        first, second = found[:chips], found[chips:]
        s.mixed[b, item] = jnp.where(
            jlane < HEAD_DIM,
            jnp.where(early, first, pltpu.roll(first, HEAD_DIM, axis=1)),
            jnp.where(early, pltpu.roll(second, HEAD_DIM, axis=1), second),
        )

    def columns_of(piece):
        return slice(piece * half, (piece + 1) * half)

    sends = []

    def batch(b):
        slots1, slots2, slots3 = s.slots1.at[b], s.slots2.at[b], s.slots3.at[b]
        gather = Gather(place, clock, s.gather_send.at[b, 0], s.gather_recv.at[b, 0], depth // 2, (
            lambda o: slots1.at[o, :, pl.ds(0, cut)],
            lambda o: slots1.at[o, :, pl.ds(cut, half)],
        ))
        sends.append(gather.finish)
        steps = gather.steps()
        yield next(steps)
        if b == 0:
            for swap in swaps:
                swap.start()
                sends.append(swap.wait_send)
        yield from steps

        tiles, landed = s.tiles.at[b], s.landed.at[b]

        def tile_copy(target):
            return remote(tiles.at[target], landed.at[chip], s.tile_send.at[b], s.tile_recv.at[b],
                          place.device(target))

        for pair in range(depth // 2):
            yield gather.due(pair)
            need(0, 20)
            gather.rest(pair)
            planes = []
            for step in (2 * pair, 2 * pair + 1):
                zo = place.sweep(step)
                planes.append(slots1[pl.ds(zo * plane, plane), :, lanes:].reshape(part, width))
            normed = norm_rows(jnp.concatenate(planes, axis=0).astype(f32), gain1_ref[...])
            product = dot_t(normed, s.wq[...]).astype(bf16).reshape(2, plane, seq, lanes)
            for side, step in enumerate((2 * pair, 2 * pair + 1)):
                zo = place.sweep(step)
                tiles[pl.ds(zo * plane, plane)] = product[side]
                for dy in (1, 0):
                    for dx in (1, 0):
                        if (step, dy, dx) != (0, 0, 0):
                            tile_copy(place.on(zo, dy, dx)).start()
            clock.spend(0.6)
        landed[chip] = tiles[chip]
        sends.append(departed(tiles.at[others_ds], s.tile_send.at[b]))
        begin = clock.now

        if b == BATCHES - 1:
            for index, turn in enumerate(peers):
                wide_copy(index, place.on(z, *turn)).start()
            for target in others():
                down_copy(target).start()
            sends.append(departed(s.wd.at[others_ds, core], s.down_send.at[0]))
            sends.append(departed(s.wo.at[pl.ds(0, 3), 0], s.wide_send.at[0]))
            sends.append(departed(s.wo.at[pl.ds(0, 3), 0], s.pass_send.at[0]))
            fetch(11, wd_hbm.at[:, pl.ds(pl.multiple_of(chip * lanes, lanes), lanes)], s.wd.at[chip, core])
            need(4, 5)
            own_normed = norm_rows(tokens_ref[...].astype(f32), gain1_ref[...])
            newk_ref[...] = dot(own_normed, s.wk[...]).astype(bf16)
            newv_ref[...] = dot(own_normed, s.wv[...]).astype(bf16)
            clock.spend(0.4)
        yield begin + 4.0
        arrived(landed.at[others_ds], s.tile_recv.at[b])
        for j in range(chips):
            s.heads[b, :, j, :] = landed[j].astype(f32)
        need(6, 7)
        for item in range(seq):
            attend(b, item)
            if item % 2 == 1:
                clock.spend(0.9)
                yield clock.now
        for j in range(chips):
            slots2[z, :, j * lanes : (j + 1) * lanes] = s.mixed[b, :, j, :].astype(bf16)
        clock.spend(0.1)

        begin = clock.now
        for step in range(depth - 1, 0, -1):
            remote(slots2.at[z], slots2.at[z], s.line_send.at[b], s.line_recv.at[b],
                   place.device(place.on(place.sweep(step)))).start()
        line_view = slots2.at[pl.ds(0, depth - 1)]
        sends.append(departed(line_view, s.line_send.at[b]))
        if b == 0:
            for index in range(3):
                yield begin + 0.9 + 0.9 * index
                if index == 0:
                    need(1)
                wide_pass(index)
        yield begin + 5.5
        arrived(line_view, s.line_recv.at[b])
        need(21)
        if b == 0:
            arrived(s.wo.at[pl.ds(0, 3), 0], s.pass_recv.at[0])
        line_rows = slots2[...].reshape(depth * seq, width)
        product = dot_t(line_rows, s.wo[...].reshape(plane * lanes, width)).astype(bf16)
        slots3[chip] = product.reshape(depth, seq, plane * lanes)
        clock.spend(0.7)

        gather = Gather(place, clock, s.gather_send.at[b, 1], s.gather_recv.at[b, 0], 1, (
            lambda o: slots3.at[o, pl.ds(0, depth // 2)],
            lambda o: slots3.at[o, pl.ds(depth // 2, depth // 2)],
        ))
        sends.append(gather.finish)
        yield from gather.steps()
        if b == 0:
            need(11)
            arrived(s.wd.at[others_ds, core], s.down_recv.at[0])
            down_swap.start()
            sends.append(down_swap.wait_send)
        both = s.rows.at[b]
        acc = s.acc.at[b]

        def serve(c, lent):
            if lent:
                arrived(both.at[c], s.row_recv.at[b])
            every = both[c, :, :width]
            served = (jax.nn.silu(dot(every, s.eg[...])) * dot(every, s.eu[...])).astype(bf16)
            note_lane = lax.broadcasted_iota(jnp.int32, (rows, lanes), 1)
            mine = (note_lane == me) | (note_lane == me + experts)
            weight = jnp.sum(jnp.where(mine, both[c, :, width:].astype(f32), 0.0), axis=1, keepdims=True)
            for n in range(4):
                at = slice(n * chunk, (n + 1) * chunk)
                value = dot(served, s.ed[:, at])
                value = jnp.where(weight != 0.0, value * weight, 0.0)
                if lent:
                    s.gift[n] = value.astype(bf16)
                    remote(s.gift.at[n], s.given.at[n], s.gift_send.at[0], s.gift_recv.at[n // 2],
                           place.partner).start()
                else:
                    acc[:, :, at] = value.reshape(chips, seq, chunk)

        yield gather.due(0)
        need(8, 9, 10)

        if b == 0:

            @pl.when((group == b) & (core == 0))
            def _():
                serve(1, True)

            clock.spend(0.6)
        gather.rest(0)

        block = rows // 2
        served_here = pl.when(group == b)
        line = depth * seq
        for n in range(2):
            at = slice(n * block, (n + 1) * block)
            for p in range(n * plane // 2, (n + 1) * plane // 2):
                of = slice(p * line, (p + 1) * line)
                token = jnp.concatenate(
                    [slots1[k * plane + p, :, lanes:].astype(f32) for k in range(depth)], axis=0)
                projected = jnp.concatenate(
                    [slots3[k * plane + p].reshape(line, plane * lanes) for k in range(depth)], axis=1)
                both[core, of, :width] = norm_rows(token + projected.astype(f32), gain2_ref[...])
                for k in range(depth):
                    both[core, p * line + k * seq : p * line + (k + 1) * seq, width:] = (
                        slots1[k * plane + p, :, :lanes])

            @served_here
            def _():
                remote(both.at[core, at], both.at[core, at], s.row_send.at[b], s.row_recv.at[b],
                       place.partner).start()

        clock.spend(0.4)

        need(2, 3, 22, 23)
        normed = both[core, :, :width]
        gate = dot_t(normed, s.wg[...])
        hidden = jax.nn.silu(gate) * dot_t(normed, s.wu[...])
        s.hidden[b] = hidden
        squares = s.squares.at[b]
        summed = jnp.broadcast_to(jnp.sum(hidden * hidden, axis=1, keepdims=True), (rows, lanes))
        squares[chip] = jnp.transpose(summed)[:1]

        def square_copy(target):
            return remote(squares.at[chip], squares.at[chip], s.square_send.at[b],
                          s.square_recv.at[b], place.device(target))

        for target in others():
            square_copy(target).start()
        sends.append(departed(squares.at[others_ds], s.square_send.at[b]))
        clock.spend(0.5)
        sent_at = clock.now

        for c in range(2):

            @pl.when((group == b) & (core == c))
            def _():
                serve(c, False)

        clock.spend(1.0)
        yield sent_at + 5.5

        @pl.when((group == b) & (core == 1))
        def _():
            serve(0, True)

        if b > 0:

            @pl.when((group == b) & (core == 0))
            def _():
                serve(1, True)

        clock.spend(0.6)

        def end_served():
            @pl.when(group == b)
            def _():
                departed(both.at[core], s.row_send.at[b])()
                departed(s.gift, s.gift_send.at[0])()

        sends.append(end_served)

        arrived(squares.at[others_ds], s.square_recv.at[b])
        total = squares[0]
        for c in range(1, chips):
            total = total + squares[c]
        scale = lax.rsqrt(total / width + epsilon)
        scale = jnp.transpose(jnp.broadcast_to(scale, (lanes, rows)))
        gain = hgain_ref[:, pl.ds(pl.multiple_of(chip * lanes, lanes), lanes)]
        dense = (s.hidden[b] * scale * gain).astype(bf16)
        need(24)

        stage = s.stage.at[b]

        def staged(piece, value, slot, index, recv, target):
            stage[piece, slot] = value.astype(bf16)
            remote(stage.at[piece, slot], s.sums.at[b, piece, index], s.sum_send.at[b, piece],
                   s.sum_recv.at[b, piece, recv], place.device(target)).start()

        def summands(piece, index, count, recv):
            view = s.sums.at[b, piece, pl.ds(index, count)]
            arrived(view, s.sum_recv.at[b, piece, recv])

        def summand(piece, index):
            return s.sums[b, piece, index].astype(f32)

        for piece in range(2):
            sends.append(departed(stage.at[piece, pl.ds(0, 4 * depth - 1)], s.sum_send.at[b, piece]))
            first, second = (place.turn(a) for a in ORDERS[piece])

            @served_here
            def _():
                arrived(s.given.at[pl.ds(2 * piece, 2)], s.gift_recv.at[piece])

            for c in (2 * piece, 2 * piece + 1):
                at = slice(c * chunk, (c + 1) * chunk)
                down = s.wd[c * (chips // 4) : (c + 1) * (chips // 4)].reshape(chunk, lanes)
                value = jax.nn.sigmoid(logit_ref[:, at]) * dot_t(dense, down)
                value = value.reshape(chips, seq, chunk)

                @served_here
                def _():
                    acc[:, :, at] += s.given[c].astype(f32).reshape(chips, seq, chunk) + value

                @pl.when(group != b)
                def _():
                    acc[:, :, at] = value

            for beside in (1, 0):
                for step in range(depth - 1, -1, -1):
                    zo = place.sweep(step)
                    turn = (1, 1) if beside else first
                    index, recv = (zo, zo) if beside else (depth + 2 * zo, depth + zo)
                    staged(piece, acc[spot(place.on(zo, *turn)), :, columns_of(piece)], step * 2 + beside,
                           index, recv, place.on(z, *first))
        clock.spend(1.0)
        begin = clock.now

        for step in range(depth - 1, -1, -1):
            yield begin + 2.5 + 0.8 * (depth - 1 - step)
            for piece in range(2):
                first, second = (place.turn(a) for a in ORDERS[piece])
                zo = place.sweep(step)
                summands(piece, zo, 1, zo)
                value = acc[spot(place.on(zo, *second)), :, columns_of(piece)] + summand(piece, zo)
                staged(piece, value, 2 * depth + step, depth + 2 * zo + 1, depth + zo, place.on(z, *second))

        def folded(piece, zo):
            summands(piece, depth + 2 * zo, 2, depth + zo)
            value = acc[spot(place.on(zo)), :, columns_of(piece)] + summand(piece, depth + 2 * zo)
            return value + summand(piece, depth + 2 * zo + 1)

        for step in range(depth - 1, 0, -1):
            yield begin + 5.2 + 0.8 * (depth - 1 - step)
            for piece in range(2):
                zo = place.sweep(step)
                staged(piece, folded(piece, zo), 3 * depth + step - 1, 3 * depth + z, 2 * depth, place.on(zo))
        yield begin + 8.0
        for piece in range(2):
            at = columns_of(piece)
            value = slots1[chip, :, lanes + piece * half : lanes + (piece + 1) * half].astype(f32)
            value = value + jnp.concatenate(
                [slots3[k * plane + spot_me, z] for k in range(piece * depth // 2, (piece + 1) * depth // 2)], axis=1
            ).astype(f32)
            acc[spot(chip), :, at] = value + folded(piece, z)
        yield begin + 11.0
        for piece in range(2):
            summands(piece, 3 * depth, depth - 1, 2 * depth)
            value = acc[spot(chip), :, columns_of(piece)]
            for step in range(1, depth):
                value = value + summand(piece, 3 * depth + place.sweep(step))
            s.final[b * seq : (b + 1) * seq, columns_of(piece)] = value.astype(bf16)

    clock.run([batch(b) for b in range(BATCHES)])
    out_ref[...] = dot(backward, s.final[...]).astype(bf16)
    for end in sends:
        end()


def copy_kernel(a_ref, b_ref, c_ref, a_out, b_out, c_out):
    a_out[...] = a_ref[...]
    b_out[...] = b_ref[...]
    c_out[...] = c_ref[...]


def layer_scratch(chips, depth, tokens, width, span, fe):
    n = BATCHES
    seq = tokens // n
    rows = chips * seq
    bf16, f32, DMA = jnp.bfloat16, jnp.float32, pltpu.SemaphoreType.DMA
    half = width // 2
    return dict(
        slots1=pltpu.VMEM((n, chips, seq, LANES + width), bf16),
        slots2=pltpu.VMEM((n, depth, seq, width), bf16),
        slots3=pltpu.VMEM((n, chips, depth, seq, chips // depth * LANES), bf16),
        keys=pltpu.VMEM((tokens, span, LANES), bf16),
        values=pltpu.VMEM((tokens, span, LANES), bf16),
        wq=pltpu.VMEM((LANES, width), bf16),
        wo=pltpu.VMEM((chips // depth, 2, LANES // 2, width), bf16),
        wg=pltpu.VMEM((LANES, width), bf16),
        wu=pltpu.VMEM((LANES, width), bf16),
        wk=pltpu.VMEM((width, LANES), bf16),
        wv=pltpu.VMEM((width, LANES), bf16),
        eg=pltpu.VMEM((width, fe), bf16),
        eu=pltpu.VMEM((width, fe), bf16),
        ed=pltpu.VMEM((fe, width), bf16),
        wd=pltpu.VMEM((chips, 2, LANES // 2, LANES), bf16),
        after=pltpu.VMEM((2 * LANES, 2 * LANES), bf16),
        bias=pltpu.VMEM((HEADS, LANES), f32),
        tiles=pltpu.VMEM((n, chips, seq, LANES), bf16),
        landed=pltpu.VMEM((n, chips, seq, LANES), bf16),
        heads=pltpu.VMEM((n, seq, chips, LANES), f32),
        mixed=pltpu.VMEM((n, seq, chips, LANES), f32),
        rows=pltpu.VMEM((n, 2, rows, width + LANES), bf16),
        final=pltpu.VMEM((tokens, width), bf16),
        hidden=pltpu.VMEM((n, rows, LANES), f32),
        squares=pltpu.VMEM((n, chips, 1, rows), f32),
        gift=pltpu.VMEM((4, rows, width // 4), bf16),
        given=pltpu.VMEM((4, rows, width // 4), bf16),
        acc=pltpu.VMEM((n, chips, seq, width), f32),
        stage=pltpu.VMEM((n, 2, 4 * depth, seq, half), bf16),
        sums=pltpu.VMEM((n, 2, 4 * depth, seq, half), bf16),
        local_sem=DMA((12,)),
        swap_send=DMA((5,)),
        swap_recv=DMA((5,)),
        gather_send=DMA((n, 2, 2)),
        gather_recv=DMA((n, 1, 2, 5 * depth // 2)),
        line_send=DMA((n,)),
        line_recv=DMA((n,)),
        wide_send=DMA((1,)),
        wide_recv=DMA((3,)),
        pass_send=DMA((1,)),
        pass_recv=DMA((1,)),
        tile_send=DMA((n,)),
        tile_recv=DMA((n,)),
        down_send=DMA((1,)),
        down_recv=DMA((1,)),
        square_send=DMA((n,)),
        square_recv=DMA((n,)),
        row_send=DMA((n,)),
        row_recv=DMA((n,)),
        gift_send=DMA((1,)),
        gift_recv=DMA((2,)),
        sum_send=DMA((n, 2)),
        sum_recv=DMA((n, 2, 2 * depth + 1)),
    )


def fused_shards(
    tokens, cache_keys, cache_values, cache_len, norm_gain_first, w_query, w_key, w_value, head_bias,
    w_output, norm_gain_second, group_id, member, group_gate, member_weight, expert_gate_w,
    expert_up_w, expert_down_w, dense_gate_w, dense_up_w, hidden_gain, dense_down_w, branch_logit,
):
    chips = lax.axis_size("ep") // 2
    seq, width = tokens.shape
    span = cache_keys.shape[1]
    bf16 = jnp.bfloat16
    scratch = layer_scratch(chips, torus_of(chips)[0], seq, width, span, expert_gate_w.shape[2])
    smem = pl.BlockSpec(memory_space=pltpu.SMEM)
    anywhere = pl.BlockSpec(memory_space=pl.ANY)
    out_shape = (
        jax.ShapeDtypeStruct((seq, width), bf16),
        jax.ShapeDtypeStruct((seq, LANES), bf16),
        jax.ShapeDtypeStruct((seq, LANES), bf16),
    )
    results = pl.pallas_call(
        functools.partial(layer_kernel, chips, tuple(scratch)),
        out_shape=out_shape,
        in_specs=[smem] * 3 + [whole()] * 9 + [anywhere] * 12,
        out_specs=(whole(),) * 3,
        scratch_shapes=list(scratch.values()),
        compiler_params=pltpu.CompilerParams(
            collective_id=1, has_side_effects=True, vmem_limit_bytes=60 * 1024 * 1024
        ),
        name="layer",
    )(
        cache_len, group_id, head_bias, tokens, norm_gain_first[None], norm_gain_second[None], hidden_gain[None],
        branch_logit[None], member.T, member_weight.T, group_id[None], group_gate[None],
        cache_keys, cache_values, w_query.T, w_output.T, dense_gate_w.T, dense_up_w.T, dense_down_w.T,
        w_key, w_value, expert_gate_w, expert_up_w, expert_down_w,
    )
    return pl.pallas_call(
        copy_kernel, out_shape=out_shape, in_specs=[whole()] * 3, out_specs=(whole(),) * 3, name="results"
    )(*results)


def one_kernel(mesh):
    chips = mesh.shape["ep"] // 2
    depth, height, width = torus_of(chips)
    return (height, width) == (2, 2) and chips * LANES == HEADS * HEAD_DIM and 4 * chips <= LANES and depth % 2 == 0 and 2 * chips == BATCHES * PER_GROUP


def solution(mesh):
    in_specs = (
        P("ep", None),
        P("ep", None, None),
        P("ep", None, None),
        P("ep"),
        P(),
        P(None, "ep"),
        P(),
        P(),
        P(),
        P(None, "ep"),
        P(),
        P("ep"),
        P("ep", None),
        P("ep"),
        P("ep", None),
        P("ep", None, None),
        P("ep", None, None),
        P("ep", None, None),
        P(None, "ep"),
        P(None, "ep"),
        P(),
        P(None, "ep"),
        P(),
    )
    out_specs = (P("ep", None), P("ep", None), P("ep", None))
    body = fused_shards if one_kernel(mesh) else shards
    return jax.shard_map(body, mesh=mesh, in_specs=in_specs, out_specs=out_specs, check_vma=False)
```

```python
import functools
import types

import jax
import jax.numpy as jnp
from jax import lax
from jax.experimental import pallas as pl
from jax.experimental.pallas import tpu as pltpu
from jax.sharding import PartitionSpec as P

HEADS = 32
HEAD_DIM = 64
KV_HEADS = 2
PER_GROUP = 16
TOP_K = 6
LANES = 128
MESH = pl.DeviceIdType.MESH

epsilon = 1e-06


def torus_of(chips):
    best = (chips, 1, 1)
    for x in range(1, chips + 1):
        for y in range(x, chips + 1):
            if chips % (x * y) == 0 and chips // (x * y) >= y:
                z = chips // (x * y)
                if z + y + x < sum(best):
                    best = (z, y, x)
    return best


def rms_scale(values):
    return lax.rsqrt(jnp.mean(values * values, axis=-1, keepdims=True) + epsilon)


class Place:
    def __init__(self, chips):
        self.chips = chips
        self.dims = torus_of(chips)
        me = lax.axis_index("ep")
        self.core = lax.rem(me, 2)
        self.chip = me // 2
        depth, height, width = self.dims
        self.x = lax.rem(self.chip, width)
        self.y = lax.rem(self.chip // width, height)
        self.z = self.chip // (width * height)

    def at(self, dz, dy, dx):
        depth, height, width = self.dims
        z = lax.rem(self.z + dz + depth, depth)
        y = lax.rem(self.y + dy + height, height)
        x = lax.rem(self.x + dx + width, width)
        return (z * height + y) * width + x

    def device(self, chip):
        return (chip * 2 + self.core,)

    def greet(self):
        barrier = pltpu.get_barrier_semaphore()
        for step in range(1, self.chips):
            other = lax.rem(self.chip + step, self.chips)
            pl.semaphore_signal(barrier, inc=1, device_id=self.device(other), device_id_type=MESH)
        pl.semaphore_wait(barrier, self.chips - 1)


def spread(place, halves):
    depth, height, width = place.dims
    sent = []
    counts = [0, 0]

    def push(half, source, origin, target):
        own, slots, send, recv = halves[half]
        copy = pltpu.make_async_remote_copy(
            src_ref=own if source is None else slots.at[source],
            dst_ref=slots.at[origin],
            send_sem=send.at[counts[half]],
            recv_sem=recv.at[origin],
            device_id=place.device(target),
            device_id_type=MESH,
        )
        counts[half] += 1
        copy.start()
        sent.append(copy)

    def arrive(half, origin):
        own, slots, send, recv = halves[half]
        pltpu.make_async_remote_copy(
            src_ref=slots.at[origin],
            dst_ref=slots.at[origin],
            send_sem=send.at[0],
            recv_sem=recv.at[origin],
            device_id=place.device(place.chip),
            device_id_type=MESH,
        ).wait_recv()

    def along(half, source, origin, axis):
        if axis == "x":
            for step in range(1, width):
                push(half, source, origin, place.at(0, 0, step))
        else:
            for step in range(1, height):
                push(half, source, origin, place.at(0, step, 0))

    orders = (("x", "y"), ("y", "x"))
    for step in range(1, depth):
        for half in range(2):
            push(half, None, place.chip, place.at(step, 0, 0))
    for half in range(2):
        for axis in orders[half]:
            along(half, None, place.chip, axis)
    for step in range(1, depth):
        for half in range(2):
            origin = place.at(-step, 0, 0)
            arrive(half, origin)
            for axis in orders[half]:
                along(half, origin, origin, axis)
    for up in range(depth):
        for half in range(2):
            reach = width if half == 0 else height
            for step in range(1, reach):
                origin = place.at(-up, 0, -step) if half == 0 else place.at(-up, -step, 0)
                arrive(half, origin)
                along(half, origin, origin, orders[half][1])
    for up in range(depth):
        for half in range(2):
            for dy in range(height):
                for dx in range(width):
                    if (dy if half == 0 else dx) != 0:
                        arrive(half, place.at(-up, -dy, -dx))
    for half in range(2):
        own, slots, _, _ = halves[half]
        slots[place.chip] = own[...]
    return sent


def deliver(place, tiles, landed, send, recv, out_ref):
    copies = []
    for step in range(1, place.chips):
        other = lax.rem(place.chip + step, place.chips)
        copy = pltpu.make_async_remote_copy(
            src_ref=tiles.at[other],
            dst_ref=landed.at[place.chip],
            send_sem=send.at[step],
            recv_sem=recv.at[place.chip],
            device_id=place.device(other),
            device_id_type=MESH,
        )
        copy.start()
        copies.append(copy)
    landed[place.chip] = tiles[place.chip]
    for step in range(1, place.chips):
        origin = lax.rem(place.chip - step + place.chips, place.chips)
        pltpu.make_async_remote_copy(
            src_ref=landed.at[origin],
            dst_ref=landed.at[origin],
            send_sem=send.at[0],
            recv_sem=recv.at[origin],
            device_id=place.device(place.chip),
            device_id_type=MESH,
        ).wait_recv()
    lanes = landed.shape[2]
    for block in range(place.chips):
        out_ref[:, block * lanes : (block + 1) * lanes] = landed[block]
    for copy in copies:
        copy.wait_send()


def flat(slots):
    count, rows, columns = slots.shape
    return slots[...].reshape(count * rows, columns)


def project_kernel(chips, a_ref, b_ref, w_ref, out_ref, slots_a, slots_b, tiles, landed,
                   send_a, recv_a, send_b, recv_b, send_t, recv_t):
    place = Place(chips)
    place.greet()
    sent = spread(place, ((a_ref, slots_a, send_a, recv_a), (b_ref, slots_b, send_b, recv_b)))
    cut = a_ref.shape[1]
    product = jnp.dot(flat(slots_a), w_ref[:cut], preferred_element_type=jnp.float32)
    product = product + jnp.dot(flat(slots_b), w_ref[cut:], preferred_element_type=jnp.float32)
    tiles[...] = product.astype(jnp.bfloat16).reshape(tiles.shape)
    deliver(place, tiles, landed, send_t, recv_t, out_ref)
    for copy in sent:
        copy.wait_send()


def gather_kernel(chips, a_ref, b_ref, gate_ref, up_ref, rows_ref, notes_ref, hidden_ref, slots_a, slots_b,
                  send_a, recv_a, send_b, recv_b):
    place = Place(chips)
    place.greet()
    sent = spread(place, ((a_ref, slots_a, send_a, recv_a), (b_ref, slots_b, send_b, recv_b)))
    cut = b_ref.shape[1]
    rows_a = slots_a[:, :, :cut].reshape(chips * a_ref.shape[0], cut)
    rows_b = flat(slots_b)
    rows_ref[:, :cut] = rows_a
    rows_ref[:, cut:] = rows_b
    notes_ref[...] = slots_a[:, :, cut:].reshape(notes_ref.shape)
    gate = jnp.dot(rows_a, gate_ref[:cut], preferred_element_type=jnp.float32)
    gate = gate + jnp.dot(rows_b, gate_ref[cut:], preferred_element_type=jnp.float32)
    upper = jnp.dot(rows_a, up_ref[:cut], preferred_element_type=jnp.float32)
    upper = upper + jnp.dot(rows_b, up_ref[cut:], preferred_element_type=jnp.float32)
    hidden_ref[...] = (jax.nn.silu(gate) * upper).astype(jnp.bfloat16)
    for copy in sent:
        copy.wait_send()


def down_kernel(chips, a_ref, b_ref, gain_ref, w_ref, out_ref, slots_a, slots_b, tiles, landed,
                send_a, recv_a, send_b, recv_b, send_t, recv_t):
    place = Place(chips)
    place.greet()
    sent = spread(place, ((a_ref, slots_a, send_a, recv_a), (b_ref, slots_b, send_b, recv_b)))
    rows, lanes = a_ref.shape
    part = chips // 2
    for half, slots in enumerate((slots_a, slots_b)):
        square = jnp.zeros((rows, lanes), jnp.float32)
        for block in range(chips):
            value = slots[block].astype(jnp.float32)
            square = square + value * value
        mean = jnp.sum(square, axis=1, keepdims=True) / (chips * lanes)
        scale = lax.rsqrt(mean + epsilon)
        total = jnp.zeros((rows, lanes), jnp.float32)
        for block in range(chips):
            gain = gain_ref[:, block * lanes : (block + 1) * lanes]
            normed = (slots[block].astype(jnp.float32) * scale * gain).astype(jnp.bfloat16)
            total = total + jnp.dot(
                normed,
                w_ref[block * lanes : (block + 1) * lanes],
                preferred_element_type=jnp.float32,
            )
        tiles[half * part : (half + 1) * part] = total.astype(jnp.bfloat16).reshape(
            part, rows // part, lanes
        )
    deliver(place, tiles, landed, send_t, recv_t, out_ref)
    for copy in sent:
        copy.wait_send()


def whole():
    return pl.BlockSpec(memory_space=pltpu.VMEM)


def spread_scratch(chips, a, b):
    slots = [pltpu.VMEM((chips,) + a.shape, a.dtype), pltpu.VMEM((chips,) + b.shape, b.dtype)]
    return slots, [pltpu.SemaphoreType.DMA((chips,))] * 4


def remote_params(number):
    return pltpu.CompilerParams(collective_id=number, has_side_effects=True)


def project(chips, number, rows, weight):
    count, width = rows.shape
    lanes = weight.shape[1]
    a, b = rows[:, : width // 2], rows[:, width // 2 :]
    slots, sems = spread_scratch(chips, a, b)
    tile = pltpu.VMEM((chips, count, lanes), jnp.bfloat16)
    return pl.pallas_call(
        functools.partial(project_kernel, chips),
        out_shape=jax.ShapeDtypeStruct((count, chips * lanes), jnp.bfloat16),
        in_specs=[whole()] * 3,
        out_specs=whole(),
        scratch_shapes=slots + [tile, tile] + sems + [pltpu.SemaphoreType.DMA((chips,))] * 2,
        compiler_params=remote_params(number),
        name="project",
    )(a, b, weight)


def gather_rows(chips, number, rows, notes, gate_w, up_w):
    count, width = rows.shape
    a = jnp.concatenate([rows[:, : width // 2], notes], axis=1)
    b = rows[:, width // 2 :]
    slots, sems = spread_scratch(chips, a, b)
    return pl.pallas_call(
        functools.partial(gather_kernel, chips),
        out_shape=(
            jax.ShapeDtypeStruct((chips * count, width), jnp.bfloat16),
            jax.ShapeDtypeStruct((chips * count, LANES), jnp.bfloat16),
            jax.ShapeDtypeStruct((chips * count, gate_w.shape[1]), jnp.bfloat16),
        ),
        in_specs=[whole()] * 4,
        out_specs=(whole(),) * 3,
        scratch_shapes=slots + sems,
        compiler_params=remote_params(number),
        name="gather_rows",
    )(a, b, gate_w, up_w)


def down_project(chips, number, hidden, gain, weight):
    count, lanes = hidden.shape
    a, b = hidden[: count // 2], hidden[count // 2 :]
    slots, sems = spread_scratch(chips, a, b)
    tile = pltpu.VMEM((chips, count // chips, lanes), jnp.bfloat16)
    return pl.pallas_call(
        functools.partial(down_kernel, chips),
        out_shape=jax.ShapeDtypeStruct((count // chips, chips * lanes), jnp.bfloat16),
        in_specs=[whole()] * 4,
        out_specs=whole(),
        scratch_shapes=slots + [tile, tile] + sems + [pltpu.SemaphoreType.DMA((chips,))] * 2,
        compiler_params=remote_params(number),
        name="down_project",
    )(a, b, gain[None, :], weight)


def stick_kernel(lens_ref, q_ref, k_ref, v_ref, bias_ref, out_ref):
    step = pl.program_id(0)
    batch, span, _ = k_ref.shape
    blocks = span // LANES
    row = lax.broadcasted_iota(jnp.int32, (3 * LANES, LANES), 0)
    column = lax.broadcasted_iota(jnp.int32, (3 * LANES, LANES), 1)
    after = (lax.rem(row, LANES) > column).astype(jnp.bfloat16)
    place = lax.broadcasted_iota(jnp.int32, (HEADS, span), 1)
    bias = bias_ref[:, :1]
    group = HEADS // KV_HEADS
    head = lax.broadcasted_iota(jnp.int32, (HEADS, LANES), 0)
    lane = lax.broadcasted_iota(jnp.int32, (HEADS, LANES), 1)
    own_lanes = (head // group) == (lane // HEAD_DIM)
    late = lax.broadcasted_iota(jnp.int32, (HEADS, HEAD_DIM), 0) >= group
    for item in range(batch):
        heads = q_ref[item].astype(jnp.float32)
        heads = jnp.where(own_lanes, jnp.concatenate([heads] * KV_HEADS, axis=1), 0.0)
        scores = lax.dot_general(
            heads.astype(jnp.bfloat16), k_ref[item], (((1,), (1,)), ((), ())), preferred_element_type=jnp.float32
        )
        scores = scores * HEAD_DIM ** (-0.5) + bias
        live = place < lens_ref[step * batch + item]
        remain = -(jnp.maximum(scores, 0.0) + jnp.log1p(jnp.exp(-jnp.abs(scores))))
        log_remain = jnp.where(live, remain, 0.0)
        stacked = jnp.concatenate(
            [log_remain[:, n * LANES : (n + 1) * LANES] for n in range(blocks)], axis=0
        )
        high = stacked.astype(jnp.bfloat16)
        rest = stacked - high.astype(jnp.float32)
        middle = rest.astype(jnp.bfloat16)
        low = (rest - middle.astype(jnp.float32)).astype(jnp.bfloat16)
        within = jnp.dot(
            jnp.concatenate([high, middle, low], axis=1), after, preferred_element_type=jnp.float32
        )
        totals = jnp.sum(stacked, axis=1, keepdims=True)
        carried = jnp.zeros((HEADS, 1), jnp.float32)
        pieces = [None] * blocks
        for n in range(blocks - 1, -1, -1):
            pieces[n] = within[n * HEADS : (n + 1) * HEADS] + carried
            carried = carried + totals[n * HEADS : (n + 1) * HEADS]
        remain_after = jnp.concatenate(pieces, axis=1)
        weights = jnp.where(live, jnp.exp(scores + remain + remain_after), 0.0)
        mixed = jnp.dot(
            weights.astype(jnp.bfloat16), v_ref[item], preferred_element_type=jnp.float32
        )
        mixed = jnp.where(late, mixed[:, HEAD_DIM:], mixed[:, :HEAD_DIM])
        out_ref[item] = mixed.astype(jnp.bfloat16)


def stick_read(queries, key_cache, value_cache, lengths, head_bias):
    batch, span, lanes = key_cache.shape
    heads = queries.reshape(batch, HEADS, HEAD_DIM)
    each = min(4, batch)
    mixed = pl.pallas_call(
        stick_kernel,
        out_shape=jax.ShapeDtypeStruct((batch, HEADS, HEAD_DIM), jnp.bfloat16),
        grid=(batch // each,),
        in_specs=[
            pl.BlockSpec(memory_space=pltpu.SMEM),
            pl.BlockSpec((each, HEADS, HEAD_DIM), lambda i: (i, 0, 0)),
            pl.BlockSpec((each, span, lanes), lambda i: (i, 0, 0)),
            pl.BlockSpec((each, span, lanes), lambda i: (i, 0, 0)),
            pl.BlockSpec((HEADS, LANES), lambda i: (0, 0)),
        ],
        out_specs=pl.BlockSpec((each, HEADS, HEAD_DIM), lambda i: (i, 0, 0)),
        name="stick_read",
    )(lengths, heads, key_cache, value_cache, jnp.broadcast_to(head_bias[:, None], (HEADS, LANES)))
    return mixed.reshape(batch, HEADS * HEAD_DIM)


def shards(
    tokens,
    cache_keys,
    cache_values,
    cache_len,
    norm_gain_first,
    w_query,
    w_key,
    w_value,
    head_bias,
    w_output,
    norm_gain_second,
    group_id,
    member,
    group_gate,
    member_weight,
    expert_gate_w,
    expert_up_w,
    expert_down_w,
    dense_gate_w,
    dense_up_w,
    hidden_gain,
    dense_down_w,
    branch_logit,
):
    devices = lax.axis_size("ep")
    chips = devices // 2
    me = lax.axis_index("ep")
    first = lax.rem(me, 2) == 0
    partner = [(i, i + 1 - 2 * (i % 2)) for i in range(devices)]
    seq_dev, width = tokens.shape

    def both(own):
        other = lax.ppermute(own, "ep", partner)
        return jnp.where(
            first, jnp.concatenate([own, other], axis=-1), jnp.concatenate([other, own], axis=-1)
        )

    query_w = both(w_query)
    output_w = both(w_output)
    gate_w = both(dense_gate_w)
    up_w = both(dense_up_w)
    down_w = both(dense_down_w)

    stream = tokens.astype(jnp.float32)
    normed_first = (stream * rms_scale(stream) * norm_gain_first).astype(jnp.bfloat16)
    new_keys = jnp.dot(normed_first, w_key, preferred_element_type=jnp.float32).astype(jnp.bfloat16)
    new_values = jnp.dot(normed_first, w_value, preferred_element_type=jnp.float32).astype(
        jnp.bfloat16
    )
    queries = project(chips, 1, normed_first, query_w)
    attended = stick_read(queries, cache_keys, cache_values, cache_len, head_bias)
    projected = project(chips, 2, attended, output_w)
    second_stream = stream + projected.astype(jnp.float32)
    normed_second = (second_stream * rms_scale(second_stream) * norm_gain_second).astype(
        jnp.bfloat16
    )

    experts = devices * expert_gate_w.shape[0]
    capacity = seq_dev // (experts // PER_GROUP)
    notes = jnp.concatenate(
        [member, group_id[:, None], jnp.zeros((seq_dev, LANES - TOP_K - 1), jnp.int32)], axis=1
    ).astype(jnp.bfloat16)
    own_rows, own_notes, hidden = gather_rows(chips, 3, normed_second, notes, gate_w, up_w)
    other_rows = lax.ppermute(own_rows, "ep", partner)
    other_notes = lax.ppermute(own_notes, "ep", partner)
    dense_out = down_project(chips, 4, hidden, hidden_gain, down_w)

    def selection(rows_notes, parity):
        table = rows_notes[:, : TOP_K + 1].astype(jnp.int32)
        named = table[:, TOP_K :] * PER_GROUP + table[:, :TOP_K]
        hits = jnp.any(named == me, axis=1).reshape(chips, seq_dev)
        index = jnp.arange(seq_dev)
        earlier = (index[:, None] < index[None, :]).astype(jnp.float32)
        slot = jnp.dot(hits.astype(jnp.float32), earlier).astype(jnp.int32)
        spot = ((jnp.arange(chips)[:, None] * 2 + parity) * capacity + slot).reshape(-1)
        spot = jnp.where(hits.reshape(-1), spot, -1)
        return (jnp.arange(devices * capacity)[:, None] == spot[None, :]).astype(jnp.bfloat16)

    parity = lax.rem(me, 2)
    packed = jnp.dot(selection(own_notes, parity), own_rows, preferred_element_type=jnp.float32)
    packed = packed + jnp.dot(
        selection(other_notes, 1 - parity), other_rows, preferred_element_type=jnp.float32
    )
    packed = packed.astype(jnp.bfloat16)
    gate_pre = jnp.dot(packed, expert_gate_w[0], preferred_element_type=jnp.float32)
    upper_pre = jnp.dot(packed, expert_up_w[0], preferred_element_type=jnp.float32)
    expert_hidden = (jax.nn.silu(gate_pre) * upper_pre).astype(jnp.bfloat16)
    served = jnp.dot(expert_hidden, expert_down_w[0], preferred_element_type=jnp.float32).astype(
        jnp.bfloat16
    )
    returned = lax.all_to_all(
        served.reshape(devices, capacity, width), "ep", split_axis=0, concat_axis=0, tiled=True
    ).reshape(experts * capacity, width)

    pair_expert = (group_id[:, None] * PER_GROUP + member).reshape(-1)
    pair_count = pair_expert.shape[0]
    expert_hits = (pair_expert[:, None] == jnp.arange(experts, dtype=jnp.int32)[None, :]).astype(
        jnp.float32
    )
    earlier = (jnp.arange(pair_count)[:, None] > jnp.arange(pair_count)[None, :]).astype(
        jnp.float32
    )
    before = jnp.dot(earlier, expert_hits, preferred_element_type=jnp.float32)
    slot_index = jnp.sum(before * expert_hits, axis=1).astype(jnp.int32)
    target = pair_expert * capacity + slot_index
    select = (target[:, None] == jnp.arange(experts * capacity, dtype=jnp.int32)[None, :]).astype(
        jnp.bfloat16
    )
    pair_out = jnp.dot(select, returned, preferred_element_type=jnp.float32)
    combine = (group_gate[:, None] * member_weight).reshape(-1, 1)
    routed = jnp.sum((pair_out * combine).reshape(seq_dev, TOP_K, width), axis=1)
    mixed_out = (
        second_stream + routed + jax.nn.sigmoid(branch_logit) * dense_out.astype(jnp.float32)
    )
    return (mixed_out.astype(jnp.bfloat16), new_keys, new_values)


LOG2E = 1.4426950408889634
DEAD = -1e30
BATCHES = 2
TRANSPOSED = (((1,), (1,)), ((), ()))
ORDERS = (("x", "y"), ("y", "x"))


def dot_t(a, b):
    return lax.dot_general(a, b, TRANSPOSED, preferred_element_type=jnp.float32)


def dot(a, b):
    return jnp.dot(a, b, preferred_element_type=jnp.float32)


def remote(src, dst, send, recv, device):
    return pltpu.make_async_remote_copy(
        src_ref=src, dst_ref=dst, send_sem=send, recv_sem=recv, device_id=device, device_id_type=MESH
    )


class Grid(Place):
    def __init__(self, chips):
        super().__init__(chips)
        self.partner = (self.chip * 2 + 1 - self.core,)
        self.depth = self.dims[0]
        self.plane = chips // self.depth

    def on(self, z, dy=0, dx=0):
        depth, height, width = self.dims
        y = lax.rem(self.y + dy, height)
        x = lax.rem(self.x + dx, width)
        return (z * height + y) * width + x

    def turn(self, axis):
        return (1, 0) if axis == "y" else (0, 1)

    def sweep(self, step):
        toward = 1 - 2 * (self.z // (self.depth // 2))
        return lax.rem(self.z + step * toward + self.depth, self.depth)

    def enter(self):
        barrier = pltpu.get_barrier_semaphore()
        for step in range(1, self.chips):
            other = lax.rem(self.chip + step, self.chips)
            pl.semaphore_signal(barrier, inc=1, device_id=self.device(other), device_id_type=MESH)
        pl.semaphore_signal(barrier, inc=1, device_id=self.partner, device_id_type=MESH)
        pl.semaphore_wait(barrier, self.chips)


class Clock:
    def __init__(self):
        self.now = 0.0

    def spend(self, time):
        self.now += time

    def run(self, batches):
        ready = {batch: 0.0 for batch in batches}
        while ready:
            batch = min(ready, key=lambda b: (max(ready[b], self.now), batches.index(b)))
            self.now = max(self.now, ready[batch])
            following = next(batch, None)
            if following is None:
                del ready[batch]
            else:
                ready[batch] = following


class Gather:
    def __init__(self, place, clock, send, recv, groups, pieces):
        self.place = place
        self.clock = clock
        self.send = send
        self.recv = recv
        self.groups = groups
        self.pieces = pieces

    def copy(self, piece, origin, index, target):
        view = self.pieces[piece](origin)
        return remote(view, view, self.send.at[piece], self.recv.at[piece, index], self.place.device(target))

    def several(self, piece, count, index):
        view = self.pieces[piece](pl.ds(0, count))
        return remote(view, view, self.send.at[piece], self.recv.at[piece, index],
                      self.place.device(self.place.chip))

    def turns(self, piece):
        first, second = ORDERS[piece]
        return self.place.turn(first), self.place.turn(second)

    def last(self, step):
        return 2 * self.place.depth + step * self.groups // self.place.depth

    def across(self, piece, step):
        place = self.place
        first, second = self.turns(piece)
        z = place.sweep(step)
        self.copy(piece, place.on(z), place.depth + z, place.on(place.z, *first)).start()
        self.copy(piece, place.on(z), self.last(step), place.on(place.z, *second)).start()

    def corner(self, piece, step):
        place = self.place
        first, second = self.turns(piece)
        z = place.sweep(step)
        origin = place.on(z, *first)
        self.copy(piece, origin, place.depth + z, place.chip).wait_recv()
        self.copy(piece, origin, self.last(step), place.on(place.z, *second)).start()

    def steps(self):
        place, depth = self.place, self.place.depth
        every = range(len(self.pieces))
        begin = self.begin = self.clock.now
        for step in range(1, depth):
            for piece in every:
                self.copy(piece, place.chip, place.z, place.on(place.sweep(step))).start()
        for piece in every:
            self.across(piece, 0)
        self.clock.spend(0.1)
        yield begin + 3.0
        for piece in every:
            self.corner(piece, 0)
        for step in range(1, depth):
            yield begin + 2.6 + 1.1 * step
            for piece in every:
                z = place.sweep(step)
                self.copy(piece, place.on(z), z, place.chip).wait_recv()
                self.across(piece, step)
        for step in range(1, depth):
            yield begin + 5.0 + 1.1 * step
            for piece in every:
                self.corner(piece, step)

    def rest(self, group):
        for piece in range(len(self.pieces)):
            self.several(piece, 2 * self.place.depth // self.groups, 2 * self.place.depth + group).wait_recv()

    def due(self, group):
        return self.begin + 7.5 + 1.1 * ((group + 1) * self.place.depth // self.groups - 1)

    def finish(self):
        for piece in range(len(self.pieces)):
            self.several(piece, self.place.chips - 1, 0).wait_send()


def norm_rows(values, gain):
    square = jnp.mean(values * values, axis=-1, keepdims=True)
    return (values * lax.rsqrt(square + epsilon) * gain).astype(jnp.bfloat16)


def layer_kernel(
    chips, names,
    lens_ref, ids_ref, bias_ref, tokens_ref, gain1_ref, gain2_ref, hgain_ref, logit_ref,
    member_ref, mweight_ref, group_ref, ggate_ref,
    keys_hbm, values_hbm, wq_hbm, wo_hbm, wg_hbm, wu_hbm, wd_hbm, wk_hbm, wv_hbm, eg_hbm, eu_hbm, ed_hbm,
    out_ref, newk_ref, newv_ref,
    *scratch,
):
    s = types.SimpleNamespace(**dict(zip(names, scratch)))
    place = Grid(chips)
    clock = Clock()
    me = place.chip * 2 + place.core
    chip, core, z, depth, plane = place.chip, place.core, place.z, place.depth, place.plane
    tokens, width = tokens_ref.shape
    seq = tokens // BATCHES
    half = width // 2
    rows = chips * seq
    lanes = LANES
    experts = chips * 2
    part = plane * seq
    bf16, f32 = jnp.bfloat16, jnp.float32
    cut = lanes + half
    chunk = width // 4
    group = me // PER_GROUP

    own_rows = pl.ds(pl.multiple_of(core * (lanes // 2), lanes // 2), lanes // 2)
    spot_me = lax.rem(chip, plane)
    weights = (
        (s.wq.at[own_rows], wq_hbm), (s.wo.at[spot_me, core], wo_hbm),
        (s.wg.at[own_rows], wg_hbm), (s.wu.at[own_rows], wu_hbm),
    )
    waiting = {}

    def fetch(key, src, dst):
        copy = pltpu.make_async_copy(src, dst, s.local_sem.at[len([k for k in waiting if k < 20])])
        copy.start()
        waiting[key] = copy.wait

    ended = set()

    def need(*keys):
        for key in keys:
            if key not in ended:
                ended.add(key)
                waiting[key]()

    for i, (dst, src) in enumerate(weights):
        fetch(i, src, dst)
    fetch(4, wk_hbm, s.wk)
    fetch(5, wv_hbm, s.wv)
    fetch(6, keys_hbm, s.keys)
    fetch(7, values_hbm, s.values)
    fetch(8, eg_hbm.at[0], s.eg)
    fetch(9, eu_hbm.at[0], s.eu)
    fetch(10, ed_hbm.at[0], s.ed)

    place_of = lax.broadcasted_iota(jnp.int32, (lanes, tokens), 0)
    expert = lax.rem(place_of, experts)
    combine = jnp.zeros((lanes, tokens), f32)
    for k in range(TOP_K):
        named = group_ref[...] * PER_GROUP + member_ref[k : k + 1, :]
        weight = ggate_ref[...] * mweight_ref[k : k + 1, :]
        combine = jnp.where(expert == named, weight, combine)
    high = combine.astype(bf16).astype(f32)
    notes = jnp.where(place_of < experts, high, jnp.where(place_of < 2 * experts, combine - high, 0.0))
    square = (tokens, tokens)
    row, column = (lax.broadcasted_iota(jnp.int32, square, axis) for axis in (0, 1))
    forward = backward = jnp.zeros(square, f32)
    order = [0] * tokens
    later = 0
    for token in range(tokens):
        named = ids_ref[token]
        slot = named * (seq + later) + (1 - named) * (token - later)
        later = later + named
        forward = jnp.where((row == slot) & (column == token), 1.0, forward)
        backward = jnp.where((row == token) & (column == slot), 1.0, backward)
        order = [jnp.where(slot == k, token, order[k]) for k in range(tokens)]
    forward, backward = forward.astype(bf16), backward.astype(bf16)
    notes = dot_t(forward, notes.astype(bf16)).astype(bf16)
    sorted_tokens = dot(forward, tokens_ref[...]).astype(bf16)
    for b in range(BATCHES):
        s.slots1[b, chip, :, :lanes] = notes[b * seq : (b + 1) * seq]
        s.slots1[b, chip, :, lanes:] = sorted_tokens[b * seq : (b + 1) * seq]

    span = s.keys.shape[1]
    blocks = span // lanes
    row = lax.broadcasted_iota(jnp.int32, (2 * lanes, 2 * lanes), 0)
    column = lax.broadcasted_iota(jnp.int32, (2 * lanes, 2 * lanes), 1)
    s.after[...] = jnp.where((lax.rem(row, lanes) > column) | (column >= lanes), 1.0, 0.0).astype(bf16)
    head_row = lax.broadcasted_iota(jnp.int32, (HEADS, lanes), 0)
    bias = jnp.zeros((HEADS, lanes), f32)
    for head in range(HEADS):
        bias = jnp.where(head_row == (head % 2) * chips + head // 2, bias_ref[head] * LOG2E, bias)
    s.bias[...] = bias

    place.enter()

    swaps = [
        remote(src, dst, s.swap_send.at[i], s.swap_recv.at[i], place.partner)
        for i, (dst, src) in enumerate(weights)
    ]
    for i, swap in enumerate(swaps):
        waiting[20 + i] = swap.wait_recv

    def down_line(zo):
        columns = pl.ds(pl.multiple_of(zo * plane * lanes, plane * lanes), plane * lanes)
        return wd_hbm.at[:, columns], s.transit.at[z]

    def down_cut(position):
        columns = pl.ds(pl.multiple_of(position * lanes, lanes), lanes)
        return s.transit.at[:, :, columns], s.wd.at[:, spot_me, core]

    def down_across():
        need(11)
        arrived(s.transit.at[pl.ds(0, depth - 1)], s.down_recv.at[0])
        for turn in peers:
            target = place.on(z, *turn)
            remote(*down_cut(lax.rem(target, plane)), s.down_send.at[1], s.down_recv.at[1],
                   place.device(target)).start()
        fetch(12, *down_cut(spot_me))

    peers = ((0, 1), (1, 0), (1, 1))

    def wide_copy(index, target):
        return remote(wo_hbm, s.wo.at[spot_me, core], s.wide_send.at[0], s.wide_recv.at[index], place.device(target))

    def wide_pass(index):
        view = s.wo.at[lax.rem(place.on(z, *peers[index]), plane), core]
        arrived(view, s.wide_recv.at[index])
        remote(view, view, s.pass_send.at[0], s.pass_recv.at[0], place.partner).start()

    def spot(of):
        return lax.rem(of, plane) * depth + of // plane

    down_swap = remote(s.wd.at[:, :, core], s.wd.at[:, :, core], s.swap_send.at[4], s.swap_recv.at[4], place.partner)
    waiting[24] = down_swap.wait_recv

    def arrived(view, recv):
        remote(view, view, s.down_send.at[0], recv, place.device(chip)).wait_recv()

    def departed(view, send):
        return remote(view, view, send, s.down_recv.at[0], place.device(chip)).wait_send

    def others():
        return [lax.rem(chip + step, chips) for step in range(1, chips)]

    others_ds = pl.ds(0, chips - 1)

    def attend(b, item):
        jrow = lax.broadcasted_iota(jnp.int32, (chips, lanes), 0)
        jlane = lax.broadcasted_iota(jnp.int32, (chips, lanes), 1)
        early = jrow < chips // KV_HEADS
        own = (jlane // HEAD_DIM) == (jrow // (chips // KV_HEADS))
        even = s.heads[b, item]
        turned = pltpu.roll(even, HEAD_DIM, axis=1)
        query = jnp.concatenate([
            jnp.where(own, jnp.where(early, even, turned), 0.0),
            jnp.where(own, jnp.where(early, turned, even), 0.0),
        ], axis=0).astype(bf16)
        index = order[b * seq + item]
        scores = dot_t(query, s.keys[index]) * (HEAD_DIM ** (-0.5) * LOG2E)
        scores = scores + jnp.concatenate([s.bias[...]] * blocks, axis=1)
        position = lax.broadcasted_iota(jnp.int32, (HEADS, span), 1)
        scores = jnp.where(position < lens_ref[index], scores, DEAD)
        soft = jnp.maximum(scores, 0.0) + jnp.log(1.0 + jnp.exp2(-jnp.abs(scores))) * LOG2E
        stacked = jnp.concatenate([soft[:, n * lanes : (n + 1) * lanes] for n in range(blocks)], axis=0)
        top = stacked.astype(bf16)
        low = (stacked - top.astype(f32)).astype(bf16)
        sums = dot(jnp.concatenate([top, low], axis=1), s.after[...])
        carried = jnp.zeros((HEADS, lanes), f32)
        pieces = [None] * blocks
        for n in range(blocks - 1, -1, -1):
            band = sums[n * HEADS : (n + 1) * HEADS]
            spent = stacked[n * HEADS : (n + 1) * HEADS] + band[:, :lanes] + carried
            pieces[n] = jnp.exp2(scores[:, n * lanes : (n + 1) * lanes] - spent).astype(bf16)
            carried = carried + band[:, lanes:]
        found = dot(jnp.concatenate(pieces, axis=1), s.values[index])
        first, second = found[:chips], found[chips:]
        s.mixed[b, item] = jnp.where(
            jlane < HEAD_DIM,
            jnp.where(early, first, pltpu.roll(first, HEAD_DIM, axis=1)),
            jnp.where(early, pltpu.roll(second, HEAD_DIM, axis=1), second),
        )

    def columns_of(piece):
        return slice(piece * half, (piece + 1) * half)

    sends = []

    def batch(b):
        slots1, slots2, slots3 = s.slots1.at[b], s.slots2.at[b], s.slots3.at[b]
        gather = Gather(place, clock, s.gather_send.at[b, 0], s.gather_recv.at[b, 0], depth // 2, (
            lambda o: slots1.at[o, :, pl.ds(0, cut)],
            lambda o: slots1.at[o, :, pl.ds(cut, half)],
        ))
        sends.append(gather.finish)
        steps = gather.steps()
        yield next(steps)
        if b == 0:
            for swap in swaps:
                swap.start()
                sends.append(swap.wait_send)
        yield from steps

        tiles, landed = s.tiles.at[b], s.landed.at[b]

        def tile_copy(target):
            return remote(tiles.at[target], landed.at[chip], s.tile_send.at[b], s.tile_recv.at[b],
                          place.device(target))

        for pair in range(depth // 2):
            yield gather.due(pair)
            need(0, 20)
            gather.rest(pair)
            planes = []
            for step in (2 * pair, 2 * pair + 1):
                zo = place.sweep(step)
                planes.append(slots1[pl.ds(zo * plane, plane), :, lanes:].reshape(part, width))
            normed = norm_rows(jnp.concatenate(planes, axis=0).astype(f32), gain1_ref[...])
            product = dot_t(normed, s.wq[...]).astype(bf16).reshape(2, plane, seq, lanes)
            for side, step in enumerate((2 * pair, 2 * pair + 1)):
                zo = place.sweep(step)
                tiles[pl.ds(zo * plane, plane)] = product[side]
                for dy in (1, 0):
                    for dx in (1, 0):
                        if (step, dy, dx) != (0, 0, 0):
                            tile_copy(place.on(zo, dy, dx)).start()
            clock.spend(0.6)
        landed[chip] = tiles[chip]
        sends.append(departed(tiles.at[others_ds], s.tile_send.at[b]))
        begin = clock.now

        if b == BATCHES - 1:
            for index, turn in enumerate(peers):
                wide_copy(index, place.on(z, *turn)).start()
            for step in range(1, depth):
                zo = place.sweep(step)
                remote(*down_line(zo), s.down_send.at[0], s.down_recv.at[0], place.device(place.on(zo))).start()
            sends.append(departed(s.transit.at[pl.ds(0, depth - 1)], s.down_send.at[0]))
            sends.append(departed(s.wd.at[:, pl.ds(0, 3), 0], s.down_send.at[1]))
            sends.append(departed(s.wo.at[pl.ds(0, 3), 0], s.wide_send.at[0]))
            sends.append(departed(s.wo.at[pl.ds(0, 3), 0], s.pass_send.at[0]))
            fetch(11, *down_line(z))
            need(4, 5)
            own_normed = norm_rows(tokens_ref[...].astype(f32), gain1_ref[...])
            newk_ref[...] = dot(own_normed, s.wk[...]).astype(bf16)
            newv_ref[...] = dot(own_normed, s.wv[...]).astype(bf16)
            clock.spend(0.4)
        yield begin + 4.0
        arrived(landed.at[others_ds], s.tile_recv.at[b])
        for j in range(chips):
            s.heads[b, :, j, :] = landed[j].astype(f32)
        need(6, 7)
        for item in range(seq):
            attend(b, item)
            if item % 2 == 1:
                clock.spend(0.9)
                yield clock.now
        for j in range(chips):
            slots2[z, :, j * lanes : (j + 1) * lanes] = s.mixed[b, :, j, :].astype(bf16)
        clock.spend(0.1)

        begin = clock.now
        for step in range(depth - 1, 0, -1):
            remote(slots2.at[z], slots2.at[z], s.line_send.at[b], s.line_recv.at[b],
                   place.device(place.on(place.sweep(step)))).start()
        line_view = slots2.at[pl.ds(0, depth - 1)]
        sends.append(departed(line_view, s.line_send.at[b]))
        if b == 0:
            for index in range(3):
                yield begin + 0.9 + 0.9 * index
                if index == 0:
                    need(1)
                wide_pass(index)
            down_across()
        yield begin + (5.5 if b == 0 else 6.5)
        arrived(line_view, s.line_recv.at[b])
        need(21)
        if b == 0:
            arrived(s.wo.at[pl.ds(0, 3), 0], s.pass_recv.at[0])
        line_rows = slots2[...].reshape(depth * seq, width)
        product = dot_t(line_rows, s.wo[...].reshape(plane * lanes, width)).astype(bf16)
        slots3[chip] = product.reshape(depth, seq, plane * lanes)
        clock.spend(0.7)

        gather = Gather(place, clock, s.gather_send.at[b, 1], s.gather_recv.at[b, 0], 1, (
            lambda o: slots3.at[o, pl.ds(0, depth // 2)],
            lambda o: slots3.at[o, pl.ds(depth // 2, depth // 2)],
        ))
        sends.append(gather.finish)
        yield from gather.steps()
        if b == 0:
            need(12)
            arrived(s.wd.at[:, pl.ds(0, 3), core], s.down_recv.at[1])
            down_swap.start()
            sends.append(down_swap.wait_send)
        both = s.rows.at[b]
        acc = s.acc.at[b]

        def serve(c, lent):
            if lent:
                arrived(both.at[c], s.row_recv.at[b])
            every = both[c, :, :width]
            served = (jax.nn.silu(dot(every, s.eg[...])) * dot(every, s.eu[...])).astype(bf16)
            note_lane = lax.broadcasted_iota(jnp.int32, (rows, lanes), 1)
            mine = (note_lane == me) | (note_lane == me + experts)
            weight = jnp.sum(jnp.where(mine, both[c, :, width:].astype(f32), 0.0), axis=1, keepdims=True)
            for n in range(4):
                at = slice(n * chunk, (n + 1) * chunk)
                value = dot(served, s.ed[:, at])
                value = jnp.where(weight != 0.0, value * weight, 0.0)
                if lent:
                    s.gift[n] = value.astype(bf16)
                    remote(s.gift.at[n], s.given.at[n], s.gift_send.at[0], s.gift_recv.at[n // 2],
                           place.partner).start()
                else:
                    acc[:, :, at] = value.reshape(chips, seq, chunk)

        yield gather.due(0)
        need(8, 9, 10)
        gather.rest(0)

        block = rows // 2
        served_here = pl.when(group == b)
        line = depth * seq
        for n in range(2):
            at = slice(n * block, (n + 1) * block)
            for p in range(n * plane // 2, (n + 1) * plane // 2):
                of = slice(p * line, (p + 1) * line)
                token = jnp.concatenate(
                    [slots1[k * plane + p, :, lanes:].astype(f32) for k in range(depth)], axis=0)
                projected = jnp.concatenate(
                    [slots3[k * plane + p].reshape(line, plane * lanes) for k in range(depth)], axis=1)
                both[core, of, :width] = norm_rows(token + projected.astype(f32), gain2_ref[...])
                for k in range(depth):
                    both[core, p * line + k * seq : p * line + (k + 1) * seq, width:] = (
                        slots1[k * plane + p, :, :lanes])

            @served_here
            def _():
                remote(both.at[core, at], both.at[core, at], s.row_send.at[b], s.row_recv.at[b],
                       place.partner).start()

        clock.spend(0.4)

        need(2, 3, 22, 23)
        normed = both[core, :, :width]
        gate = dot_t(normed, s.wg[...])
        hidden = jax.nn.silu(gate) * dot_t(normed, s.wu[...])
        s.hidden[b] = hidden
        squares = s.squares.at[b]
        summed = jnp.broadcast_to(jnp.sum(hidden * hidden, axis=1, keepdims=True), (rows, lanes))
        squares[chip] = jnp.transpose(summed)[:1]

        def square_copy(target):
            return remote(squares.at[chip], squares.at[chip], s.square_send.at[b],
                          s.square_recv.at[b], place.device(target))

        for target in others():
            square_copy(target).start()
        sends.append(departed(squares.at[others_ds], s.square_send.at[b]))
        clock.spend(0.5)
        sent_at = clock.now

        for c in range(2):

            @pl.when((group == b) & (core == c))
            def _():
                serve(c, False)

        clock.spend(1.0)
        yield sent_at + 5.5

        @pl.when((group == b) & (core == 1))
        def _():
            serve(0, True)

        @pl.when((group == b) & (core == 0))
        def _():
            serve(1, True)

        clock.spend(0.6)

        def end_served():
            @pl.when(group == b)
            def _():
                departed(both.at[core], s.row_send.at[b])()
                departed(s.gift, s.gift_send.at[0])()

        sends.append(end_served)

        arrived(squares.at[others_ds], s.square_recv.at[b])
        total = squares[0]
        for c in range(1, chips):
            total = total + squares[c]
        scale = lax.rsqrt(total / width + epsilon)
        scale = jnp.transpose(jnp.broadcast_to(scale, (lanes, rows)))
        gain = hgain_ref[:, pl.ds(pl.multiple_of(chip * lanes, lanes), lanes)]
        dense = (s.hidden[b] * scale * gain).astype(bf16)
        need(24)

        stage = s.stage.at[b]

        def staged(piece, value, slot, index, recv, target):
            stage[piece, slot] = value.astype(bf16)
            remote(stage.at[piece, slot], s.sums.at[b, piece, index], s.sum_send.at[b, piece],
                   s.sum_recv.at[b, piece, recv], place.device(target)).start()

        def summands(piece, index, count, recv):
            view = s.sums.at[b, piece, pl.ds(index, count)]
            arrived(view, s.sum_recv.at[b, piece, recv])

        def summand(piece, index):
            return s.sums[b, piece, index].astype(f32)

        for piece in range(2):
            sends.append(departed(stage.at[piece, pl.ds(0, 4 * depth - 1)], s.sum_send.at[b, piece]))
            first, second = (place.turn(a) for a in ORDERS[piece])

            @served_here
            def _():
                arrived(s.given.at[pl.ds(2 * piece, 2)], s.gift_recv.at[piece])

            for c in (2 * piece, 2 * piece + 1):
                at = slice(c * chunk, (c + 1) * chunk)
                down = s.wd[c * depth // 4 : (c + 1) * depth // 4].reshape(chunk, lanes)
                value = jax.nn.sigmoid(logit_ref[:, at]) * dot_t(dense, down)
                value = value.reshape(chips, seq, chunk)

                @served_here
                def _():
                    acc[:, :, at] += s.given[c].astype(f32).reshape(chips, seq, chunk) + value

                @pl.when(group != b)
                def _():
                    acc[:, :, at] = value

            for beside in (1, 0):
                for step in range(depth - 1, -1, -1):
                    zo = place.sweep(step)
                    turn = (1, 1) if beside else first
                    index, recv = (zo, zo) if beside else (depth + 2 * zo, depth + zo)
                    staged(piece, acc[spot(place.on(zo, *turn)), :, columns_of(piece)], step * 2 + beside,
                           index, recv, place.on(z, *first))
        clock.spend(1.0)
        begin = clock.now

        for step in range(depth - 1, -1, -1):
            yield begin + 5.0 + 0.2 * (depth - 1 - step)
            for piece in range(2):
                first, second = (place.turn(a) for a in ORDERS[piece])
                zo = place.sweep(step)
                summands(piece, zo, 1, zo)
                value = acc[spot(place.on(zo, *second)), :, columns_of(piece)] + summand(piece, zo)
                staged(piece, value, 2 * depth + step, depth + 2 * zo + 1, depth + zo, place.on(z, *second))

        def folded(piece, zo):
            summands(piece, depth + 2 * zo, 2, depth + zo)
            value = acc[spot(place.on(zo)), :, columns_of(piece)] + summand(piece, depth + 2 * zo)
            return value + summand(piece, depth + 2 * zo + 1)

        for step in range(depth - 1, 0, -1):
            yield begin + 8.0 + 0.2 * (depth - 1 - step)
            for piece in range(2):
                zo = place.sweep(step)
                staged(piece, folded(piece, zo), 3 * depth + step - 1, 3 * depth + z, 2 * depth, place.on(zo))
        yield begin + 9.0
        for piece in range(2):
            at = columns_of(piece)
            value = slots1[chip, :, lanes + piece * half : lanes + (piece + 1) * half].astype(f32)
            value = value + jnp.concatenate(
                [slots3[k * plane + spot_me, z] for k in range(piece * depth // 2, (piece + 1) * depth // 2)], axis=1
            ).astype(f32)
            acc[spot(chip), :, at] = value + folded(piece, z)
        yield begin + 13.0
        for piece in range(2):
            summands(piece, 3 * depth, depth - 1, 2 * depth)
            value = acc[spot(chip), :, columns_of(piece)]
            for step in range(1, depth):
                value = value + summand(piece, 3 * depth + place.sweep(step))
            s.final[b * seq : (b + 1) * seq, columns_of(piece)] = value.astype(bf16)

    clock.run([batch(b) for b in range(BATCHES)])
    out_ref[...] = dot(backward, s.final[...]).astype(bf16)
    for end in sends:
        end()


def copy_kernel(a_ref, b_ref, c_ref, a_out, b_out, c_out):
    a_out[...] = a_ref[...]
    b_out[...] = b_ref[...]
    c_out[...] = c_ref[...]


def layer_scratch(chips, depth, tokens, width, span, fe):
    n = BATCHES
    seq = tokens // n
    rows = chips * seq
    bf16, f32, DMA = jnp.bfloat16, jnp.float32, pltpu.SemaphoreType.DMA
    half = width // 2
    return dict(
        slots1=pltpu.VMEM((n, chips, seq, LANES + width), bf16),
        slots2=pltpu.VMEM((n, depth, seq, width), bf16),
        slots3=pltpu.VMEM((n, chips, depth, seq, chips // depth * LANES), bf16),
        keys=pltpu.VMEM((tokens, span, LANES), bf16),
        values=pltpu.VMEM((tokens, span, LANES), bf16),
        wq=pltpu.VMEM((LANES, width), bf16),
        wo=pltpu.VMEM((chips // depth, 2, LANES // 2, width), bf16),
        wg=pltpu.VMEM((LANES, width), bf16),
        wu=pltpu.VMEM((LANES, width), bf16),
        wk=pltpu.VMEM((width, LANES), bf16),
        wv=pltpu.VMEM((width, LANES), bf16),
        eg=pltpu.VMEM((width, fe), bf16),
        eu=pltpu.VMEM((width, fe), bf16),
        ed=pltpu.VMEM((fe, width), bf16),
        wd=pltpu.VMEM((depth, chips // depth, 2, LANES // 2, LANES), bf16),
        transit=pltpu.VMEM((depth, LANES // 2, chips // depth * LANES), bf16),
        after=pltpu.VMEM((2 * LANES, 2 * LANES), bf16),
        bias=pltpu.VMEM((HEADS, LANES), f32),
        tiles=pltpu.VMEM((n, chips, seq, LANES), bf16),
        landed=pltpu.VMEM((n, chips, seq, LANES), bf16),
        heads=pltpu.VMEM((n, seq, chips, LANES), f32),
        mixed=pltpu.VMEM((n, seq, chips, LANES), f32),
        rows=pltpu.VMEM((n, 2, rows, width + LANES), bf16),
        final=pltpu.VMEM((tokens, width), bf16),
        hidden=pltpu.VMEM((n, rows, LANES), f32),
        squares=pltpu.VMEM((n, chips, 1, rows), f32),
        gift=pltpu.VMEM((4, rows, width // 4), bf16),
        given=pltpu.VMEM((4, rows, width // 4), bf16),
        acc=pltpu.VMEM((n, chips, seq, width), f32),
        stage=pltpu.VMEM((n, 2, 4 * depth, seq, half), bf16),
        sums=pltpu.VMEM((n, 2, 4 * depth, seq, half), bf16),
        local_sem=DMA((13,)),
        swap_send=DMA((5,)),
        swap_recv=DMA((5,)),
        gather_send=DMA((n, 2, 2)),
        gather_recv=DMA((n, 1, 2, 5 * depth // 2)),
        line_send=DMA((n,)),
        line_recv=DMA((n,)),
        wide_send=DMA((1,)),
        wide_recv=DMA((3,)),
        pass_send=DMA((1,)),
        pass_recv=DMA((1,)),
        tile_send=DMA((n,)),
        tile_recv=DMA((n,)),
        down_send=DMA((2,)),
        down_recv=DMA((2,)),
        square_send=DMA((n,)),
        square_recv=DMA((n,)),
        row_send=DMA((n,)),
        row_recv=DMA((n,)),
        gift_send=DMA((1,)),
        gift_recv=DMA((2,)),
        sum_send=DMA((n, 2)),
        sum_recv=DMA((n, 2, 2 * depth + 1)),
    )


def fused_shards(
    tokens, cache_keys, cache_values, cache_len, norm_gain_first, w_query, w_key, w_value, head_bias,
    w_output, norm_gain_second, group_id, member, group_gate, member_weight, expert_gate_w,
    expert_up_w, expert_down_w, dense_gate_w, dense_up_w, hidden_gain, dense_down_w, branch_logit,
):
    chips = lax.axis_size("ep") // 2
    seq, width = tokens.shape
    span = cache_keys.shape[1]
    bf16 = jnp.bfloat16
    scratch = layer_scratch(chips, torus_of(chips)[0], seq, width, span, expert_gate_w.shape[2])
    smem = pl.BlockSpec(memory_space=pltpu.SMEM)
    anywhere = pl.BlockSpec(memory_space=pl.ANY)
    out_shape = (
        jax.ShapeDtypeStruct((seq, width), bf16),
        jax.ShapeDtypeStruct((seq, LANES), bf16),
        jax.ShapeDtypeStruct((seq, LANES), bf16),
    )
    results = pl.pallas_call(
        functools.partial(layer_kernel, chips, tuple(scratch)),
        out_shape=out_shape,
        in_specs=[smem] * 3 + [whole()] * 9 + [anywhere] * 12,
        out_specs=(whole(),) * 3,
        scratch_shapes=list(scratch.values()),
        compiler_params=pltpu.CompilerParams(
            collective_id=1, has_side_effects=True, vmem_limit_bytes=60 * 1024 * 1024
        ),
        name="layer",
    )(
        cache_len, group_id, head_bias, tokens, norm_gain_first[None], norm_gain_second[None], hidden_gain[None],
        branch_logit[None], member.T, member_weight.T, group_id[None], group_gate[None],
        cache_keys, cache_values, w_query.T, w_output.T, dense_gate_w.T, dense_up_w.T, dense_down_w.T,
        w_key, w_value, expert_gate_w, expert_up_w, expert_down_w,
    )
    return pl.pallas_call(
        copy_kernel, out_shape=out_shape, in_specs=[whole()] * 3, out_specs=(whole(),) * 3, name="results"
    )(*results)


def one_kernel(mesh):
    chips = mesh.shape["ep"] // 2
    depth, height, width = torus_of(chips)
    return (height, width) == (2, 2) and chips * LANES == HEADS * HEAD_DIM and 4 * chips <= LANES and depth % 4 == 0 and 2 * chips == BATCHES * PER_GROUP


def solution(mesh):
    in_specs = (
        P("ep", None),
        P("ep", None, None),
        P("ep", None, None),
        P("ep"),
        P(),
        P(None, "ep"),
        P(),
        P(),
        P(),
        P(None, "ep"),
        P(),
        P("ep"),
        P("ep", None),
        P("ep"),
        P("ep", None),
        P("ep", None, None),
        P("ep", None, None),
        P("ep", None, None),
        P(None, "ep"),
        P(None, "ep"),
        P(),
        P(None, "ep"),
        P(),
    )
    out_specs = (P("ep", None), P("ep", None), P("ep", None))
    body = fused_shards if one_kernel(mesh) else shards
    return jax.shard_map(body, mesh=mesh, in_specs=in_specs, out_specs=out_specs, check_vma=False)
```

```python
import functools
import types

import jax
import jax.numpy as jnp
from jax import lax
from jax.experimental import pallas as pl
from jax.experimental.pallas import tpu as pltpu
from jax.sharding import PartitionSpec as P

HEADS = 32
HEAD_DIM = 64
KV_HEADS = 2
PER_GROUP = 16
TOP_K = 6
LANES = 128
MESH = pl.DeviceIdType.MESH

epsilon = 1e-06


def torus_of(chips):
    best = (chips, 1, 1)
    for x in range(1, chips + 1):
        for y in range(x, chips + 1):
            if chips % (x * y) == 0 and chips // (x * y) >= y:
                z = chips // (x * y)
                if z + y + x < sum(best):
                    best = (z, y, x)
    return best


def rms_scale(values):
    return lax.rsqrt(jnp.mean(values * values, axis=-1, keepdims=True) + epsilon)


class Place:
    def __init__(self, chips):
        self.chips = chips
        self.dims = torus_of(chips)
        me = lax.axis_index("ep")
        self.core = lax.rem(me, 2)
        self.chip = me // 2
        depth, height, width = self.dims
        self.x = lax.rem(self.chip, width)
        self.y = lax.rem(self.chip // width, height)
        self.z = self.chip // (width * height)

    def at(self, dz, dy, dx):
        depth, height, width = self.dims
        z = lax.rem(self.z + dz + depth, depth)
        y = lax.rem(self.y + dy + height, height)
        x = lax.rem(self.x + dx + width, width)
        return (z * height + y) * width + x

    def device(self, chip):
        return (chip * 2 + self.core,)

    def greet(self):
        barrier = pltpu.get_barrier_semaphore()
        for step in range(1, self.chips):
            other = lax.rem(self.chip + step, self.chips)
            pl.semaphore_signal(barrier, inc=1, device_id=self.device(other), device_id_type=MESH)
        pl.semaphore_wait(barrier, self.chips - 1)


def spread(place, halves):
    depth, height, width = place.dims
    sent = []
    counts = [0, 0]

    def push(half, source, origin, target):
        own, slots, send, recv = halves[half]
        copy = pltpu.make_async_remote_copy(
            src_ref=own if source is None else slots.at[source],
            dst_ref=slots.at[origin],
            send_sem=send.at[counts[half]],
            recv_sem=recv.at[origin],
            device_id=place.device(target),
            device_id_type=MESH,
        )
        counts[half] += 1
        copy.start()
        sent.append(copy)

    def arrive(half, origin):
        own, slots, send, recv = halves[half]
        pltpu.make_async_remote_copy(
            src_ref=slots.at[origin],
            dst_ref=slots.at[origin],
            send_sem=send.at[0],
            recv_sem=recv.at[origin],
            device_id=place.device(place.chip),
            device_id_type=MESH,
        ).wait_recv()

    def along(half, source, origin, axis):
        if axis == "x":
            for step in range(1, width):
                push(half, source, origin, place.at(0, 0, step))
        else:
            for step in range(1, height):
                push(half, source, origin, place.at(0, step, 0))

    orders = (("x", "y"), ("y", "x"))
    for step in range(1, depth):
        for half in range(2):
            push(half, None, place.chip, place.at(step, 0, 0))
    for half in range(2):
        for axis in orders[half]:
            along(half, None, place.chip, axis)
    for step in range(1, depth):
        for half in range(2):
            origin = place.at(-step, 0, 0)
            arrive(half, origin)
            for axis in orders[half]:
                along(half, origin, origin, axis)
    for up in range(depth):
        for half in range(2):
            reach = width if half == 0 else height
            for step in range(1, reach):
                origin = place.at(-up, 0, -step) if half == 0 else place.at(-up, -step, 0)
                arrive(half, origin)
                along(half, origin, origin, orders[half][1])
    for up in range(depth):
        for half in range(2):
            for dy in range(height):
                for dx in range(width):
                    if (dy if half == 0 else dx) != 0:
                        arrive(half, place.at(-up, -dy, -dx))
    for half in range(2):
        own, slots, _, _ = halves[half]
        slots[place.chip] = own[...]
    return sent


def deliver(place, tiles, landed, send, recv, out_ref):
    copies = []
    for step in range(1, place.chips):
        other = lax.rem(place.chip + step, place.chips)
        copy = pltpu.make_async_remote_copy(
            src_ref=tiles.at[other],
            dst_ref=landed.at[place.chip],
            send_sem=send.at[step],
            recv_sem=recv.at[place.chip],
            device_id=place.device(other),
            device_id_type=MESH,
        )
        copy.start()
        copies.append(copy)
    landed[place.chip] = tiles[place.chip]
    for step in range(1, place.chips):
        origin = lax.rem(place.chip - step + place.chips, place.chips)
        pltpu.make_async_remote_copy(
            src_ref=landed.at[origin],
            dst_ref=landed.at[origin],
            send_sem=send.at[0],
            recv_sem=recv.at[origin],
            device_id=place.device(place.chip),
            device_id_type=MESH,
        ).wait_recv()
    lanes = landed.shape[2]
    for block in range(place.chips):
        out_ref[:, block * lanes : (block + 1) * lanes] = landed[block]
    for copy in copies:
        copy.wait_send()


def flat(slots):
    count, rows, columns = slots.shape
    return slots[...].reshape(count * rows, columns)


def project_kernel(chips, a_ref, b_ref, w_ref, out_ref, slots_a, slots_b, tiles, landed,
                   send_a, recv_a, send_b, recv_b, send_t, recv_t):
    place = Place(chips)
    place.greet()
    sent = spread(place, ((a_ref, slots_a, send_a, recv_a), (b_ref, slots_b, send_b, recv_b)))
    cut = a_ref.shape[1]
    product = jnp.dot(flat(slots_a), w_ref[:cut], preferred_element_type=jnp.float32)
    product = product + jnp.dot(flat(slots_b), w_ref[cut:], preferred_element_type=jnp.float32)
    tiles[...] = product.astype(jnp.bfloat16).reshape(tiles.shape)
    deliver(place, tiles, landed, send_t, recv_t, out_ref)
    for copy in sent:
        copy.wait_send()


def gather_kernel(chips, a_ref, b_ref, gate_ref, up_ref, rows_ref, notes_ref, hidden_ref, slots_a, slots_b,
                  send_a, recv_a, send_b, recv_b):
    place = Place(chips)
    place.greet()
    sent = spread(place, ((a_ref, slots_a, send_a, recv_a), (b_ref, slots_b, send_b, recv_b)))
    cut = b_ref.shape[1]
    rows_a = slots_a[:, :, :cut].reshape(chips * a_ref.shape[0], cut)
    rows_b = flat(slots_b)
    rows_ref[:, :cut] = rows_a
    rows_ref[:, cut:] = rows_b
    notes_ref[...] = slots_a[:, :, cut:].reshape(notes_ref.shape)
    gate = jnp.dot(rows_a, gate_ref[:cut], preferred_element_type=jnp.float32)
    gate = gate + jnp.dot(rows_b, gate_ref[cut:], preferred_element_type=jnp.float32)
    upper = jnp.dot(rows_a, up_ref[:cut], preferred_element_type=jnp.float32)
    upper = upper + jnp.dot(rows_b, up_ref[cut:], preferred_element_type=jnp.float32)
    hidden_ref[...] = (jax.nn.silu(gate) * upper).astype(jnp.bfloat16)
    for copy in sent:
        copy.wait_send()


def down_kernel(chips, a_ref, b_ref, gain_ref, w_ref, out_ref, slots_a, slots_b, tiles, landed,
                send_a, recv_a, send_b, recv_b, send_t, recv_t):
    place = Place(chips)
    place.greet()
    sent = spread(place, ((a_ref, slots_a, send_a, recv_a), (b_ref, slots_b, send_b, recv_b)))
    rows, lanes = a_ref.shape
    part = chips // 2
    for half, slots in enumerate((slots_a, slots_b)):
        square = jnp.zeros((rows, lanes), jnp.float32)
        for block in range(chips):
            value = slots[block].astype(jnp.float32)
            square = square + value * value
        mean = jnp.sum(square, axis=1, keepdims=True) / (chips * lanes)
        scale = lax.rsqrt(mean + epsilon)
        total = jnp.zeros((rows, lanes), jnp.float32)
        for block in range(chips):
            gain = gain_ref[:, block * lanes : (block + 1) * lanes]
            normed = (slots[block].astype(jnp.float32) * scale * gain).astype(jnp.bfloat16)
            total = total + jnp.dot(
                normed,
                w_ref[block * lanes : (block + 1) * lanes],
                preferred_element_type=jnp.float32,
            )
        tiles[half * part : (half + 1) * part] = total.astype(jnp.bfloat16).reshape(
            part, rows // part, lanes
        )
    deliver(place, tiles, landed, send_t, recv_t, out_ref)
    for copy in sent:
        copy.wait_send()


def whole():
    return pl.BlockSpec(memory_space=pltpu.VMEM)


def spread_scratch(chips, a, b):
    slots = [pltpu.VMEM((chips,) + a.shape, a.dtype), pltpu.VMEM((chips,) + b.shape, b.dtype)]
    return slots, [pltpu.SemaphoreType.DMA((chips,))] * 4


def remote_params(number):
    return pltpu.CompilerParams(collective_id=number, has_side_effects=True)


def project(chips, number, rows, weight):
    count, width = rows.shape
    lanes = weight.shape[1]
    a, b = rows[:, : width // 2], rows[:, width // 2 :]
    slots, sems = spread_scratch(chips, a, b)
    tile = pltpu.VMEM((chips, count, lanes), jnp.bfloat16)
    return pl.pallas_call(
        functools.partial(project_kernel, chips),
        out_shape=jax.ShapeDtypeStruct((count, chips * lanes), jnp.bfloat16),
        in_specs=[whole()] * 3,
        out_specs=whole(),
        scratch_shapes=slots + [tile, tile] + sems + [pltpu.SemaphoreType.DMA((chips,))] * 2,
        compiler_params=remote_params(number),
        name="project",
    )(a, b, weight)


def gather_rows(chips, number, rows, notes, gate_w, up_w):
    count, width = rows.shape
    a = jnp.concatenate([rows[:, : width // 2], notes], axis=1)
    b = rows[:, width // 2 :]
    slots, sems = spread_scratch(chips, a, b)
    return pl.pallas_call(
        functools.partial(gather_kernel, chips),
        out_shape=(
            jax.ShapeDtypeStruct((chips * count, width), jnp.bfloat16),
            jax.ShapeDtypeStruct((chips * count, LANES), jnp.bfloat16),
            jax.ShapeDtypeStruct((chips * count, gate_w.shape[1]), jnp.bfloat16),
        ),
        in_specs=[whole()] * 4,
        out_specs=(whole(),) * 3,
        scratch_shapes=slots + sems,
        compiler_params=remote_params(number),
        name="gather_rows",
    )(a, b, gate_w, up_w)


def down_project(chips, number, hidden, gain, weight):
    count, lanes = hidden.shape
    a, b = hidden[: count // 2], hidden[count // 2 :]
    slots, sems = spread_scratch(chips, a, b)
    tile = pltpu.VMEM((chips, count // chips, lanes), jnp.bfloat16)
    return pl.pallas_call(
        functools.partial(down_kernel, chips),
        out_shape=jax.ShapeDtypeStruct((count // chips, chips * lanes), jnp.bfloat16),
        in_specs=[whole()] * 4,
        out_specs=whole(),
        scratch_shapes=slots + [tile, tile] + sems + [pltpu.SemaphoreType.DMA((chips,))] * 2,
        compiler_params=remote_params(number),
        name="down_project",
    )(a, b, gain[None, :], weight)


def stick_kernel(lens_ref, q_ref, k_ref, v_ref, bias_ref, out_ref):
    step = pl.program_id(0)
    batch, span, _ = k_ref.shape
    blocks = span // LANES
    row = lax.broadcasted_iota(jnp.int32, (3 * LANES, LANES), 0)
    column = lax.broadcasted_iota(jnp.int32, (3 * LANES, LANES), 1)
    after = (lax.rem(row, LANES) > column).astype(jnp.bfloat16)
    place = lax.broadcasted_iota(jnp.int32, (HEADS, span), 1)
    bias = bias_ref[:, :1]
    group = HEADS // KV_HEADS
    head = lax.broadcasted_iota(jnp.int32, (HEADS, LANES), 0)
    lane = lax.broadcasted_iota(jnp.int32, (HEADS, LANES), 1)
    own_lanes = (head // group) == (lane // HEAD_DIM)
    late = lax.broadcasted_iota(jnp.int32, (HEADS, HEAD_DIM), 0) >= group
    for item in range(batch):
        heads = q_ref[item].astype(jnp.float32)
        heads = jnp.where(own_lanes, jnp.concatenate([heads] * KV_HEADS, axis=1), 0.0)
        scores = lax.dot_general(
            heads.astype(jnp.bfloat16), k_ref[item], (((1,), (1,)), ((), ())), preferred_element_type=jnp.float32
        )
        scores = scores * HEAD_DIM ** (-0.5) + bias
        live = place < lens_ref[step * batch + item]
        remain = -(jnp.maximum(scores, 0.0) + jnp.log1p(jnp.exp(-jnp.abs(scores))))
        log_remain = jnp.where(live, remain, 0.0)
        stacked = jnp.concatenate(
            [log_remain[:, n * LANES : (n + 1) * LANES] for n in range(blocks)], axis=0
        )
        high = stacked.astype(jnp.bfloat16)
        rest = stacked - high.astype(jnp.float32)
        middle = rest.astype(jnp.bfloat16)
        low = (rest - middle.astype(jnp.float32)).astype(jnp.bfloat16)
        within = jnp.dot(
            jnp.concatenate([high, middle, low], axis=1), after, preferred_element_type=jnp.float32
        )
        totals = jnp.sum(stacked, axis=1, keepdims=True)
        carried = jnp.zeros((HEADS, 1), jnp.float32)
        pieces = [None] * blocks
        for n in range(blocks - 1, -1, -1):
            pieces[n] = within[n * HEADS : (n + 1) * HEADS] + carried
            carried = carried + totals[n * HEADS : (n + 1) * HEADS]
        remain_after = jnp.concatenate(pieces, axis=1)
        weights = jnp.where(live, jnp.exp(scores + remain + remain_after), 0.0)
        mixed = jnp.dot(
            weights.astype(jnp.bfloat16), v_ref[item], preferred_element_type=jnp.float32
        )
        mixed = jnp.where(late, mixed[:, HEAD_DIM:], mixed[:, :HEAD_DIM])
        out_ref[item] = mixed.astype(jnp.bfloat16)


def stick_read(queries, key_cache, value_cache, lengths, head_bias):
    batch, span, lanes = key_cache.shape
    heads = queries.reshape(batch, HEADS, HEAD_DIM)
    each = min(4, batch)
    mixed = pl.pallas_call(
        stick_kernel,
        out_shape=jax.ShapeDtypeStruct((batch, HEADS, HEAD_DIM), jnp.bfloat16),
        grid=(batch // each,),
        in_specs=[
            pl.BlockSpec(memory_space=pltpu.SMEM),
            pl.BlockSpec((each, HEADS, HEAD_DIM), lambda i: (i, 0, 0)),
            pl.BlockSpec((each, span, lanes), lambda i: (i, 0, 0)),
            pl.BlockSpec((each, span, lanes), lambda i: (i, 0, 0)),
            pl.BlockSpec((HEADS, LANES), lambda i: (0, 0)),
        ],
        out_specs=pl.BlockSpec((each, HEADS, HEAD_DIM), lambda i: (i, 0, 0)),
        name="stick_read",
    )(lengths, heads, key_cache, value_cache, jnp.broadcast_to(head_bias[:, None], (HEADS, LANES)))
    return mixed.reshape(batch, HEADS * HEAD_DIM)


def shards(
    tokens,
    cache_keys,
    cache_values,
    cache_len,
    norm_gain_first,
    w_query,
    w_key,
    w_value,
    head_bias,
    w_output,
    norm_gain_second,
    group_id,
    member,
    group_gate,
    member_weight,
    expert_gate_w,
    expert_up_w,
    expert_down_w,
    dense_gate_w,
    dense_up_w,
    hidden_gain,
    dense_down_w,
    branch_logit,
):
    devices = lax.axis_size("ep")
    chips = devices // 2
    me = lax.axis_index("ep")
    first = lax.rem(me, 2) == 0
    partner = [(i, i + 1 - 2 * (i % 2)) for i in range(devices)]
    seq_dev, width = tokens.shape

    def both(own):
        other = lax.ppermute(own, "ep", partner)
        return jnp.where(
            first, jnp.concatenate([own, other], axis=-1), jnp.concatenate([other, own], axis=-1)
        )

    query_w = both(w_query)
    output_w = both(w_output)
    gate_w = both(dense_gate_w)
    up_w = both(dense_up_w)
    down_w = both(dense_down_w)

    stream = tokens.astype(jnp.float32)
    normed_first = (stream * rms_scale(stream) * norm_gain_first).astype(jnp.bfloat16)
    new_keys = jnp.dot(normed_first, w_key, preferred_element_type=jnp.float32).astype(jnp.bfloat16)
    new_values = jnp.dot(normed_first, w_value, preferred_element_type=jnp.float32).astype(
        jnp.bfloat16
    )
    queries = project(chips, 1, normed_first, query_w)
    attended = stick_read(queries, cache_keys, cache_values, cache_len, head_bias)
    projected = project(chips, 2, attended, output_w)
    second_stream = stream + projected.astype(jnp.float32)
    normed_second = (second_stream * rms_scale(second_stream) * norm_gain_second).astype(
        jnp.bfloat16
    )

    experts = devices * expert_gate_w.shape[0]
    capacity = seq_dev // (experts // PER_GROUP)
    notes = jnp.concatenate(
        [member, group_id[:, None], jnp.zeros((seq_dev, LANES - TOP_K - 1), jnp.int32)], axis=1
    ).astype(jnp.bfloat16)
    own_rows, own_notes, hidden = gather_rows(chips, 3, normed_second, notes, gate_w, up_w)
    other_rows = lax.ppermute(own_rows, "ep", partner)
    other_notes = lax.ppermute(own_notes, "ep", partner)
    dense_out = down_project(chips, 4, hidden, hidden_gain, down_w)

    def selection(rows_notes, parity):
        table = rows_notes[:, : TOP_K + 1].astype(jnp.int32)
        named = table[:, TOP_K :] * PER_GROUP + table[:, :TOP_K]
        hits = jnp.any(named == me, axis=1).reshape(chips, seq_dev)
        index = jnp.arange(seq_dev)
        earlier = (index[:, None] < index[None, :]).astype(jnp.float32)
        slot = jnp.dot(hits.astype(jnp.float32), earlier).astype(jnp.int32)
        spot = ((jnp.arange(chips)[:, None] * 2 + parity) * capacity + slot).reshape(-1)
        spot = jnp.where(hits.reshape(-1), spot, -1)
        return (jnp.arange(devices * capacity)[:, None] == spot[None, :]).astype(jnp.bfloat16)

    parity = lax.rem(me, 2)
    packed = jnp.dot(selection(own_notes, parity), own_rows, preferred_element_type=jnp.float32)
    packed = packed + jnp.dot(
        selection(other_notes, 1 - parity), other_rows, preferred_element_type=jnp.float32
    )
    packed = packed.astype(jnp.bfloat16)
    gate_pre = jnp.dot(packed, expert_gate_w[0], preferred_element_type=jnp.float32)
    upper_pre = jnp.dot(packed, expert_up_w[0], preferred_element_type=jnp.float32)
    expert_hidden = (jax.nn.silu(gate_pre) * upper_pre).astype(jnp.bfloat16)
    served = jnp.dot(expert_hidden, expert_down_w[0], preferred_element_type=jnp.float32).astype(
        jnp.bfloat16
    )
    returned = lax.all_to_all(
        served.reshape(devices, capacity, width), "ep", split_axis=0, concat_axis=0, tiled=True
    ).reshape(experts * capacity, width)

    pair_expert = (group_id[:, None] * PER_GROUP + member).reshape(-1)
    pair_count = pair_expert.shape[0]
    expert_hits = (pair_expert[:, None] == jnp.arange(experts, dtype=jnp.int32)[None, :]).astype(
        jnp.float32
    )
    earlier = (jnp.arange(pair_count)[:, None] > jnp.arange(pair_count)[None, :]).astype(
        jnp.float32
    )
    before = jnp.dot(earlier, expert_hits, preferred_element_type=jnp.float32)
    slot_index = jnp.sum(before * expert_hits, axis=1).astype(jnp.int32)
    target = pair_expert * capacity + slot_index
    select = (target[:, None] == jnp.arange(experts * capacity, dtype=jnp.int32)[None, :]).astype(
        jnp.bfloat16
    )
    pair_out = jnp.dot(select, returned, preferred_element_type=jnp.float32)
    combine = (group_gate[:, None] * member_weight).reshape(-1, 1)
    routed = jnp.sum((pair_out * combine).reshape(seq_dev, TOP_K, width), axis=1)
    mixed_out = (
        second_stream + routed + jax.nn.sigmoid(branch_logit) * dense_out.astype(jnp.float32)
    )
    return (mixed_out.astype(jnp.bfloat16), new_keys, new_values)


LOG2E = 1.4426950408889634
DEAD = -1e30
BATCHES = 2
TRANSPOSED = (((1,), (1,)), ((), ()))
ORDERS = (("x", "y"), ("y", "x"))


def dot_t(a, b):
    return lax.dot_general(a, b, TRANSPOSED, preferred_element_type=jnp.float32)


def dot(a, b):
    return jnp.dot(a, b, preferred_element_type=jnp.float32)


def remote(src, dst, send, recv, device):
    return pltpu.make_async_remote_copy(
        src_ref=src, dst_ref=dst, send_sem=send, recv_sem=recv, device_id=device, device_id_type=MESH
    )


class Grid(Place):
    def __init__(self, chips):
        super().__init__(chips)
        self.partner = (self.chip * 2 + 1 - self.core,)
        self.depth = self.dims[0]
        self.plane = chips // self.depth

    def on(self, z, dy=0, dx=0):
        depth, height, width = self.dims
        y = lax.rem(self.y + dy, height)
        x = lax.rem(self.x + dx, width)
        return (z * height + y) * width + x

    def turn(self, axis):
        return (1, 0) if axis == "y" else (0, 1)

    def sweep(self, step):
        toward = 1 - 2 * (self.z // (self.depth // 2))
        return lax.rem(self.z + step * toward + self.depth, self.depth)

    def enter(self):
        barrier = pltpu.get_barrier_semaphore()
        for step in range(1, self.chips):
            other = lax.rem(self.chip + step, self.chips)
            pl.semaphore_signal(barrier, inc=1, device_id=self.device(other), device_id_type=MESH)
        pl.semaphore_signal(barrier, inc=1, device_id=self.partner, device_id_type=MESH)
        pl.semaphore_wait(barrier, self.chips)


class Clock:
    def __init__(self):
        self.now = 0.0

    def spend(self, time):
        self.now += time

    def run(self, batches):
        ready = {batch: 0.0 for batch in batches}
        while ready:
            batch = min(ready, key=lambda b: (max(ready[b], self.now), batches.index(b)))
            self.now = max(self.now, ready[batch])
            following = next(batch, None)
            if following is None:
                del ready[batch]
            else:
                ready[batch] = following


class Gather:
    def __init__(self, place, clock, send, recv, groups, pieces):
        self.place = place
        self.clock = clock
        self.send = send
        self.recv = recv
        self.groups = groups
        self.pieces = pieces

    def copy(self, piece, origin, index, target):
        view = self.pieces[piece](origin)
        return remote(view, view, self.send.at[piece], self.recv.at[piece, index], self.place.device(target))

    def several(self, piece, count, index):
        view = self.pieces[piece](pl.ds(0, count))
        return remote(view, view, self.send.at[piece], self.recv.at[piece, index],
                      self.place.device(self.place.chip))

    def turns(self, piece):
        first, second = ORDERS[piece]
        return self.place.turn(first), self.place.turn(second)

    def last(self, step):
        return 2 * self.place.depth + step * self.groups // self.place.depth

    def across(self, piece, step):
        place = self.place
        first, second = self.turns(piece)
        z = place.sweep(step)
        self.copy(piece, place.on(z), place.depth + z, place.on(place.z, *first)).start()
        self.copy(piece, place.on(z), self.last(step), place.on(place.z, *second)).start()

    def corner(self, piece, step):
        place = self.place
        first, second = self.turns(piece)
        z = place.sweep(step)
        origin = place.on(z, *first)
        self.copy(piece, origin, place.depth + z, place.chip).wait_recv()
        self.copy(piece, origin, self.last(step), place.on(place.z, *second)).start()

    def steps(self):
        place, depth = self.place, self.place.depth
        every = range(len(self.pieces))
        begin = self.begin = self.clock.now
        for step in range(1, depth):
            for piece in every:
                self.copy(piece, place.chip, place.z, place.on(place.sweep(step))).start()
        for piece in every:
            self.across(piece, 0)
        self.clock.spend(0.1)
        yield begin + 3.0
        for piece in every:
            self.corner(piece, 0)
        for step in range(1, depth):
            yield begin + 2.6 + 1.1 * step
            for piece in every:
                z = place.sweep(step)
                self.copy(piece, place.on(z), z, place.chip).wait_recv()
                self.across(piece, step)
        for step in range(1, depth):
            yield begin + 5.0 + 1.1 * step
            for piece in every:
                self.corner(piece, step)

    def rest(self, group):
        for piece in range(len(self.pieces)):
            self.several(piece, 2 * self.place.depth // self.groups, 2 * self.place.depth + group).wait_recv()

    def due(self, group):
        return self.begin + 7.5 + 1.1 * ((group + 1) * self.place.depth // self.groups - 1)

    def finish(self):
        for piece in range(len(self.pieces)):
            self.several(piece, self.place.chips - 1, 0).wait_send()


def norm_rows(values, gain):
    square = jnp.mean(values * values, axis=-1, keepdims=True)
    return (values * lax.rsqrt(square + epsilon) * gain).astype(jnp.bfloat16)


def layer_kernel(
    chips, names,
    lens_ref, ids_ref, bias_ref, tokens_ref, gain1_ref, gain2_ref, hgain_ref, logit_ref,
    member_ref, mweight_ref, group_ref, ggate_ref,
    keys_hbm, values_hbm, wq_hbm, wo_hbm, wg_hbm, wu_hbm, wd_hbm, wk_hbm, wv_hbm, eg_hbm, eu_hbm, ed_hbm,
    out_ref, newk_ref, newv_ref,
    *scratch,
):
    s = types.SimpleNamespace(**dict(zip(names, scratch)))
    place = Grid(chips)
    clock = Clock()
    me = place.chip * 2 + place.core
    chip, core, z, depth, plane = place.chip, place.core, place.z, place.depth, place.plane
    tokens, width = tokens_ref.shape
    seq = tokens // BATCHES
    half = width // 2
    rows = chips * seq
    lanes = LANES
    experts = chips * 2
    part = plane * seq
    bf16, f32 = jnp.bfloat16, jnp.float32
    cut = lanes + half
    chunk = width // 4
    group = me // PER_GROUP

    own_rows = pl.ds(pl.multiple_of(core * (lanes // 2), lanes // 2), lanes // 2)
    spot_me = lax.rem(chip, plane)
    weights = (
        (s.wq.at[own_rows], wq_hbm), (s.wo.at[spot_me, core], wo_hbm),
        (s.wg.at[own_rows], wg_hbm), (s.wu.at[own_rows], wu_hbm),
    )
    waiting = {}

    def fetch(key, src, dst):
        copy = pltpu.make_async_copy(src, dst, s.local_sem.at[len([k for k in waiting if k < 20])])
        copy.start()
        waiting[key] = copy.wait

    ended = set()

    def need(*keys):
        for key in keys:
            if key not in ended:
                ended.add(key)
                waiting[key]()

    for i, (dst, src) in enumerate(weights):
        fetch(i, src, dst)
    fetch(4, wk_hbm, s.wk)
    fetch(5, wv_hbm, s.wv)
    fetch(6, keys_hbm, s.keys)
    fetch(7, values_hbm, s.values)
    fetch(8, eg_hbm.at[0], s.eg)
    fetch(9, eu_hbm.at[0], s.eu)
    fetch(10, ed_hbm.at[0], s.ed)

    place_of = lax.broadcasted_iota(jnp.int32, (lanes, tokens), 0)
    expert = lax.rem(place_of, experts)
    combine = jnp.zeros((lanes, tokens), f32)
    for k in range(TOP_K):
        named = group_ref[...] * PER_GROUP + member_ref[k : k + 1, :]
        weight = ggate_ref[...] * mweight_ref[k : k + 1, :]
        combine = jnp.where(expert == named, weight, combine)
    high = combine.astype(bf16).astype(f32)
    notes = jnp.where(place_of < experts, high, jnp.where(place_of < 2 * experts, combine - high, 0.0))
    square = (tokens, tokens)
    row, column = (lax.broadcasted_iota(jnp.int32, square, axis) for axis in (0, 1))
    forward = backward = jnp.zeros(square, f32)
    order = [0] * tokens
    later = 0
    for token in range(tokens):
        named = ids_ref[token]
        slot = named * (seq + later) + (1 - named) * (token - later)
        later = later + named
        forward = jnp.where((row == slot) & (column == token), 1.0, forward)
        backward = jnp.where((row == token) & (column == slot), 1.0, backward)
        order = [jnp.where(slot == k, token, order[k]) for k in range(tokens)]
    forward, backward = forward.astype(bf16), backward.astype(bf16)
    notes = dot_t(forward, notes.astype(bf16)).astype(bf16)
    sorted_tokens = dot(forward, tokens_ref[...]).astype(bf16)
    for b in range(BATCHES):
        s.slots1[b, chip, :, :lanes] = notes[b * seq : (b + 1) * seq]
        s.slots1[b, chip, :, lanes:] = sorted_tokens[b * seq : (b + 1) * seq]

    span = s.keys.shape[1]
    blocks = span // lanes
    row = lax.broadcasted_iota(jnp.int32, (2 * lanes, 2 * lanes), 0)
    column = lax.broadcasted_iota(jnp.int32, (2 * lanes, 2 * lanes), 1)
    s.after[...] = jnp.where((lax.rem(row, lanes) > column) | (column >= lanes), 1.0, 0.0).astype(bf16)
    head_row = lax.broadcasted_iota(jnp.int32, (HEADS, lanes), 0)
    bias = jnp.zeros((HEADS, lanes), f32)
    for head in range(HEADS):
        bias = jnp.where(head_row == (head % 2) * chips + head // 2, bias_ref[head] * LOG2E, bias)
    s.bias[...] = bias

    place.enter()

    swaps = [
        remote(src, dst, s.swap_send.at[i], s.swap_recv.at[i], place.partner)
        for i, (dst, src) in enumerate(weights)
    ]
    for i, swap in enumerate(swaps):
        waiting[20 + i] = swap.wait_recv

    def down_line(zo):
        columns = pl.ds(pl.multiple_of(zo * plane * lanes, plane * lanes), plane * lanes)
        return wd_hbm.at[:, columns], s.transit.at[z]

    def down_cut(position):
        columns = pl.ds(pl.multiple_of(position * lanes, lanes), lanes)
        return s.transit.at[:, :, columns], s.wd.at[:, spot_me, core]

    def down_across():
        need(11)
        arrived(s.transit.at[pl.ds(0, depth - 1)], s.down_recv.at[0])
        for turn in peers:
            target = place.on(z, *turn)
            remote(*down_cut(lax.rem(target, plane)), s.down_send.at[1], s.down_recv.at[1],
                   place.device(target)).start()
        fetch(12, *down_cut(spot_me))

    peers = ((0, 1), (1, 0), (1, 1))

    def wide_copy(index, target):
        return remote(wo_hbm, s.wo.at[spot_me, core], s.wide_send.at[0], s.wide_recv.at[index], place.device(target))

    def wide_pass(index):
        view = s.wo.at[lax.rem(place.on(z, *peers[index]), plane), core]
        arrived(view, s.wide_recv.at[index])
        remote(view, view, s.pass_send.at[0], s.pass_recv.at[0], place.partner).start()

    def spot(of):
        return lax.rem(of, plane) * depth + of // plane

    down_swap = remote(s.wd.at[:, :, core], s.wd.at[:, :, core], s.swap_send.at[4], s.swap_recv.at[4], place.partner)
    waiting[24] = down_swap.wait_recv

    def arrived(view, recv):
        remote(view, view, s.down_send.at[0], recv, place.device(chip)).wait_recv()

    def departed(view, send):
        return remote(view, view, send, s.down_recv.at[0], place.device(chip)).wait_send

    def others():
        return [lax.rem(chip + step, chips) for step in range(1, chips)]

    others_ds = pl.ds(0, chips - 1)

    def attend(b, item):
        jrow = lax.broadcasted_iota(jnp.int32, (chips, lanes), 0)
        jlane = lax.broadcasted_iota(jnp.int32, (chips, lanes), 1)
        early = jrow < chips // KV_HEADS
        own = (jlane // HEAD_DIM) == (jrow // (chips // KV_HEADS))
        even = s.heads[b, item]
        turned = pltpu.roll(even, HEAD_DIM, axis=1)
        query = jnp.concatenate([
            jnp.where(own, jnp.where(early, even, turned), 0.0),
            jnp.where(own, jnp.where(early, turned, even), 0.0),
        ], axis=0).astype(bf16)
        index = order[b * seq + item]
        scores = dot_t(query, s.keys[index]) * (HEAD_DIM ** (-0.5) * LOG2E)
        scores = scores + jnp.concatenate([s.bias[...]] * blocks, axis=1)
        position = lax.broadcasted_iota(jnp.int32, (HEADS, span), 1)
        scores = jnp.where(position < lens_ref[index], scores, DEAD)
        soft = jnp.maximum(scores, 0.0) + jnp.log(1.0 + jnp.exp2(-jnp.abs(scores))) * LOG2E
        stacked = jnp.concatenate([soft[:, n * lanes : (n + 1) * lanes] for n in range(blocks)], axis=0)
        top = stacked.astype(bf16)
        low = (stacked - top.astype(f32)).astype(bf16)
        sums = dot(jnp.concatenate([top, low], axis=1), s.after[...])
        carried = jnp.zeros((HEADS, lanes), f32)
        pieces = [None] * blocks
        for n in range(blocks - 1, -1, -1):
            band = sums[n * HEADS : (n + 1) * HEADS]
            spent = stacked[n * HEADS : (n + 1) * HEADS] + band[:, :lanes] + carried
            pieces[n] = jnp.exp2(scores[:, n * lanes : (n + 1) * lanes] - spent).astype(bf16)
            carried = carried + band[:, lanes:]
        found = dot(jnp.concatenate(pieces, axis=1), s.values[index])
        first, second = found[:chips], found[chips:]
        s.mixed[b, item] = jnp.where(
            jlane < HEAD_DIM,
            jnp.where(early, first, pltpu.roll(first, HEAD_DIM, axis=1)),
            jnp.where(early, pltpu.roll(second, HEAD_DIM, axis=1), second),
        )

    def columns_of(piece):
        return slice(piece * half, (piece + 1) * half)

    sends = []

    def batch(b):
        slots1, slots2, slots3 = s.slots1.at[b], s.slots2.at[b], s.slots3.at[b]
        gather = Gather(place, clock, s.gather_send.at[b, 0], s.gather_recv.at[b, 0], depth // 2, (
            lambda o: slots1.at[o, :, pl.ds(0, cut)],
            lambda o: slots1.at[o, :, pl.ds(cut, half)],
        ))
        sends.append(gather.finish)
        steps = gather.steps()
        yield next(steps)
        if b == 0:
            for swap in swaps:
                swap.start()
                sends.append(swap.wait_send)
        yield from steps

        tiles, landed = s.tiles.at[b], s.landed.at[b]

        def tile_copy(target):
            return remote(tiles.at[target], landed.at[chip], s.tile_send.at[b], s.tile_recv.at[b],
                          place.device(target))

        for pair in range(depth // 2):
            yield gather.due(pair)
            need(0, 20)
            gather.rest(pair)
            planes = []
            for step in (2 * pair, 2 * pair + 1):
                zo = place.sweep(step)
                planes.append(slots1[pl.ds(zo * plane, plane), :, lanes:].reshape(part, width))
            normed = norm_rows(jnp.concatenate(planes, axis=0).astype(f32), gain1_ref[...])
            product = dot_t(normed, s.wq[...]).astype(bf16).reshape(2, plane, seq, lanes)
            for side, step in enumerate((2 * pair, 2 * pair + 1)):
                zo = place.sweep(step)
                tiles[pl.ds(zo * plane, plane)] = product[side]
                for dy in (1, 0):
                    for dx in (1, 0):
                        if (step, dy, dx) != (0, 0, 0):
                            tile_copy(place.on(zo, dy, dx)).start()
            clock.spend(0.6)
        landed[chip] = tiles[chip]
        sends.append(departed(tiles.at[others_ds], s.tile_send.at[b]))
        begin = clock.now

        if b == BATCHES - 1:
            for index, turn in enumerate(peers):
                wide_copy(index, place.on(z, *turn)).start()
            for step in range(1, depth):
                zo = place.sweep(step)
                remote(*down_line(zo), s.down_send.at[0], s.down_recv.at[0], place.device(place.on(zo))).start()
            sends.append(departed(s.transit.at[pl.ds(0, depth - 1)], s.down_send.at[0]))
            sends.append(departed(s.wd.at[:, pl.ds(0, 3), 0], s.down_send.at[1]))
            sends.append(departed(s.wo.at[pl.ds(0, 3), 0], s.wide_send.at[0]))
            sends.append(departed(s.wo.at[pl.ds(0, 3), 0], s.pass_send.at[0]))
            fetch(11, *down_line(z))
            need(4, 5)
            own_normed = norm_rows(tokens_ref[...].astype(f32), gain1_ref[...])
            newk_ref[...] = dot(own_normed, s.wk[...]).astype(bf16)
            newv_ref[...] = dot(own_normed, s.wv[...]).astype(bf16)
            clock.spend(0.4)
        yield begin + 4.0
        arrived(landed.at[others_ds], s.tile_recv.at[b])
        for j in range(chips):
            s.heads[b, :, j, :] = landed[j].astype(f32)
        need(6, 7)
        for item in range(seq):
            attend(b, item)
            if item % 2 == 1:
                clock.spend(0.9)
                yield clock.now
        for j in range(chips):
            slots2[z, :, j * lanes : (j + 1) * lanes] = s.mixed[b, :, j, :].astype(bf16)
        clock.spend(0.1)

        begin = clock.now
        for step in range(depth - 1, 0, -1):
            remote(slots2.at[z], slots2.at[z], s.line_send.at[b], s.line_recv.at[b],
                   place.device(place.on(place.sweep(step)))).start()
        line_view = slots2.at[pl.ds(0, depth - 1)]
        sends.append(departed(line_view, s.line_send.at[b]))
        if b == 0:
            for index in range(3):
                yield begin + 0.9 + 0.9 * index
                if index == 0:
                    need(1)
                wide_pass(index)
            down_across()
        yield begin + (5.5 if b == 0 else 6.5)
        arrived(line_view, s.line_recv.at[b])
        need(21)
        if b == 0:
            arrived(s.wo.at[pl.ds(0, 3), 0], s.pass_recv.at[0])
        line_rows = slots2[...].reshape(depth * seq, width)
        product = dot_t(line_rows, s.wo[...].reshape(plane * lanes, width)).astype(bf16)
        slots3[chip] = product.reshape(depth, seq, plane * lanes)
        clock.spend(0.7)

        gather = Gather(place, clock, s.gather_send.at[b, 1], s.gather_recv.at[b, 0], 1, (
            lambda o: slots3.at[o, pl.ds(0, depth // 2)],
            lambda o: slots3.at[o, pl.ds(depth // 2, depth // 2)],
        ))
        sends.append(gather.finish)
        yield from gather.steps()
        if b == 0:
            need(12)
            arrived(s.wd.at[:, pl.ds(0, 3), core], s.down_recv.at[1])
            down_swap.start()
            sends.append(down_swap.wait_send)
        both = s.rows.at[b]
        acc = s.acc.at[b]

        def serve(c, lent):
            if lent:
                arrived(both.at[c], s.row_recv.at[b])
            every = both[c, :, :width]
            served = (jax.nn.silu(dot(every, s.eg[...])) * dot(every, s.eu[...])).astype(bf16)
            note_lane = lax.broadcasted_iota(jnp.int32, (rows, lanes), 1)
            mine = (note_lane == me) | (note_lane == me + experts)
            weight = jnp.sum(jnp.where(mine, both[c, :, width:].astype(f32), 0.0), axis=1, keepdims=True)
            for n in range(4):
                at = slice(n * chunk, (n + 1) * chunk)
                value = dot(served, s.ed[:, at])
                value = jnp.where(weight != 0.0, value * weight, 0.0)
                if lent:
                    s.gift[n] = value.astype(bf16)
                    remote(s.gift.at[n], s.given.at[n], s.gift_send.at[0], s.gift_recv.at[n // 2],
                           place.partner).start()
                else:
                    acc[:, :, at] = value.reshape(chips, seq, chunk)

        yield gather.due(0)
        need(8, 9, 10)
        gather.rest(0)

        block = rows // 2
        served_here = pl.when(group == b)
        line = depth * seq
        for n in range(2):
            at = slice(n * block, (n + 1) * block)
            for p in range(n * plane // 2, (n + 1) * plane // 2):
                of = slice(p * line, (p + 1) * line)
                token = jnp.concatenate(
                    [slots1[k * plane + p, :, lanes:].astype(f32) for k in range(depth)], axis=0)
                projected = jnp.concatenate(
                    [slots3[k * plane + p].reshape(line, plane * lanes) for k in range(depth)], axis=1)
                both[core, of, :width] = norm_rows(token + projected.astype(f32), gain2_ref[...])
                for k in range(depth):
                    both[core, p * line + k * seq : p * line + (k + 1) * seq, width:] = (
                        slots1[k * plane + p, :, :lanes])

            @served_here
            def _():
                remote(both.at[core, at], both.at[core, at], s.row_send.at[b], s.row_recv.at[b],
                       place.partner).start()

        clock.spend(0.4)

        need(2, 3, 22, 23)
        normed = both[core, :, :width]
        gate = dot_t(normed, s.wg[...])
        hidden = jax.nn.silu(gate) * dot_t(normed, s.wu[...])
        s.hidden[b] = hidden
        squares = s.squares.at[b]
        summed = jnp.broadcast_to(jnp.sum(hidden * hidden, axis=1, keepdims=True), (rows, lanes))
        squares[chip] = jnp.transpose(summed)[:1]

        def square_copy(target):
            return remote(squares.at[chip], squares.at[chip], s.square_send.at[b],
                          s.square_recv.at[b], place.device(target))

        for target in others():
            square_copy(target).start()
        sends.append(departed(squares.at[others_ds], s.square_send.at[b]))
        clock.spend(0.5)
        sent_at = clock.now

        for c in range(2):

            @pl.when((group == b) & (core == c))
            def _():
                serve(c, False)

        clock.spend(1.0)
        yield sent_at + (1.5 if b == 0 else 5.5)

        @pl.when((group == b) & (core == 1))
        def _():
            serve(0, True)

        @pl.when((group == b) & (core == 0))
        def _():
            serve(1, True)

        clock.spend(0.6)

        def end_served():
            @pl.when(group == b)
            def _():
                departed(both.at[core], s.row_send.at[b])()
                departed(s.gift, s.gift_send.at[0])()

        sends.append(end_served)
        yield sent_at + 5.5

        arrived(squares.at[others_ds], s.square_recv.at[b])
        total = squares[0]
        for c in range(1, chips):
            total = total + squares[c]
        scale = lax.rsqrt(total / width + epsilon)
        scale = jnp.transpose(jnp.broadcast_to(scale, (lanes, rows)))
        gain = hgain_ref[:, pl.ds(pl.multiple_of(chip * lanes, lanes), lanes)]
        dense = (s.hidden[b] * scale * gain).astype(bf16)
        need(24)

        stage = s.stage.at[b]
        if b > 0:
            yield sent_at + 7.5

        def staged(piece, value, slot, index, recv, target):
            stage[piece, slot] = value.astype(bf16)
            remote(stage.at[piece, slot], s.sums.at[b, piece, index], s.sum_send.at[b, piece],
                   s.sum_recv.at[b, piece, recv], place.device(target)).start()

        def summands(piece, index, count, recv):
            view = s.sums.at[b, piece, pl.ds(index, count)]
            arrived(view, s.sum_recv.at[b, piece, recv])

        def summand(piece, index):
            return s.sums[b, piece, index].astype(f32)

        for piece in range(2):
            sends.append(departed(stage.at[piece, pl.ds(0, 4 * depth - 1)], s.sum_send.at[b, piece]))
            first, second = (place.turn(a) for a in ORDERS[piece])

            @served_here
            def _():
                arrived(s.given.at[pl.ds(2 * piece, 2)], s.gift_recv.at[piece])

            for c in (2 * piece, 2 * piece + 1):
                at = slice(c * chunk, (c + 1) * chunk)
                down = s.wd[c * depth // 4 : (c + 1) * depth // 4].reshape(chunk, lanes)
                value = jax.nn.sigmoid(logit_ref[:, at]) * dot_t(dense, down)
                value = value.reshape(chips, seq, chunk)

                @served_here
                def _():
                    acc[:, :, at] += s.given[c].astype(f32).reshape(chips, seq, chunk) + value

                @pl.when(group != b)
                def _():
                    acc[:, :, at] = value

            for beside in (1, 0):
                for step in range(depth - 1, -1, -1):
                    zo = place.sweep(step)
                    turn = (1, 1) if beside else first
                    index, recv = (zo, zo) if beside else (depth + 2 * zo, depth + zo)
                    staged(piece, acc[spot(place.on(zo, *turn)), :, columns_of(piece)], step * 2 + beside,
                           index, recv, place.on(z, *first))
        clock.spend(1.0)
        begin = clock.now

        for step in range(depth - 1, -1, -1):
            yield begin + (4.3 if b == 0 else 5.0) + 0.02 * (depth - 1 - step)
            for piece in range(2):
                first, second = (place.turn(a) for a in ORDERS[piece])
                zo = place.sweep(step)
                summands(piece, zo, 1, zo)
                value = acc[spot(place.on(zo, *second)), :, columns_of(piece)] + summand(piece, zo)
                staged(piece, value, 2 * depth + step, depth + 2 * zo + 1, depth + zo, place.on(z, *second))

        def folded(piece, zo):
            summands(piece, depth + 2 * zo, 2, depth + zo)
            value = acc[spot(place.on(zo)), :, columns_of(piece)] + summand(piece, depth + 2 * zo)
            return value + summand(piece, depth + 2 * zo + 1)

        for step in range(depth - 1, 0, -1):
            yield begin + 8.0 + 0.2 * (depth - 1 - step)
            for piece in range(2):
                zo = place.sweep(step)
                staged(piece, folded(piece, zo), 3 * depth + step - 1, 3 * depth + z, 2 * depth, place.on(zo))
        yield begin + 15.0
        for piece in range(2):
            at = columns_of(piece)
            value = slots1[chip, :, lanes + piece * half : lanes + (piece + 1) * half].astype(f32)
            value = value + jnp.concatenate(
                [slots3[k * plane + spot_me, z] for k in range(piece * depth // 2, (piece + 1) * depth // 2)], axis=1
            ).astype(f32)
            acc[spot(chip), :, at] = value + folded(piece, z)
        yield begin + 20.0
        for piece in range(2):
            summands(piece, 3 * depth, depth - 1, 2 * depth)
            value = acc[spot(chip), :, columns_of(piece)]
            for step in range(1, depth):
                value = value + summand(piece, 3 * depth + place.sweep(step))
            s.final[b * seq : (b + 1) * seq, columns_of(piece)] = value.astype(bf16)

    clock.run([batch(b) for b in range(BATCHES)])
    out_ref[...] = dot(backward, s.final[...]).astype(bf16)
    for end in sends:
        end()


def copy_kernel(a_ref, b_ref, c_ref, a_out, b_out, c_out):
    a_out[...] = a_ref[...]
    b_out[...] = b_ref[...]
    c_out[...] = c_ref[...]


def layer_scratch(chips, depth, tokens, width, span, fe):
    n = BATCHES
    seq = tokens // n
    rows = chips * seq
    bf16, f32, DMA = jnp.bfloat16, jnp.float32, pltpu.SemaphoreType.DMA
    half = width // 2
    return dict(
        slots1=pltpu.VMEM((n, chips, seq, LANES + width), bf16),
        slots2=pltpu.VMEM((n, depth, seq, width), bf16),
        slots3=pltpu.VMEM((n, chips, depth, seq, chips // depth * LANES), bf16),
        keys=pltpu.VMEM((tokens, span, LANES), bf16),
        values=pltpu.VMEM((tokens, span, LANES), bf16),
        wq=pltpu.VMEM((LANES, width), bf16),
        wo=pltpu.VMEM((chips // depth, 2, LANES // 2, width), bf16),
        wg=pltpu.VMEM((LANES, width), bf16),
        wu=pltpu.VMEM((LANES, width), bf16),
        wk=pltpu.VMEM((width, LANES), bf16),
        wv=pltpu.VMEM((width, LANES), bf16),
        eg=pltpu.VMEM((width, fe), bf16),
        eu=pltpu.VMEM((width, fe), bf16),
        ed=pltpu.VMEM((fe, width), bf16),
        wd=pltpu.VMEM((depth, chips // depth, 2, LANES // 2, LANES), bf16),
        transit=pltpu.VMEM((depth, LANES // 2, chips // depth * LANES), bf16),
        after=pltpu.VMEM((2 * LANES, 2 * LANES), bf16),
        bias=pltpu.VMEM((HEADS, LANES), f32),
        tiles=pltpu.VMEM((n, chips, seq, LANES), bf16),
        landed=pltpu.VMEM((n, chips, seq, LANES), bf16),
        heads=pltpu.VMEM((n, seq, chips, LANES), f32),
        mixed=pltpu.VMEM((n, seq, chips, LANES), f32),
        rows=pltpu.VMEM((n, 2, rows, width + LANES), bf16),
        final=pltpu.VMEM((tokens, width), bf16),
        hidden=pltpu.VMEM((n, rows, LANES), f32),
        squares=pltpu.VMEM((n, chips, 1, rows), f32),
        gift=pltpu.VMEM((4, rows, width // 4), bf16),
        given=pltpu.VMEM((4, rows, width // 4), bf16),
        acc=pltpu.VMEM((n, chips, seq, width), f32),
        stage=pltpu.VMEM((n, 2, 4 * depth, seq, half), bf16),
        sums=pltpu.VMEM((n, 2, 4 * depth, seq, half), bf16),
        local_sem=DMA((13,)),
        swap_send=DMA((5,)),
        swap_recv=DMA((5,)),
        gather_send=DMA((n, 2, 2)),
        gather_recv=DMA((n, 1, 2, 5 * depth // 2)),
        line_send=DMA((n,)),
        line_recv=DMA((n,)),
        wide_send=DMA((1,)),
        wide_recv=DMA((3,)),
        pass_send=DMA((1,)),
        pass_recv=DMA((1,)),
        tile_send=DMA((n,)),
        tile_recv=DMA((n,)),
        down_send=DMA((2,)),
        down_recv=DMA((2,)),
        square_send=DMA((n,)),
        square_recv=DMA((n,)),
        row_send=DMA((n,)),
        row_recv=DMA((n,)),
        gift_send=DMA((1,)),
        gift_recv=DMA((2,)),
        sum_send=DMA((n, 2)),
        sum_recv=DMA((n, 2, 2 * depth + 1)),
    )


def fused_shards(
    tokens, cache_keys, cache_values, cache_len, norm_gain_first, w_query, w_key, w_value, head_bias,
    w_output, norm_gain_second, group_id, member, group_gate, member_weight, expert_gate_w,
    expert_up_w, expert_down_w, dense_gate_w, dense_up_w, hidden_gain, dense_down_w, branch_logit,
):
    chips = lax.axis_size("ep") // 2
    seq, width = tokens.shape
    span = cache_keys.shape[1]
    bf16 = jnp.bfloat16
    scratch = layer_scratch(chips, torus_of(chips)[0], seq, width, span, expert_gate_w.shape[2])
    smem = pl.BlockSpec(memory_space=pltpu.SMEM)
    anywhere = pl.BlockSpec(memory_space=pl.ANY)
    out_shape = (
        jax.ShapeDtypeStruct((seq, width), bf16),
        jax.ShapeDtypeStruct((seq, LANES), bf16),
        jax.ShapeDtypeStruct((seq, LANES), bf16),
    )
    results = pl.pallas_call(
        functools.partial(layer_kernel, chips, tuple(scratch)),
        out_shape=out_shape,
        in_specs=[smem] * 3 + [whole()] * 9 + [anywhere] * 12,
        out_specs=(whole(),) * 3,
        scratch_shapes=list(scratch.values()),
        compiler_params=pltpu.CompilerParams(
            collective_id=1, has_side_effects=True, vmem_limit_bytes=60 * 1024 * 1024
        ),
        name="layer",
    )(
        cache_len, group_id, head_bias, tokens, norm_gain_first[None], norm_gain_second[None], hidden_gain[None],
        branch_logit[None], member.T, member_weight.T, group_id[None], group_gate[None],
        cache_keys, cache_values, w_query.T, w_output.T, dense_gate_w.T, dense_up_w.T, dense_down_w.T,
        w_key, w_value, expert_gate_w, expert_up_w, expert_down_w,
    )
    return pl.pallas_call(
        copy_kernel, out_shape=out_shape, in_specs=[whole()] * 3, out_specs=(whole(),) * 3, name="results"
    )(*results)


def one_kernel(mesh):
    chips = mesh.shape["ep"] // 2
    depth, height, width = torus_of(chips)
    return (height, width) == (2, 2) and chips * LANES == HEADS * HEAD_DIM and 4 * chips <= LANES and depth % 4 == 0 and 2 * chips == BATCHES * PER_GROUP


def solution(mesh):
    in_specs = (
        P("ep", None),
        P("ep", None, None),
        P("ep", None, None),
        P("ep"),
        P(),
        P(None, "ep"),
        P(),
        P(),
        P(),
        P(None, "ep"),
        P(),
        P("ep"),
        P("ep", None),
        P("ep"),
        P("ep", None),
        P("ep", None, None),
        P("ep", None, None),
        P("ep", None, None),
        P(None, "ep"),
        P(None, "ep"),
        P(),
        P(None, "ep"),
        P(),
    )
    out_specs = (P("ep", None), P("ep", None), P("ep", None))
    body = fused_shards if one_kernel(mesh) else shards
    return jax.shard_map(body, mesh=mesh, in_specs=in_specs, out_specs=out_specs, check_vma=False)
```
